256 devices in a mesh: kv: 32 (over z, y), tp: 8 (over x, core).
Axes of the slice: x: 4, y: 4, z: 8, core: 2. Of those that a mesh axis runs over, the one named last changes fastest.
Arguments:
- stream: bfloat16 [128, 4096], P(None, ('kv', 'tp')), may hold values from -60 to 60
- memory_state: float32 [128, 32, 128, 128], P('kv', 'tp'), may hold values from -3 to 3
- attn_gain: float32 [4096], P('kv'), may hold values from 0.1 to 1.9
- query_weight: bfloat16 [4096, 4096], P('kv', 'tp'), may hold values from -0.09375 to 0.09375
- key_weight: bfloat16 [4096, 4096], P('kv', 'tp'), may hold values from -0.09375 to 0.09375
- value_weight: bfloat16 [4096, 4096], P('kv', 'tp'), may hold values from -0.09375 to 0.09375
- outgate_weight: bfloat16 [4096, 4096], P('kv', 'tp'), may hold values from -0.09375 to 0.09375
- beta_weight: bfloat16 [4096, 32], P('kv', 'tp'), may hold values from -0.09375 to 0.09375
- decay_weight: bfloat16 [4096, 32], P('kv', 'tp'), may hold values from -0.09375 to 0.09375
- decay_log: float32 [32], P('tp'), may hold values from -4 to 1
- decay_shift: float32 [32], P('tp'), may hold values from -3 to 3
- head_gain: float32 [128], replicated, may hold values from 0.1 to 1.9
- output_weight: bfloat16 [4096, 4096], P('tp', 'kv'), may hold values from -0.09375 to 0.09375
- mixer_gain: float32 [4096], P('kv'), may hold values from 0.1 to 1.9
- up_weight: bfloat16 [4096, 16384], P('kv', 'tp'), may hold values from -0.09375 to 0.09375
- down_weight: bfloat16 [16384, 4096], P('tp', 'kv'), may hold values from -0.046875 to 0.046875
Outputs:
- layer_out: bfloat16 [128, 4096], P(None, ('kv', 'tp'))
- memory_next: float32 [128, 32, 128, 128], P('kv', 'tp')
The draws below stay inside these ranges and needn't reach their ends.
All inputs are finite; a program needn't handle non-finite values.
Results may differ from the reference program's by a relative error of at most 0.025.
Values may be sent and summed in bfloat16 or wider, within the bound.
A program may use at most 64 MiB of HBM per device.

```python
import math
import jax
import jax.numpy as jnp
from jax import lax

D = 4096
HEADS = 32
HEAD_DIM = 128
FF = 16384
SEQ_DEV = 4
BATCH = 128
VAL = 4096


def draw_stream(key, part):
    keys = jax.random.split(key, 3)
    columns = jnp.arange(D, dtype=jnp.float32) / D
    base = jnp.clip(jax.random.normal(keys[0], (BATCH, D), jnp.float32), -5.0, 5.0)
    rising = jnp.exp(math.log(3.0) * columns)
    rising = rising / jnp.mean(rising)
    column_scale = rising * jax.random.uniform(keys[1], (D,), jnp.float32, 0.6, 1.4)
    row_scale = jnp.exp(jax.random.uniform(keys[2], (BATCH, 1), jnp.float32, math.log(0.3), math.log(3.0)))
    return (base * column_scale[None, :] * row_scale).astype(jnp.bfloat16)


def shard_levels(own_key, dims, shards, least, largest):
    loudness, own = 1.0, jax.random.fold_in(own_key, 6)
    for dim, blocks in shards:
        draws = jnp.exp(jax.random.uniform(jax.random.fold_in(own, dim), (blocks,), jnp.float32, least / len(shards), largest / len(shards)))
        loudness = loudness * jnp.repeat(draws, dims[dim] // blocks).reshape([-1 if axis == dim else 1 for axis in range(len(dims))])
    return loudness


def centred(own_key, dims, width, limit, cuts=(), kind=jnp.bfloat16):
    drawn = jax.random.normal(own_key, dims, jnp.float32) * width
    if len(cuts) > 0:
        drawn = shard_levels(own_key, dims, cuts, -0.22, 0.18) * drawn
    return jnp.clip(drawn, min=-limit, max=limit).astype(kind)


def setup_inputs(seed: int = 0) -> dict:
    streams_of = jax.random.split(jax.random.key(seed), 17)
    stream = draw_stream(jax.random.fold_in(streams_of[16], 71), 0)
    memory_state = centred(streams_of[1], (BATCH, HEADS, HEAD_DIM, HEAD_DIM), 0.5, 3.0, ((0, 32), (1, 8)), jnp.float32)
    attn_gain = jnp.clip(1.0 + 0.18 * jax.random.normal(streams_of[2], (D,), jnp.float32), 0.1, 1.9)
    query_weight = centred(streams_of[3], (D, VAL), D ** -0.5, 0.09375, ((0, 32), (1, 8)))
    key_weight = centred(streams_of[4], (D, VAL), D ** -0.5, 0.09375, ((0, 32), (1, 8)))
    value_weight = centred(streams_of[5], (D, VAL), D ** -0.5, 0.09375, ((0, 32), (1, 8)))
    outgate_weight = centred(streams_of[6], (D, VAL), D ** -0.5, 0.09375, ((0, 32), (1, 8)))
    beta_weight = centred(streams_of[7], (D, HEADS), D ** -0.5, 0.09375, ((0, 32), (1, 8)))
    decay_weight = centred(streams_of[8], (D, HEADS), D ** -0.5, 0.09375, ((0, 32), (1, 8)))
    decay_log = jnp.clip(-4.0 + 5.0 * jax.random.uniform(streams_of[9], (HEADS,), jnp.float32) ** shard_levels(streams_of[9], (HEADS,), ((0, 8),), -0.2, 0.2), -4.0, 1.0)
    decay_shift = centred(streams_of[10], (HEADS,), 1.0, 3.0, ((0, 8),), jnp.float32)
    head_gain = jnp.clip(1.0 + 0.18 * jax.random.normal(streams_of[11], (HEAD_DIM,), jnp.float32), 0.1, 1.9)
    output_weight = centred(streams_of[12], (VAL, D), VAL ** -0.5, 0.09375, ((0, 8), (1, 32)))
    mixer_gain = jnp.clip(1.0 + 0.18 * jax.random.normal(streams_of[13], (D,), jnp.float32), 0.1, 1.9)
    up_weight = centred(streams_of[14], (D, FF), D ** -0.5, 0.09375, ((0, 32), (1, 8)))
    down_weight = centred(streams_of[15], (FF, D), FF ** -0.5, 0.046875, ((0, 8), (1, 32)))
    return dict(stream=stream, memory_state=memory_state, attn_gain=attn_gain, query_weight=query_weight, key_weight=key_weight, value_weight=value_weight, outgate_weight=outgate_weight, beta_weight=beta_weight, decay_weight=decay_weight, decay_log=decay_log, decay_shift=decay_shift, head_gain=head_gain, output_weight=output_weight, mixer_gain=mixer_gain, up_weight=up_weight, down_weight=down_weight)


epsilon = 1e-06

def normed_rows(stream, gain_vec):
    widened = stream.astype(jnp.float32)
    factor = lax.rsqrt(lax.optimization_barrier(jnp.sum(widened * widened, axis=1)) / D + epsilon)
    scaled = (widened * gain_vec.astype(jnp.float32)).astype(jnp.bfloat16)
    return (scaled, factor[:, None])

def unit_rows(values):
    return values * lax.rsqrt(lax.optimization_barrier(jnp.sum(values * values, axis=-1, keepdims=True)) + epsilon)

def head_output(memory_state, query_sum, key_sum, value_sum, gate_sum, beta_sum, decay_sum, decay_log, decay_shift, head_gain):
    row_count = query_sum.shape[0]
    head_count = beta_sum.shape[1]

    def to_heads(values):
        return values.reshape(row_count, head_count, HEAD_DIM)
    query_heads = unit_rows(jax.nn.silu(to_heads(query_sum))) * HEAD_DIM ** (-0.5)
    key_heads = unit_rows(jax.nn.silu(to_heads(key_sum)))
    value_heads = jax.nn.silu(to_heads(value_sum))
    beta_heads = jax.nn.sigmoid(beta_sum)
    decay_heads = jnp.exp(-jnp.exp(decay_log) * jax.nn.softplus(decay_sum + decay_shift))
    kept_state = memory_state * decay_heads[:, :, None, None]
    recalled = jnp.einsum('bhkv,bhk->bhv', kept_state, key_heads)
    correction = beta_heads[:, :, None] * (value_heads - recalled)
    memory_next = kept_state + key_heads[:, :, :, None] * correction[:, :, None, :]
    readout = jnp.einsum('bhkv,bhk->bhv', memory_next, query_heads)
    normed = readout * lax.rsqrt(lax.optimization_barrier(jnp.mean(readout * readout, axis=-1, keepdims=True)) + epsilon)
    gated = normed * head_gain.astype(jnp.float32) * jax.nn.silu(to_heads(gate_sum))
    return (gated.reshape(row_count, head_count * HEAD_DIM).astype(jnp.bfloat16), memory_next)

def reference(stream, memory_state, attn_gain, query_weight, key_weight, value_weight, outgate_weight, beta_weight, decay_weight, decay_log, decay_shift, head_gain, output_weight, mixer_gain, up_weight, down_weight):
    batch_rows = stream.shape[0]
    scaled, factor = normed_rows(stream, attn_gain)

    def project(weight):
        return jnp.dot(scaled, weight, preferred_element_type=jnp.float32) * factor
    sums = tuple((project(weight) for weight in (query_weight, key_weight, value_weight, outgate_weight, beta_weight, decay_weight)))
    groups = batch_rows // SEQ_DEV

    def regroup(values):
        return values.reshape((groups, SEQ_DEV) + values.shape[1:])

    def one_group(inputs):
        return head_output(*inputs, decay_log, decay_shift, head_gain)
    heads_out, memory_next = lax.map(one_group, (regroup(memory_state),) + tuple((regroup(values) for values in sums)))
    heads_out = heads_out.reshape(batch_rows, heads_out.shape[-1])
    memory_next = memory_next.reshape(memory_state.shape)
    attn = jnp.dot(heads_out, output_weight, preferred_element_type=jnp.float32)
    middle = (stream.astype(jnp.float32) + attn).astype(jnp.bfloat16)
    scaled_mix, factor_mix = normed_rows(middle, mixer_gain)
    up_values = jnp.dot(scaled_mix, up_weight, preferred_element_type=jnp.float32) * factor_mix
    hidden = jnp.square(jax.nn.relu(up_values)).astype(jnp.bfloat16)
    mixer = jnp.dot(hidden, down_weight, preferred_element_type=jnp.float32)
    layer_out = (middle.astype(jnp.float32) + mixer).astype(jnp.bfloat16)
    return (layer_out, memory_next)
```

```python
import functools

import jax
import jax.numpy as jnp
from jax import lax
from jax.experimental import pallas as pl
from jax.experimental.pallas import tpu as pltpu
from jax.sharding import PartitionSpec as P

MESH = pl.DeviceIdType.MESH
F32 = jnp.float32
BF16 = jnp.bfloat16
EPS = 1e-06
Y = 4
L = 128
HEADS_DEV = 4
ROWS = 4


def transposed(x):
    return jnp.transpose(x, (1, 0))


def silu(x):
    return x * jax.nn.sigmoid(x)


def softplus(x):
    return jnp.maximum(x, 0.0) + jnp.log1p(jnp.exp(-jnp.abs(x)))


def layer_kernel(
    Z,
    T,
    stream_ref,
    attn_gain_ref,
    mixer_gain_ref,
    head_gain_ref,
    beta_ref,
    decay_ref,
    decay_log_ref,
    decay_shift_ref,
    state_ref,
    wq_ref,
    wk_ref,
    wv_ref,
    wg_ref,
    wo_ref,
    wu_ref,
    wd_ref,
    out_ref,
    next_ref,
    state,
    state_out,
    w_in,
    wo,
    gains,
    etile,
    pad,
    sgath,
    w1,
    xz,
    s2,
    r2,
    rows_f,
    hall,
    a4,
    r4,
    mgath,
    wu,
    wd,
    sq,
    u6,
    r6,
    hall7,
    d8,
    r8,
    lsem,
    ssem,
    rsem,
):
    N = Z * Y
    PL = Y * T
    B = N * ROWS
    DT = L // T
    D = N * L
    kv = lax.axis_index("kv")
    tp = lax.axis_index("tp")
    z = lax.div(kv, Y)
    y = lax.rem(kv, Y)
    me_p = y * T + tp

    def plane_dev(p):
        return (z * Y + lax.div(p, T), lax.rem(p, T))

    def kv_dev(p):
        return (p, tp)

    def each_peer(n, me, act):
        def step(i, c):
            off = 1 + lax.rem(i + (n // 2 - 1), n - 1)
            act(lax.rem(me + off, n))
            return c

        lax.fori_loop(0, n - 1, step, 0)

    def put(src, dst, k, dev):
        pltpu.make_async_remote_copy(
            src_ref=src,
            dst_ref=dst,
            send_sem=ssem.at[k],
            recv_sem=rsem.at[k],
            device_id=dev,
            device_id_type=MESH,
        ).start()

    def got(ref, k):
        pltpu.make_async_copy(ref, ref, rsem.at[k]).wait()

    def sent(ref, k):
        pltpu.make_async_copy(ref, ref, ssem.at[k]).wait()

    barrier = pltpu.get_barrier_semaphore()

    def greet(dev):
        pl.semaphore_signal(barrier, inc=1, device_id=dev, device_id_type=MESH)

    each_peer(N, kv, lambda p: greet(kv_dev(p)))

    def greet_plane(p):
        @pl.when(lax.rem(p, T) != tp)
        def _():
            greet(plane_dev(p))

    each_peer(PL, me_p, greet_plane)

    loads = [
        pltpu.make_async_copy(w, w_in.at[m], lsem.at[m])
        for m, w in enumerate((wq_ref, wk_ref, wv_ref, wg_ref))
    ]
    load_out = pltpu.make_async_copy(wo_ref, wo, lsem.at[4])
    load_state = pltpu.make_async_copy(state_ref, state, lsem.at[5])
    for c in loads:
        c.start()
    load_out.start()
    load_state.start()

    gains[y] = jnp.broadcast_to(attn_gain_ref[...], (8, L))
    gains[y, 1:2, :] = mixer_gain_ref[...]
    pad[...] = jnp.zeros((L, L), F32)
    pad[:, 0:4] = beta_ref[...].astype(F32)
    pad[:, 4:8] = decay_ref[...].astype(F32)
    etile[y] = transposed(pad[...])[0:16].astype(BF16)
    pad[...] = jnp.zeros((L, L), F32)
    pad[0:B, 0:DT] = stream_ref[...].astype(F32)
    own_stream = transposed(pad[0:B, :])[0:DT]
    sgath[me_p] = own_stream.astype(BF16)

    pl.semaphore_wait(barrier, (N - 1) + (PL - 1) - (Y - 1))

    each_peer(PL, me_p, lambda p: put(sgath.at[me_p], sgath.at[me_p], 0, plane_dev(p)))
    for off in (2, 1, 3):
        yy = lax.rem(y + off, Y)
        put(gains.at[y], gains.at[y], 1, (z * Y + yy, tp))
        put(etile.at[y], etile.at[y], 2, (z * Y + yy, tp))
    for c in loads:
        c.wait()

    def head_cols(m, yy):
        return w_in.at[m, :, pl.ds(pl.multiple_of(yy * L, L), L)]

    def w1_cols(m):
        return w1.at[y, :, pl.ds(m * L, L)]

    own_w1 = [pltpu.make_async_copy(head_cols(m, y), w1_cols(m), lsem.at[6 + m]) for m in range(4)]
    for m in range(4):
        for off in (2, 1, 3):
            yy = lax.rem(y + off, Y)
            put(head_cols(m, yy), w1_cols(m), 3, (z * Y + yy, tp))
        own_w1[m].start()

    got(sgath.at[pl.ds(0, PL - 1)], 0)
    got(gains.at[pl.ds(0, Y - 1)], 1)
    got(etile.at[pl.ds(0, Y - 1)], 2)
    scaled = []
    x_part = jnp.zeros((16, B), F32)
    squares = jnp.zeros((1, B), F32)
    for j in range(Y):
        block = sgath[j * T : (j + 1) * T].astype(F32).reshape(L, B)
        squares = squares + jnp.sum(block * block, axis=0, keepdims=True)
        part = (transposed(block) * gains[j, 0:1, :]).astype(BF16)
        scaled.append(part)
        x_part = x_part + lax.dot_general(
            etile[j], part, (((1,), (1,)), ((), ())), preferred_element_type=F32
        )
    row16 = lax.broadcasted_iota(jnp.int32, (16, B), 0)
    xz[z] = jnp.where(row16 == 8, squares, x_part)
    for off in (4, 3, 5, 2, 6, 1, 7):
        if off < Z:
            zz = lax.rem(z + off, Z)
            put(xz.at[z], xz.at[z], 4, (zz * Y + y, tp))

    for c in own_w1:
        c.wait()
    got(w1.at[pl.ds(0, Y - 1)], 3)
    proj = jnp.zeros((B, 4 * L), F32)
    for j in range(Y):
        proj = proj + jnp.dot(scaled[j], w1[j], preferred_element_type=F32)
    low = lax.broadcasted_iota(jnp.int32, (B // 8, 8, L), 1) < 4

    def pair_tiles(a, b):
        return (
            jnp.where(low, a, pltpu.roll(b, 4, 1)),
            jnp.where(low, pltpu.roll(a, 4, 1), b),
        )

    pq, pk, pv, pg = [proj[:, m * L : (m + 1) * L].reshape(B // 8, 8, L) for m in range(4)]
    even_a, odd_a = pair_tiles(pq, pk)
    even_b, odd_b = pair_tiles(pv, pg)
    s2[:, 0] = jnp.concatenate([even_a, even_b], axis=1).astype(BF16)
    s2[:, 1] = jnp.concatenate([odd_a, odd_b], axis=1).astype(BF16)
    each_peer(
        N, kv, lambda p: put(s2.at[lax.div(p, 2), lax.rem(p, 2)], r2.at[kv], 5, kv_dev(p))
    )
    r2[kv] = s2[lax.div(kv, 2), lax.rem(kv, 2)]

    def up_cols(yy):
        return wu_ref.at[:, pl.ds(pl.multiple_of(yy * 4 * L, L), 4 * L)]

    own_up = pltpu.make_async_copy(up_cols(y), wu.at[y], lsem.at[10])
    own_up.start()
    for off in (2, 1, 3):
        yy = lax.rem(y + off, Y)
        put(up_cols(yy), wu.at[y], 6, (z * Y + yy, tp))

    got(xz.at[pl.ds(0, Z - 1)], 4)
    x_all = xz[0]
    for j in range(1, Z):
        x_all = x_all + xz[j]
    fac = lax.rsqrt(x_all[8:9] / D + EPS)
    xf = x_all * fac
    dlog = jnp.zeros((16, B), F32)
    dshift = jnp.zeros((16, B), F32)
    for h in range(HEADS_DEV):
        dlog = jnp.where(row16 == 4 + h, decay_log_ref[h], dlog)
        dshift = jnp.where(row16 == 4 + h, decay_shift_ref[h], dshift)
    scal = jnp.where(
        row16 < 4,
        jax.nn.sigmoid(xf),
        jnp.where(row16 < 8, jnp.exp(-jnp.exp(dlog) * softplus(xf + dshift)), fac),
    )
    lane_group = lax.div(lax.broadcasted_iota(jnp.int32, (16, B), 1), 4)
    mine = jnp.zeros((16, B), F32)
    for m in range(4):
        rolled = pltpu.roll(scal, lax.rem(B + m * ROWS - kv * ROWS, B), 1)
        mine = jnp.where(lane_group == m, rolled, mine)
    cols = transposed(jnp.concatenate([mine, jnp.zeros((L - 16, B), F32)], axis=0))[0:16]

    got(r2.at[pl.ds(0, N - 1)], 5)
    load_state.wait()
    row_id = lax.broadcasted_iota(jnp.int32, (16, 1), 0)
    acts = []
    for h in range(HEADS_DEV):
        total = r2[h].astype(F32)
        for j in range(1, Z):
            total = total + r2[j * Y + h].astype(F32)
        a = silu(total * cols[:, 8:9])
        inv = lax.rsqrt(jnp.sum(a * a, axis=1, keepdims=True) + EPS)
        norm = jnp.where(row_id < 4, inv * L ** (-0.5), jnp.where(row_id < 8, inv, 1.0))
        acts.append(a * norm)
        rows_f[1, 4 * h : 4 * h + 4, :] = a[12:16]
    flipped = transposed(jnp.concatenate(acts + [jnp.zeros((L - 64, L), F32)], axis=0))
    for h in range(HEADS_DEV):
        for r in range(ROWS):
            q_col = flipped[:, h * 16 + r : h * 16 + r + 1]
            k_col = flipped[:, h * 16 + 4 + r : h * 16 + 5 + r]
            kept = state[r, h] * cols[r : r + 1, 4 + h : 5 + h]
            recalled = jnp.sum(kept * k_col, axis=0, keepdims=True)
            corr = cols[r : r + 1, h : h + 1] * (acts[h][8 + r : 9 + r] - recalled)
            new = kept + k_col * corr
            state_out[r, h] = new
            rows_f[0, 4 * h + r : 4 * h + r + 1, :] = jnp.sum(new * q_col, axis=0, keepdims=True)
    readout = rows_f[0]
    readout = readout * lax.rsqrt(jnp.mean(readout * readout, axis=1, keepdims=True) + EPS)
    hall[kv] = (readout * head_gain_ref[...] * rows_f[1]).astype(BF16)

    each_peer(N, kv, lambda p: put(hall.at[kv], hall.at[kv], 7, kv_dev(p)))
    store_state = pltpu.make_async_copy(state_out, next_ref, lsem.at[11])
    store_state.start()

    def down_rows(yy):
        return wd_ref.at[pl.ds(pl.multiple_of(yy * 4 * L, L), 4 * L), :]

    own_down = pltpu.make_async_copy(down_rows(y), wd.at[y], lsem.at[12])
    own_down.start()
    for off in (2, 1, 3):
        yy = lax.rem(y + off, Y)
        put(down_rows(yy), wd.at[y], 8, (z * Y + yy, tp))

    load_out.wait()
    got(hall.at[pl.ds(0, N - 1)], 7)
    heads = hall[...].astype(F32).reshape(N // 2, 2, 2, 8, L)
    attn = jnp.zeros((B, L), F32)
    for c in range(2):
        h_even, h_odd = pair_tiles(heads[:, 0, c], heads[:, 1, c])
        for i, hh in ((2 * c, h_even), (2 * c + 1, h_odd)):
            attn = attn + jnp.dot(
                hh.reshape(B, L).astype(BF16),
                wo[i * L : (i + 1) * L, :],
                preferred_element_type=F32,
            )
    a4[...] = transposed(attn).reshape(T, DT, B).astype(BF16)
    each_peer(T, tp, lambda p: put(a4.at[p], r4.at[tp], 9, (kv, p)))
    r4[tp] = a4[tp]
    got(r4.at[pl.ds(0, T - 1)], 9)
    attn_mine = r4[0].astype(F32)
    for j in range(1, T):
        attn_mine = attn_mine + r4[j].astype(F32)
    middle = (own_stream + attn_mine).astype(BF16)

    mgath[me_p] = middle
    each_peer(PL, me_p, lambda p: put(mgath.at[me_p], mgath.at[me_p], 10, plane_dev(p)))
    own_up.wait()
    got(wu.at[pl.ds(0, Y - 1)], 6)
    got(mgath.at[pl.ds(0, PL - 1)], 10)
    up = jnp.zeros((B, 4 * L), F32)
    squares2 = jnp.zeros((1, B), F32)
    for j in range(Y):
        block = mgath[j * T : (j + 1) * T].astype(F32).reshape(L, B)
        squares2 = squares2 + jnp.sum(block * block, axis=0, keepdims=True)
        part = (transposed(block) * gains[j, 1:2, :]).astype(BF16)
        up = up + jnp.dot(part, wu[j], preferred_element_type=F32)
    u6[...] = up.astype(BF16).reshape(Z, 16, 4 * L)
    sq[z] = jnp.broadcast_to(squares2, (8, B))
    offs = [o for o in (4, 3, 5, 2, 6, 1, 7) if o < Z]
    for off in offs:
        zz = lax.rem(z + off, Z)
        put(u6.at[zz], r6.at[z], 11, (zz * Y + y, tp))
    for off in offs:
        zz = lax.rem(z + off, Z)
        put(sq.at[z], sq.at[z], 12, (zz * Y + y, tp))
    r6[z] = u6[z]
    got(r6.at[pl.ds(0, Z - 1)], 11)
    up_mine = r6[0].astype(F32)
    for j in range(1, Z):
        up_mine = up_mine + r6[j].astype(F32)
    hidden = jnp.square(jnp.maximum(up_mine, 0.0)).astype(BF16)
    hall7[z] = hidden
    for off in offs:
        zz = lax.rem(z + off, Z)
        put(hall7.at[z], hall7.at[z], 13, (zz * Y + y, tp))
    own_down.wait()
    got(wd.at[pl.ds(0, Y - 1)], 8)
    got(hall7.at[pl.ds(0, Z - 1)], 13)
    hid = hall7[...].reshape(B, 4 * L)
    for j in range(Y):
        part = jnp.dot(hid, wd[j], preferred_element_type=F32)
        d8[j * T : (j + 1) * T] = transposed(part).reshape(T, DT, B).astype(BF16)
    each_peer(PL, me_p, lambda p: put(d8.at[p], r8.at[me_p], 14, plane_dev(p)))
    r8[me_p] = d8[me_p]
    got(sq.at[pl.ds(0, Z - 1)], 12)
    total2 = sq[0, 0:1, :]
    for j in range(1, Z):
        total2 = total2 + sq[j, 0:1, :]
    factor2 = lax.rsqrt(total2 / D + EPS)
    got(r8.at[pl.ds(0, PL - 1)], 14)
    parts = [r8[j].astype(F32) for j in range(4)]
    for j in range(4, PL):
        parts[j % 4] = parts[j % 4] + r8[j].astype(F32)
    mixed = (parts[0] + parts[1]) + (parts[2] + parts[3])
    final = middle.astype(F32) + mixed * (factor2 * factor2)
    final = transposed(jnp.concatenate([final, jnp.zeros((L - DT, B), F32)], axis=0))
    out_ref[...] = final[:, 0:DT].astype(BF16)

    sent(sgath.at[pl.ds(0, PL - 1)], 0)
    sent(gains.at[pl.ds(0, Y - 1)], 1)
    sent(etile.at[pl.ds(0, Y - 1)], 2)
    sent(w1.at[pl.ds(0, Y - 1)], 3)
    sent(xz.at[pl.ds(0, Z - 1)], 4)
    sent(r2.at[pl.ds(0, N - 1)], 5)
    sent(wu.at[pl.ds(0, Y - 1)], 6)
    sent(hall.at[pl.ds(0, N - 1)], 7)
    sent(wd.at[pl.ds(0, Y - 1)], 8)
    sent(r4.at[pl.ds(0, T - 1)], 9)
    sent(mgath.at[pl.ds(0, PL - 1)], 10)
    sent(r6.at[pl.ds(0, Z - 1)], 11)
    sent(sq.at[pl.ds(0, Z - 1)], 12)
    sent(hall7.at[pl.ds(0, Z - 1)], 13)
    sent(r8.at[pl.ds(0, PL - 1)], 14)
    store_state.wait()


def shards(
    Z,
    T,
    stream,
    memory_state,
    attn_gain,
    query_weight,
    key_weight,
    value_weight,
    outgate_weight,
    beta_weight,
    decay_weight,
    decay_log,
    decay_shift,
    head_gain,
    output_weight,
    mixer_gain,
    up_weight,
    down_weight,
):
    N, PL, B, DT = Z * Y, Y * T, Z * Y * ROWS, L // T
    vmem = pl.BlockSpec(memory_space=pltpu.VMEM)
    smem = pl.BlockSpec(memory_space=pltpu.SMEM)
    hbm = pl.BlockSpec(memory_space=pl.ANY)
    layer_out, memory_next = pl.pallas_call(
        functools.partial(layer_kernel, Z, T),
        out_shape=(
            jax.ShapeDtypeStruct(stream.shape, BF16),
            jax.ShapeDtypeStruct(memory_state.shape, F32),
        ),
        in_specs=[vmem] * 6 + [smem] * 2 + [hbm] * 8,
        out_specs=(vmem, hbm),
        scratch_shapes=[
            pltpu.VMEM((ROWS, HEADS_DEV, L, L), F32),
            pltpu.VMEM((ROWS, HEADS_DEV, L, L), F32),
            pltpu.VMEM((4, L, 4 * L), BF16),
            pltpu.VMEM((4 * L, L), BF16),
            pltpu.VMEM((Y, 8, L), F32),
            pltpu.VMEM((Y, 16, L), BF16),
            pltpu.VMEM((L, L), F32),
            pltpu.VMEM((PL, DT, B), BF16),
            pltpu.VMEM((Y, L, 4 * L), BF16),
            pltpu.VMEM((Z, 16, B), F32),
            pltpu.VMEM((N // 2, 2, 16, L), BF16),
            pltpu.VMEM((N, 16, L), BF16),
            pltpu.VMEM((2, 16, L), F32),
            pltpu.VMEM((N, 16, L), BF16),
            pltpu.VMEM((T, DT, B), BF16),
            pltpu.VMEM((T, DT, B), BF16),
            pltpu.VMEM((PL, DT, B), BF16),
            pltpu.VMEM((Y, L, 4 * L), BF16),
            pltpu.VMEM((Y, 4 * L, L), BF16),
            pltpu.VMEM((Z, 8, B), F32),
            pltpu.VMEM((Z, 16, 4 * L), BF16),
            pltpu.VMEM((Z, 16, 4 * L), BF16),
            pltpu.VMEM((Z, 16, 4 * L), BF16),
            pltpu.VMEM((PL, DT, B), BF16),
            pltpu.VMEM((PL, DT, B), BF16),
            pltpu.SemaphoreType.DMA((16,)),
            pltpu.SemaphoreType.DMA((16,)),
            pltpu.SemaphoreType.DMA((16,)),
        ],
        compiler_params=pltpu.CompilerParams(collective_id=0, has_side_effects=True),
    )(
        stream,
        attn_gain.reshape(1, L),
        mixer_gain.reshape(1, L),
        head_gain.reshape(1, L),
        beta_weight,
        decay_weight,
        decay_log,
        decay_shift,
        memory_state,
        query_weight,
        key_weight,
        value_weight,
        outgate_weight,
        output_weight,
        up_weight,
        down_weight,
    )
    return layer_out, memory_next


def solution(mesh):
    in_specs = (
        P(None, ("kv", "tp")),
        P("kv", "tp", None, None),
        P("kv"),
        P("kv", "tp"),
        P("kv", "tp"),
        P("kv", "tp"),
        P("kv", "tp"),
        P("kv", "tp"),
        P("kv", "tp"),
        P("tp"),
        P("tp"),
        P(),
        P("tp", "kv"),
        P("kv"),
        P("kv", "tp"),
        P("tp", "kv"),
    )
    out_specs = (P(None, ("kv", "tp")), P("kv", "tp", None, None))
    body = functools.partial(shards, mesh.shape["kv"] // Y, mesh.shape["tp"])
    return jax.shard_map(body, mesh=mesh, in_specs=in_specs, out_specs=out_specs, check_vma=False)
```

```python
import functools

import jax
import jax.numpy as jnp
from jax import lax
from jax.experimental import pallas as pl
from jax.experimental.pallas import tpu as pltpu
from jax.sharding import PartitionSpec as P

MESH = pl.DeviceIdType.MESH
F32 = jnp.float32
BF16 = jnp.bfloat16
EPS = 1e-06
Y = 4
L = 128
HEADS_DEV = 4
ROWS = 4


def transposed(x):
    return jnp.transpose(x, (1, 0))


def silu(x):
    return x * jax.nn.sigmoid(x)


def softplus(x):
    return jnp.maximum(x, 0.0) + jnp.log1p(jnp.exp(-jnp.abs(x)))


def layer_kernel(
    Z,
    T,
    stream_hbm,
    attn_gain_hbm,
    mixer_gain_hbm,
    head_gain_hbm,
    beta_hbm,
    decay_hbm,
    decay_log_hbm,
    decay_shift_hbm,
    state_ref,
    wq_ref,
    wk_ref,
    wv_ref,
    wg_ref,
    wo_ref,
    wu_ref,
    wd_ref,
    out_ref,
    next_ref,
    stream_ref,
    attn_gain_ref,
    mixer_gain_ref,
    head_gain_ref,
    beta_ref,
    decay_ref,
    decay_log_ref,
    decay_shift_ref,
    state,
    state_out,
    w_in,
    wo,
    gains,
    etile,
    sgath,
    w1,
    xz,
    s2,
    r2,
    rows_f,
    hall,
    a4,
    r4,
    mgath,
    wu,
    wd,
    sq,
    u6,
    r6,
    hall7,
    d8,
    r8,
    layer,
    lsem,
    ssem,
    rsem,
):
    N = Z * Y
    PL = Y * T
    B = N * ROWS
    DT = L // T
    D = N * L
    kv = lax.axis_index("kv")
    tp = lax.axis_index("tp")
    z = lax.div(kv, Y)
    y = lax.rem(kv, Y)
    me_p = y * T + tp

    def plane_dev(p):
        return (z * Y + lax.div(p, T), lax.rem(p, T))

    def kv_dev(p):
        return (p, tp)

    def each_peer(n, me, act):
        def step(i, c):
            off = 1 + lax.rem(i + (n // 2 - 1), n - 1)
            act(lax.rem(me + off, n))
            return c

        lax.fori_loop(0, n - 1, step, 0)

    def put(src, dst, k, dev):
        pltpu.make_async_remote_copy(
            src_ref=src,
            dst_ref=dst,
            send_sem=ssem.at[k],
            recv_sem=rsem.at[k],
            device_id=dev,
            device_id_type=MESH,
        ).start()

    def got(ref, k):
        with jax.named_scope(f"got{k}"):
            pltpu.make_async_copy(ref, ref, rsem.at[k]).wait()

    def sent(ref, k):
        pltpu.make_async_copy(ref, ref, ssem.at[k]).wait()

    barrier = pltpu.get_barrier_semaphore()

    def greet(dev):
        pl.semaphore_signal(barrier, inc=1, device_id=dev, device_id_type=MESH)

    each_peer(N, kv, lambda p: greet(kv_dev(p)))

    def greet_plane(p):
        @pl.when(lax.rem(p, T) != tp)
        def _():
            greet(plane_dev(p))

    each_peer(PL, me_p, greet_plane)

    loads = [
        pltpu.make_async_copy(w, w_in.at[m], lsem.at[m])
        for m, w in enumerate((wq_ref, wk_ref, wv_ref, wg_ref))
    ]
    small = [
        pltpu.make_async_copy(a, b, lsem.at[16 + i])
        for i, (a, b) in enumerate((
            (stream_hbm, stream_ref),
            (attn_gain_hbm, attn_gain_ref),
            (mixer_gain_hbm, mixer_gain_ref),
            (beta_hbm, beta_ref),
            (decay_hbm, decay_ref),
        ))
    ]
    late = [
        pltpu.make_async_copy(a, b, lsem.at[21 + i])
        for i, (a, b) in enumerate((
            (head_gain_hbm, head_gain_ref),
            (decay_log_hbm, decay_log_ref),
            (decay_shift_hbm, decay_shift_ref),
        ))
    ]
    for c in small:
        c.start()
    load_out = pltpu.make_async_copy(wo_ref, wo, lsem.at[4])
    load_state = pltpu.make_async_copy(state_ref, state, lsem.at[5])
    for c in loads:
        c.start()
    load_out.start()
    load_state.start()
    for c in late:
        c.start()

    for c in small:
        c.wait()
    gains[y] = jnp.broadcast_to(attn_gain_ref[...], (8, L))
    gains[y, 1:2, :] = mixer_gain_ref[...]
    etile[y] = jnp.concatenate(
        [beta_ref[...].astype(F32), decay_ref[...].astype(F32), jnp.zeros((8, L), F32)], axis=0
    ).astype(BF16)
    own_stream = stream_ref[...].astype(F32)
    sgath[me_p] = stream_ref[...]

    with jax.named_scope("greeted"):
        pl.semaphore_wait(barrier, (N - 1) + (PL - 1) - (Y - 1))

    each_peer(PL, me_p, lambda p: put(sgath.at[me_p], sgath.at[me_p], 0, plane_dev(p)))
    for off in (2, 1, 3):
        yy = lax.rem(y + off, Y)
        put(gains.at[y], gains.at[y], 1, (z * Y + yy, tp))
        put(etile.at[y], etile.at[y], 2, (z * Y + yy, tp))
    for c in loads:
        c.wait()

    def head_cols(m, yy):
        return w_in.at[m, :, pl.ds(pl.multiple_of(yy * L, L), L)]

    def w1_cols(m):
        return w1.at[y, :, pl.ds(m * L, L)]

    own_w1 = [pltpu.make_async_copy(head_cols(m, y), w1_cols(m), lsem.at[6 + m]) for m in range(4)]
    for m in range(4):
        for off in (2, 1, 3):
            yy = lax.rem(y + off, Y)
            put(head_cols(m, yy), w1_cols(m), 3, (z * Y + yy, tp))
        own_w1[m].start()

    got(sgath.at[pl.ds(0, PL - 1)], 0)
    got(gains.at[pl.ds(0, Y - 1)], 1)
    got(etile.at[pl.ds(0, Y - 1)], 2)
    scaled = []
    x_part = jnp.zeros((16, B), F32)
    squares = jnp.zeros((1, B), F32)
    for j in range(Y):
        block = sgath[j * T : (j + 1) * T].astype(F32).reshape(L, B)
        squares = squares + jnp.sum(block * block, axis=0, keepdims=True)
        part = (transposed(block) * gains[j, 0:1, :]).astype(BF16)
        scaled.append(part)
        x_part = x_part + lax.dot_general(
            etile[j], part, (((1,), (1,)), ((), ())), preferred_element_type=F32
        )
    row16 = lax.broadcasted_iota(jnp.int32, (16, B), 0)
    xz[z] = jnp.where(row16 == 8, squares, x_part)
    for off in (4, 3, 5, 2, 6, 1, 7):
        if off < Z:
            zz = lax.rem(z + off, Z)
            put(xz.at[z], xz.at[z], 4, (zz * Y + y, tp))

    for c in own_w1:
        c.wait()
    got(w1.at[pl.ds(0, Y - 1)], 3)
    proj = jnp.zeros((B, 4 * L), F32)
    for j in range(Y):
        proj = proj + jnp.dot(scaled[j], w1[j], preferred_element_type=F32)
    low = lax.broadcasted_iota(jnp.int32, (B // 8, 8, L), 1) < 4

    def pair_tiles(a, b):
        return (
            jnp.where(low, a, pltpu.roll(b, 4, 1)),
            jnp.where(low, pltpu.roll(a, 4, 1), b),
        )

    pq, pk, pv, pg = [proj[:, m * L : (m + 1) * L].reshape(B // 8, 8, L) for m in range(4)]
    even_a, odd_a = pair_tiles(pq, pk)
    even_b, odd_b = pair_tiles(pv, pg)
    s2[:, 0] = jnp.concatenate([even_a, even_b], axis=1).astype(BF16)
    s2[:, 1] = jnp.concatenate([odd_a, odd_b], axis=1).astype(BF16)
    each_peer(
        N, kv, lambda p: put(s2.at[lax.div(p, 2), lax.rem(p, 2)], r2.at[kv], 5, kv_dev(p))
    )
    r2[kv] = s2[lax.div(kv, 2), lax.rem(kv, 2)]

    def up_cols(yy):
        return wu_ref.at[:, pl.ds(pl.multiple_of(yy * 4 * L, L), 4 * L)]

    own_up = pltpu.make_async_copy(up_cols(y), wu.at[y], lsem.at[10])
    own_up.start()
    for off in (2, 1, 3):
        yy = lax.rem(y + off, Y)
        put(up_cols(yy), wu.at[y], 6, (z * Y + yy, tp))

    for c in late:
        c.wait()
    got(xz.at[pl.ds(0, Z - 1)], 4)
    x_all = xz[0]
    for j in range(1, Z):
        x_all = x_all + xz[j]
    fac = lax.rsqrt(x_all[8:9] / D + EPS)
    xf = x_all * fac
    dlog = jnp.zeros((16, B), F32)
    dshift = jnp.zeros((16, B), F32)
    for h in range(HEADS_DEV):
        dlog = jnp.where(row16 == 4 + h, decay_log_ref[h], dlog)
        dshift = jnp.where(row16 == 4 + h, decay_shift_ref[h], dshift)
    scal = jnp.where(
        row16 < 4,
        jax.nn.sigmoid(xf),
        jnp.where(row16 < 8, jnp.exp(-jnp.exp(dlog) * softplus(xf + dshift)), fac),
    )
    lane_group = lax.div(lax.broadcasted_iota(jnp.int32, (16, B), 1), 4)
    mine = jnp.zeros((16, B), F32)
    for m in range(4):
        rolled = pltpu.roll(scal, lax.rem(B + m * ROWS - kv * ROWS, B), 1)
        mine = jnp.where(lane_group == m, rolled, mine)
    cols = transposed(jnp.concatenate([mine, jnp.zeros((L - 16, B), F32)], axis=0))[0:16]

    got(r2.at[pl.ds(0, N - 1)], 5)
    load_state.wait()
    row_id = lax.broadcasted_iota(jnp.int32, (16, 1), 0)
    acts = []
    for h in range(HEADS_DEV):
        total = r2[h].astype(F32)
        for j in range(1, Z):
            total = total + r2[j * Y + h].astype(F32)
        a = silu(total * cols[:, 8:9])
        inv = lax.rsqrt(jnp.sum(a * a, axis=1, keepdims=True) + EPS)
        norm = jnp.where(row_id < 4, inv * L ** (-0.5), jnp.where(row_id < 8, inv, 1.0))
        acts.append(a * norm)
        rows_f[1, 4 * h : 4 * h + 4, :] = a[12:16]
    flipped = transposed(jnp.concatenate(acts + [jnp.zeros((L - 64, L), F32)], axis=0))
    for h in range(HEADS_DEV):
        for r in range(ROWS):
            q_col = flipped[:, h * 16 + r : h * 16 + r + 1]
            k_col = flipped[:, h * 16 + 4 + r : h * 16 + 5 + r]
            kept = state[r, h] * cols[r : r + 1, 4 + h : 5 + h]
            recalled = jnp.sum(kept * k_col, axis=0, keepdims=True)
            corr = cols[r : r + 1, h : h + 1] * (acts[h][8 + r : 9 + r] - recalled)
            new = kept + k_col * corr
            state_out[r, h] = new
            rows_f[0, 4 * h + r : 4 * h + r + 1, :] = jnp.sum(new * q_col, axis=0, keepdims=True)
    readout = rows_f[0]
    readout = readout * lax.rsqrt(jnp.mean(readout * readout, axis=1, keepdims=True) + EPS)
    hall[kv] = (readout * head_gain_ref[...] * rows_f[1]).astype(BF16)

    each_peer(N, kv, lambda p: put(hall.at[kv], hall.at[kv], 7, kv_dev(p)))
    store_state = pltpu.make_async_copy(state_out, next_ref, lsem.at[11])
    store_state.start()

    def down_rows(yy):
        return wd_ref.at[pl.ds(pl.multiple_of(yy * 4 * L, L), 4 * L), :]

    own_down = pltpu.make_async_copy(down_rows(y), wd.at[y], lsem.at[12])
    own_down.start()
    for off in (2, 1, 3):
        yy = lax.rem(y + off, Y)
        put(down_rows(yy), wd.at[y], 8, (z * Y + yy, tp))

    load_out.wait()
    got(hall.at[pl.ds(0, N - 1)], 7)
    heads = hall[...].astype(F32).reshape(N // 2, 2, 2, 8, L)
    attn = jnp.zeros((B, L), F32)
    for c in range(2):
        h_even, h_odd = pair_tiles(heads[:, 0, c], heads[:, 1, c])
        for i, hh in ((2 * c, h_even), (2 * c + 1, h_odd)):
            attn = attn + jnp.dot(
                hh.reshape(B, L).astype(BF16),
                wo[i * L : (i + 1) * L, :],
                preferred_element_type=F32,
            )
    a4[...] = transposed(attn).reshape(T, DT, B).astype(BF16)
    each_peer(T, tp, lambda p: put(a4.at[p], r4.at[tp], 9, (kv, p)))
    r4[tp] = a4[tp]
    got(r4.at[pl.ds(0, T - 1)], 9)
    attn_mine = r4[0].astype(F32)
    for j in range(1, T):
        attn_mine = attn_mine + r4[j].astype(F32)
    middle = (own_stream + attn_mine).astype(BF16)

    mgath[me_p] = middle
    each_peer(PL, me_p, lambda p: put(mgath.at[me_p], mgath.at[me_p], 10, plane_dev(p)))
    own_up.wait()
    got(wu.at[pl.ds(0, Y - 1)], 6)
    got(mgath.at[pl.ds(0, PL - 1)], 10)
    up = jnp.zeros((B, 4 * L), F32)
    squares2 = jnp.zeros((1, B), F32)
    for j in range(Y):
        block = mgath[j * T : (j + 1) * T].astype(F32).reshape(L, B)
        squares2 = squares2 + jnp.sum(block * block, axis=0, keepdims=True)
        part = (transposed(block) * gains[j, 1:2, :]).astype(BF16)
        up = up + jnp.dot(part, wu[j], preferred_element_type=F32)
    u6[...] = up.astype(BF16).reshape(Z, 16, 4 * L)
    sq[z] = jnp.broadcast_to(squares2, (8, B))
    offs = [o for o in (4, 3, 5, 2, 6, 1, 7) if o < Z]
    for off in offs:
        zz = lax.rem(z + off, Z)
        put(u6.at[zz], r6.at[z], 11, (zz * Y + y, tp))
    for off in offs:
        zz = lax.rem(z + off, Z)
        put(sq.at[z], sq.at[z], 12, (zz * Y + y, tp))
    r6[z] = u6[z]
    got(r6.at[pl.ds(0, Z - 1)], 11)
    up_mine = r6[0].astype(F32)
    for j in range(1, Z):
        up_mine = up_mine + r6[j].astype(F32)
    hidden = jnp.square(jnp.maximum(up_mine, 0.0)).astype(BF16)
    hall7[z] = hidden
    for off in offs:
        zz = lax.rem(z + off, Z)
        put(hall7.at[z], hall7.at[z], 13, (zz * Y + y, tp))
    own_down.wait()
    got(wd.at[pl.ds(0, Y - 1)], 8)
    got(hall7.at[pl.ds(0, Z - 1)], 13)
    hid = hall7[...].reshape(B, 4 * L)
    for j in range(Y):
        part = jnp.dot(hid, wd[j], preferred_element_type=F32)
        d8[j * T : (j + 1) * T] = transposed(part).reshape(T, DT, B).astype(BF16)
    each_peer(PL, me_p, lambda p: put(d8.at[p], r8.at[me_p], 14, plane_dev(p)))
    r8[me_p] = d8[me_p]
    got(sq.at[pl.ds(0, Z - 1)], 12)
    total2 = sq[0, 0:1, :]
    for j in range(1, Z):
        total2 = total2 + sq[j, 0:1, :]
    factor2 = lax.rsqrt(total2 / D + EPS)
    got(r8.at[pl.ds(0, PL - 1)], 14)
    parts = [r8[j].astype(F32) for j in range(4)]
    for j in range(4, PL):
        parts[j % 4] = parts[j % 4] + r8[j].astype(F32)
    mixed = (parts[0] + parts[1]) + (parts[2] + parts[3])
    final = middle.astype(F32) + mixed * (factor2 * factor2)
    layer[...] = final.astype(BF16)
    store_layer = pltpu.make_async_copy(layer, out_ref, lsem.at[15])
    store_layer.start()

    sent(sgath.at[pl.ds(0, PL - 1)], 0)
    sent(gains.at[pl.ds(0, Y - 1)], 1)
    sent(etile.at[pl.ds(0, Y - 1)], 2)
    sent(w1.at[pl.ds(0, Y - 1)], 3)
    sent(xz.at[pl.ds(0, Z - 1)], 4)
    sent(r2.at[pl.ds(0, N - 1)], 5)
    sent(wu.at[pl.ds(0, Y - 1)], 6)
    sent(hall.at[pl.ds(0, N - 1)], 7)
    sent(wd.at[pl.ds(0, Y - 1)], 8)
    sent(r4.at[pl.ds(0, T - 1)], 9)
    sent(mgath.at[pl.ds(0, PL - 1)], 10)
    sent(r6.at[pl.ds(0, Z - 1)], 11)
    sent(sq.at[pl.ds(0, Z - 1)], 12)
    sent(hall7.at[pl.ds(0, Z - 1)], 13)
    sent(r8.at[pl.ds(0, PL - 1)], 14)
    store_state.wait()
    store_layer.wait()


def hand_over(layer_in, state_in, layer_ref, state_ref, sems):
    copies = [
        pltpu.make_async_copy(state_in, state_ref, sems.at[0]),
        pltpu.make_async_copy(layer_in, layer_ref, sems.at[1]),
    ]
    for c in copies:
        c.start()
    for c in copies:
        c.wait()


def shards(
    Z,
    T,
    stream,
    memory_state,
    attn_gain,
    query_weight,
    key_weight,
    value_weight,
    outgate_weight,
    beta_weight,
    decay_weight,
    decay_log,
    decay_shift,
    head_gain,
    output_weight,
    mixer_gain,
    up_weight,
    down_weight,
):
    N, PL, B, DT = Z * Y, Y * T, Z * Y * ROWS, L // T
    hbm = pl.BlockSpec(memory_space=pltpu.HBM)
    anywhere = pl.BlockSpec(memory_space=pl.ANY)
    layer_out, memory_next = pl.pallas_call(
        functools.partial(layer_kernel, Z, T),
        out_shape=(
            pltpu.VMEM((DT, B), BF16),
            pltpu.VMEM(memory_state.shape, F32),
        ),
        in_specs=[hbm] * 16,
        out_specs=(anywhere, anywhere),
        scratch_shapes=[
            pltpu.VMEM((DT, B), BF16),
            pltpu.VMEM((1, L), F32),
            pltpu.VMEM((1, L), F32),
            pltpu.VMEM((1, L), F32),
            pltpu.VMEM((HEADS_DEV, L), BF16),
            pltpu.VMEM((HEADS_DEV, L), BF16),
            pltpu.SMEM((HEADS_DEV,), F32),
            pltpu.SMEM((HEADS_DEV,), F32),
            pltpu.VMEM((ROWS, HEADS_DEV, L, L), F32),
            pltpu.VMEM((ROWS, HEADS_DEV, L, L), F32),
            pltpu.VMEM((4, L, 4 * L), BF16),
            pltpu.VMEM((4 * L, L), BF16),
            pltpu.VMEM((Y, 8, L), F32),
            pltpu.VMEM((Y, 16, L), BF16),
            pltpu.VMEM((PL, DT, B), BF16),
            pltpu.VMEM((Y, L, 4 * L), BF16),
            pltpu.VMEM((Z, 16, B), F32),
            pltpu.VMEM((N // 2, 2, 16, L), BF16),
            pltpu.VMEM((N, 16, L), BF16),
            pltpu.VMEM((2, 16, L), F32),
            pltpu.VMEM((N, 16, L), BF16),
            pltpu.VMEM((T, DT, B), BF16),
            pltpu.VMEM((T, DT, B), BF16),
            pltpu.VMEM((PL, DT, B), BF16),
            pltpu.VMEM((Y, L, 4 * L), BF16),
            pltpu.VMEM((Y, 4 * L, L), BF16),
            pltpu.VMEM((Z, 8, B), F32),
            pltpu.VMEM((Z, 16, 4 * L), BF16),
            pltpu.VMEM((Z, 16, 4 * L), BF16),
            pltpu.VMEM((Z, 16, 4 * L), BF16),
            pltpu.VMEM((PL, DT, B), BF16),
            pltpu.VMEM((PL, DT, B), BF16),
            pltpu.VMEM((DT, B), BF16),
            pltpu.SemaphoreType.DMA((24,)),
            pltpu.SemaphoreType.DMA((16,)),
            pltpu.SemaphoreType.DMA((16,)),
        ],
        compiler_params=pltpu.CompilerParams(
            collective_id=0,
            has_side_effects=True,
            vmem_limit_bytes=67043328 - memory_state.size * 4 - 8192,
        ),
    )(
        stream.T,
        attn_gain.reshape(1, L),
        mixer_gain.reshape(1, L),
        head_gain.reshape(1, L),
        beta_weight.T,
        decay_weight.T,
        decay_log,
        decay_shift,
        memory_state,
        query_weight,
        key_weight,
        value_weight,
        outgate_weight,
        output_weight,
        up_weight,
        down_weight,
    )
    layer_out, memory_next = pl.pallas_call(
        hand_over,
        out_shape=(
            jax.ShapeDtypeStruct((DT, B), BF16),
            jax.ShapeDtypeStruct(memory_state.shape, F32),
        ),
        in_specs=[anywhere] * 2,
        out_specs=(hbm, hbm),
        scratch_shapes=[pltpu.SemaphoreType.DMA((2,))],
        compiler_params=pltpu.CompilerParams(vmem_limit_bytes=2**20),
    )(layer_out, memory_next)
    return layer_out.T, memory_next


def solution(mesh):
    in_specs = (
        P(None, ("kv", "tp")),
        P("kv", "tp", None, None),
        P("kv"),
        P("kv", "tp"),
        P("kv", "tp"),
        P("kv", "tp"),
        P("kv", "tp"),
        P("kv", "tp"),
        P("kv", "tp"),
        P("tp"),
        P("tp"),
        P(),
        P("tp", "kv"),
        P("kv"),
        P("kv", "tp"),
        P("tp", "kv"),
    )
    out_specs = (P(None, ("kv", "tp")), P("kv", "tp", None, None))
    body = functools.partial(shards, mesh.shape["kv"] // Y, mesh.shape["tp"])
    return jax.shard_map(body, mesh=mesh, in_specs=in_specs, out_specs=out_specs, check_vma=False)
```

```python
import functools

import jax
import jax.numpy as jnp
from jax import lax
from jax.experimental import pallas as pl
from jax.experimental.pallas import tpu as pltpu
from jax.sharding import PartitionSpec as P

MESH = pl.DeviceIdType.MESH
F32 = jnp.float32
BF16 = jnp.bfloat16
EPS = 1e-06
Y = 4
L = 128
HEADS_DEV = 4
ROWS = 4


def transposed(x):
    return jnp.transpose(x, (1, 0))


def silu(x):
    return x * jax.nn.sigmoid(x)


def softplus(x):
    return jnp.maximum(x, 0.0) + jnp.log1p(jnp.exp(-jnp.abs(x)))


def layer_kernel(
    Z,
    T,
    stream_hbm,
    attn_gain_hbm,
    mixer_gain_hbm,
    head_gain_hbm,
    beta_hbm,
    decay_hbm,
    decay_log_hbm,
    decay_shift_hbm,
    state_ref,
    wq_ref,
    wk_ref,
    wv_ref,
    wg_ref,
    wo_ref,
    wu_ref,
    wd_ref,
    out_ref,
    next_ref,
    stream_ref,
    attn_gain_ref,
    mixer_gain_ref,
    head_gain_ref,
    beta_ref,
    decay_ref,
    decay_log_ref,
    decay_shift_ref,
    state,
    w_in,
    wo,
    gains,
    etile,
    sgath,
    w1,
    xz,
    s2,
    r2,
    rows_f,
    hall,
    a4,
    r4,
    mgath,
    wu,
    wd,
    sq,
    u6,
    r6,
    hall7,
    d8,
    r8,
    wot,
    wut,
    wdt,
    gcol,
    lsem,
    ssem,
    rsem,
):
    N = Z * Y
    PL = Y * T
    B = N * ROWS
    DT = L // T
    D = N * L
    kv = lax.axis_index("kv")
    tp = lax.axis_index("tp")
    z = lax.div(kv, Y)
    y = lax.rem(kv, Y)
    me_p = y * T + tp

    def plane_dev(p):
        return (z * Y + lax.div(p, T), lax.rem(p, T))

    def kv_dev(p):
        return (p, tp)

    def each_peer(n, me, act):
        def step(i, c):
            off = 1 + lax.rem(i + (n // 2 - 1), n - 1)
            act(lax.rem(me + off, n))
            return c

        lax.fori_loop(0, n - 1, step, 0)

    def put(src, dst, k, dev):
        pltpu.make_async_remote_copy(
            src_ref=src,
            dst_ref=dst,
            send_sem=ssem.at[k],
            recv_sem=rsem.at[k],
            device_id=dev,
            device_id_type=MESH,
        ).start()

    def got(ref, k):
        with jax.named_scope(f"got{k}"):
            pltpu.make_async_copy(ref, ref, rsem.at[k]).wait()

    def sent(ref, k):
        pltpu.make_async_copy(ref, ref, ssem.at[k]).wait()

    loads = [
        pltpu.make_async_copy(w, w_in.at[m], lsem.at[m])
        for m, w in enumerate((wq_ref, wk_ref, wv_ref, wg_ref))
    ]
    small = [
        pltpu.make_async_copy(a, b, lsem.at[16 + i])
        for i, (a, b) in enumerate((
            (stream_hbm, stream_ref),
            (attn_gain_hbm, attn_gain_ref),
            (mixer_gain_hbm, mixer_gain_ref),
            (beta_hbm, beta_ref),
            (decay_hbm, decay_ref),
        ))
    ]
    late = [
        pltpu.make_async_copy(a, b, lsem.at[21 + i])
        for i, (a, b) in enumerate((
            (head_gain_hbm, head_gain_ref),
            (decay_log_hbm, decay_log_ref),
            (decay_shift_hbm, decay_shift_ref),
        ))
    ]
    for c in small:
        c.start()
    load_out = pltpu.make_async_copy(wo_ref, wo, lsem.at[4])
    load_state = pltpu.make_async_copy(state_ref, state, lsem.at[5])
    for c in loads:
        c.start()
    load_out.start()
    load_state.start()
    for c in late:
        c.start()

    barrier = pltpu.get_barrier_semaphore()

    def greet(dev):
        pl.semaphore_signal(barrier, inc=1, device_id=dev, device_id_type=MESH)

    with jax.named_scope("greet"):
        for off in (4, 3, 5, 2, 6, 1, 7):
            if off < Z:
                greet((lax.rem(z + off, Z) * Y + y, tp))
        each_peer(PL, me_p, lambda p: greet(plane_dev(p)))

    for c in small:
        c.wait()
    gains[y] = jnp.broadcast_to(attn_gain_ref[...], (8, L))
    gains[y, 1:2, :] = mixer_gain_ref[...]
    etile[y] = jnp.concatenate(
        [beta_ref[...].astype(F32), decay_ref[...].astype(F32), jnp.zeros((8, L), F32)], axis=0
    ).astype(BF16)
    own_stream = stream_ref[...].astype(F32)
    sgath[me_p] = stream_ref[...]

    with jax.named_scope("greeted"):
        pl.semaphore_wait(barrier, (Z - 1) + (PL - 1))

    each_peer(PL, me_p, lambda p: put(sgath.at[me_p], sgath.at[me_p], 0, plane_dev(p)))
    for off in (2, 1, 3):
        yy = lax.rem(y + off, Y)
        put(gains.at[y], gains.at[y], 1, (z * Y + yy, tp))
        put(etile.at[y], etile.at[y], 2, (z * Y + yy, tp))
    for c in loads:
        c.wait()

    def head_cols(m, yy):
        return w_in.at[m, :, pl.ds(pl.multiple_of(yy * L, L), L)]

    def w1_cols(m):
        return w1.at[y, :, pl.ds(m * L, L)]

    own_w1 = [pltpu.make_async_copy(head_cols(m, y), w1_cols(m), lsem.at[6 + m]) for m in range(4)]
    for m in range(4):
        for off in (2, 1, 3):
            yy = lax.rem(y + off, Y)
            put(head_cols(m, yy), w1_cols(m), 3, (z * Y + yy, tp))
        own_w1[m].start()

    got(sgath.at[pl.ds(0, PL - 1)], 0)
    got(gains.at[pl.ds(0, Y - 1)], 1)
    got(etile.at[pl.ds(0, Y - 1)], 2)
    scaled = []
    x_part = jnp.zeros((16, B), F32)
    squares = jnp.zeros((1, B), F32)
    for j in range(Y):
        block = sgath[j * T : (j + 1) * T].astype(F32).reshape(L, B)
        squares = squares + jnp.sum(block * block, axis=0, keepdims=True)
        part = (transposed(block) * gains[j, 0:1, :]).astype(BF16)
        scaled.append(part)
        x_part = x_part + lax.dot_general(
            etile[j], part, (((1,), (1,)), ((), ())), preferred_element_type=F32
        )
    row16 = lax.broadcasted_iota(jnp.int32, (16, B), 0)
    xz[z] = jnp.where(row16 == 8, squares, x_part)
    for off in (4, 3, 5, 2, 6, 1, 7):
        if off < Z:
            zz = lax.rem(z + off, Z)
            put(xz.at[z], xz.at[z], 4, (zz * Y + y, tp))

    for c in own_w1:
        c.wait()
    got(w1.at[pl.ds(0, Y - 1)], 3)
    proj = jnp.zeros((B, 4 * L), F32)
    for j in range(Y):
        proj = proj + jnp.dot(scaled[j], w1[j], preferred_element_type=F32)
    low = lax.broadcasted_iota(jnp.int32, (B // 8, 8, L), 1) < 4

    def pair_tiles(a, b):
        return (
            jnp.where(low, a, pltpu.roll(b, 4, 1)),
            jnp.where(low, pltpu.roll(a, 4, 1), b),
        )

    pq, pk, pv, pg = [proj[:, m * L : (m + 1) * L].reshape(B // 8, 8, L) for m in range(4)]
    even_a, odd_a = pair_tiles(pq, pk)
    even_b, odd_b = pair_tiles(pv, pg)
    s2[:, 0] = jnp.concatenate([even_a, even_b], axis=1).astype(BF16)
    s2[:, 1] = jnp.concatenate([odd_a, odd_b], axis=1).astype(BF16)
    each_peer(
        N, kv, lambda p: put(s2.at[lax.div(p, 2), lax.rem(p, 2)], r2.at[kv], 5, kv_dev(p))
    )
    r2[kv] = s2[lax.div(kv, 2), lax.rem(kv, 2)]

    def up_cols(yy):
        return wu_ref.at[:, pl.ds(pl.multiple_of(yy * 4 * L, L), 4 * L)]

    own_up = pltpu.make_async_copy(up_cols(y), wu.at[y], lsem.at[10])
    own_up.start()
    for off in (2, 1, 3):
        yy = lax.rem(y + off, Y)
        put(up_cols(yy), wu.at[y], 6, (z * Y + yy, tp))

    for c in late:
        c.wait()
    got(xz.at[pl.ds(0, Z - 1)], 4)
    x_all = xz[0]
    for j in range(1, Z):
        x_all = x_all + xz[j]
    fac = lax.rsqrt(x_all[8:9] / D + EPS)
    xf = x_all * fac
    dlog = jnp.zeros((16, B), F32)
    dshift = jnp.zeros((16, B), F32)
    for h in range(HEADS_DEV):
        dlog = jnp.where(row16 == 4 + h, decay_log_ref[h], dlog)
        dshift = jnp.where(row16 == 4 + h, decay_shift_ref[h], dshift)
    scal = jnp.where(
        row16 < 4,
        jax.nn.sigmoid(xf),
        jnp.where(row16 < 8, jnp.exp(-jnp.exp(dlog) * softplus(xf + dshift)), fac),
    )
    lane_group = lax.div(lax.broadcasted_iota(jnp.int32, (16, B), 1), 4)
    mine = jnp.zeros((16, B), F32)
    for m in range(4):
        rolled = pltpu.roll(scal, lax.rem(B + m * ROWS - kv * ROWS, B), 1)
        mine = jnp.where(lane_group == m, rolled, mine)
    cols = transposed(jnp.concatenate([mine, jnp.zeros((L - 16, B), F32)], axis=0))[0:16]

    got(r2.at[pl.ds(0, N - 1)], 5)
    load_state.wait()
    row_id = lax.broadcasted_iota(jnp.int32, (16, 1), 0)
    acts = []
    for h in range(HEADS_DEV):
        total = r2[h].astype(F32)
        for j in range(1, Z):
            total = total + r2[j * Y + h].astype(F32)
        a = silu(total * cols[:, 8:9])
        inv = lax.rsqrt(jnp.sum(a * a, axis=1, keepdims=True) + EPS)
        norm = jnp.where(row_id < 4, inv * L ** (-0.5), jnp.where(row_id < 8, inv, 1.0))
        acts.append(a * norm)
        rows_f[1, 4 * h : 4 * h + 4, :] = a[12:16]
    flipped = transposed(jnp.concatenate(acts + [jnp.zeros((L - 64, L), F32)], axis=0))
    for h in range(HEADS_DEV):
        for r in range(ROWS):
            q_col = flipped[:, h * 16 + r : h * 16 + r + 1]
            k_col = flipped[:, h * 16 + 4 + r : h * 16 + 5 + r]
            kept = state[r, h] * cols[r : r + 1, 4 + h : 5 + h]
            recalled = jnp.sum(kept * k_col, axis=0, keepdims=True)
            corr = cols[r : r + 1, h : h + 1] * (acts[h][8 + r : 9 + r] - recalled)
            new = kept + k_col * corr
            next_ref[r, h] = new
            rows_f[0, 4 * h + r : 4 * h + r + 1, :] = jnp.sum(new * q_col, axis=0, keepdims=True)
    readout = rows_f[0]
    readout = readout * lax.rsqrt(jnp.mean(readout * readout, axis=1, keepdims=True) + EPS)
    hall[kv] = (readout * head_gain_ref[...] * rows_f[1]).astype(BF16)

    each_peer(N, kv, lambda p: put(hall.at[kv], hall.at[kv], 7, kv_dev(p)))

    def down_rows(yy):
        return wd_ref.at[pl.ds(pl.multiple_of(yy * 4 * L, L), 4 * L), :]

    own_down = pltpu.make_async_copy(down_rows(y), wd.at[y], lsem.at[12])
    own_down.start()
    for off in (2, 1, 3):
        yy = lax.rem(y + off, Y)
        put(down_rows(yy), wd.at[y], 8, (z * Y + yy, tp))

    load_out.wait()
    for i in range(HEADS_DEV):
        wot[:, i * L : (i + 1) * L] = transposed(wo[i * L : (i + 1) * L, :].astype(F32)).astype(BF16)
    own_up.wait()
    got(wu.at[pl.ds(0, Y - 1)], 6)
    for j in range(Y):
        for i in range(4):
            wut[i * L : (i + 1) * L, j * L : (j + 1) * L] = transposed(
                wu[j, :, i * L : (i + 1) * L].astype(F32)
            ).astype(BF16)
        gcol[j] = transposed(jnp.broadcast_to(gains[j, 1:2, :], (B, L)))
    got(hall.at[pl.ds(0, N - 1)], 7)
    heads = hall[...].astype(F32).reshape(N // 2, 2, 2, 8, L)
    attn = jnp.zeros((L, B), F32)
    for c in range(2):
        h_even, h_odd = pair_tiles(heads[:, 0, c], heads[:, 1, c])
        for i, hh in ((2 * c, h_even), (2 * c + 1, h_odd)):
            attn = attn + lax.dot_general(
                wot[:, i * L : (i + 1) * L],
                hh.reshape(B, L).astype(BF16),
                (((1,), (1,)), ((), ())),
                preferred_element_type=F32,
            )
    a4[...] = attn.reshape(T, DT, B).astype(BF16)
    each_peer(T, tp, lambda p: put(a4.at[p], r4.at[tp], 9, (kv, p)))
    r4[tp] = a4[tp]
    got(r4.at[pl.ds(0, T - 1)], 9)
    attn_mine = r4[0].astype(F32)
    for j in range(1, T):
        attn_mine = attn_mine + r4[j].astype(F32)
    middle = (own_stream + attn_mine).astype(BF16)

    mgath[me_p] = middle
    each_peer(PL, me_p, lambda p: put(mgath.at[me_p], mgath.at[me_p], 10, plane_dev(p)))
    got(mgath.at[pl.ds(0, PL - 1)], 10)
    up = jnp.zeros((4 * L, B), F32)
    squares2 = jnp.zeros((1, B), F32)
    for j in range(Y):
        block = mgath[j * T : (j + 1) * T].astype(F32).reshape(L, B)
        squares2 = squares2 + jnp.sum(block * block, axis=0, keepdims=True)
        part = (block * gcol[j]).astype(BF16)
        up = up + jnp.dot(wut[:, j * L : (j + 1) * L], part, preferred_element_type=F32)
    u6[...] = up.astype(BF16).reshape(Z, 4 * L // Z, B)
    sq[z] = jnp.broadcast_to(squares2, (8, B))
    offs = [o for o in (4, 3, 5, 2, 6, 1, 7) if o < Z]
    for off in offs:
        zz = lax.rem(z + off, Z)
        put(u6.at[zz], r6.at[z], 11, (zz * Y + y, tp))
    r6[z] = u6[z]
    own_down.wait()
    got(wd.at[pl.ds(0, Y - 1)], 8)
    for j in range(Y):
        for i in range(4):
            wdt[j * L : (j + 1) * L, i * L : (i + 1) * L] = transposed(
                wd[j, i * L : (i + 1) * L, :].astype(F32)
            ).astype(BF16)
    got(r6.at[pl.ds(0, Z - 1)], 11)
    up_mine = r6[0].astype(F32)
    for j in range(1, Z):
        up_mine = up_mine + r6[j].astype(F32)
    hidden = jnp.square(jnp.maximum(up_mine, 0.0)).astype(BF16)
    hall7[z] = hidden
    for off in offs:
        zz = lax.rem(z + off, Z)
        put(hall7.at[z], hall7.at[z], 13, (zz * Y + y, tp))
    for off in offs:
        zz = lax.rem(z + off, Z)
        put(sq.at[z], sq.at[z], 12, (zz * Y + y, tp))
    got(hall7.at[pl.ds(0, Z - 1)], 13)
    down = jnp.dot(wdt[...], hall7[...].reshape(4 * L, B), preferred_element_type=F32)
    d8[...] = down.reshape(PL, DT, B).astype(BF16)
    each_peer(PL, me_p, lambda p: put(d8.at[p], r8.at[me_p], 14, plane_dev(p)))
    r8[me_p] = d8[me_p]
    got(sq.at[pl.ds(0, Z - 1)], 12)
    total2 = sq[0, 0:1, :]
    for j in range(1, Z):
        total2 = total2 + sq[j, 0:1, :]
    factor2 = lax.rsqrt(total2 / D + EPS)
    got(r8.at[pl.ds(0, PL - 1)], 14)
    parts = [r8[j].astype(F32) for j in range(4)]
    for j in range(4, PL):
        parts[j % 4] = parts[j % 4] + r8[j].astype(F32)
    mixed = (parts[0] + parts[1]) + (parts[2] + parts[3])
    final = middle.astype(F32) + mixed * (factor2 * factor2)
    out_ref[...] = final.astype(BF16)

    sent(sgath.at[pl.ds(0, PL - 1)], 0)
    sent(gains.at[pl.ds(0, Y - 1)], 1)
    sent(etile.at[pl.ds(0, Y - 1)], 2)
    sent(w1.at[pl.ds(0, Y - 1)], 3)
    sent(xz.at[pl.ds(0, Z - 1)], 4)
    sent(r2.at[pl.ds(0, N - 1)], 5)
    sent(wu.at[pl.ds(0, Y - 1)], 6)
    sent(hall.at[pl.ds(0, N - 1)], 7)
    sent(wd.at[pl.ds(0, Y - 1)], 8)
    sent(r4.at[pl.ds(0, T - 1)], 9)
    sent(mgath.at[pl.ds(0, PL - 1)], 10)
    sent(r6.at[pl.ds(0, Z - 1)], 11)
    sent(sq.at[pl.ds(0, Z - 1)], 12)
    sent(hall7.at[pl.ds(0, Z - 1)], 13)
    sent(r8.at[pl.ds(0, PL - 1)], 14)


def hand_over(layer_in, state_in, layer_ref, state_ref, sems):
    copies = [pltpu.make_async_copy(layer_in, layer_ref, sems.at[4])]
    for r in range(ROWS):
        copies.append(pltpu.make_async_copy(state_in.at[r], state_ref.at[r], sems.at[r]))
    for c in copies:
        c.start()
    for c in copies:
        c.wait()


def shards(
    Z,
    T,
    stream,
    memory_state,
    attn_gain,
    query_weight,
    key_weight,
    value_weight,
    outgate_weight,
    beta_weight,
    decay_weight,
    decay_log,
    decay_shift,
    head_gain,
    output_weight,
    mixer_gain,
    up_weight,
    down_weight,
):
    N, PL, B, DT = Z * Y, Y * T, Z * Y * ROWS, L // T
    hbm = pl.BlockSpec(memory_space=pltpu.HBM)
    anywhere = pl.BlockSpec(memory_space=pl.ANY)
    vmem = pl.BlockSpec(memory_space=pltpu.VMEM)
    layer_out, memory_next = pl.pallas_call(
        functools.partial(layer_kernel, Z, T),
        out_shape=(
            pltpu.VMEM((DT, B), BF16),
            pltpu.VMEM(memory_state.shape, F32),
        ),
        in_specs=[hbm] * 16,
        out_specs=(vmem, vmem),
        scratch_shapes=[
            pltpu.VMEM((DT, B), BF16),
            pltpu.VMEM((1, L), F32),
            pltpu.VMEM((1, L), F32),
            pltpu.VMEM((1, L), F32),
            pltpu.VMEM((HEADS_DEV, L), BF16),
            pltpu.VMEM((HEADS_DEV, L), BF16),
            pltpu.SMEM((HEADS_DEV,), F32),
            pltpu.SMEM((HEADS_DEV,), F32),
            pltpu.VMEM((ROWS, HEADS_DEV, L, L), F32),
            pltpu.VMEM((4, L, 4 * L), BF16),
            pltpu.VMEM((4 * L, L), BF16),
            pltpu.VMEM((Y, 8, L), F32),
            pltpu.VMEM((Y, 16, L), BF16),
            pltpu.VMEM((PL, DT, B), BF16),
            pltpu.VMEM((Y, L, 4 * L), BF16),
            pltpu.VMEM((Z, 16, B), F32),
            pltpu.VMEM((N // 2, 2, 16, L), BF16),
            pltpu.VMEM((N, 16, L), BF16),
            pltpu.VMEM((2, 16, L), F32),
            pltpu.VMEM((N, 16, L), BF16),
            pltpu.VMEM((T, DT, B), BF16),
            pltpu.VMEM((T, DT, B), BF16),
            pltpu.VMEM((PL, DT, B), BF16),
            pltpu.VMEM((Y, L, 4 * L), BF16),
            pltpu.VMEM((Y, 4 * L, L), BF16),
            pltpu.VMEM((Z, 8, B), F32),
            pltpu.VMEM((Z, 4 * L // Z, B), BF16),
            pltpu.VMEM((Z, 4 * L // Z, B), BF16),
            pltpu.VMEM((Z, 4 * L // Z, B), BF16),
            pltpu.VMEM((PL, DT, B), BF16),
            pltpu.VMEM((PL, DT, B), BF16),
            pltpu.VMEM((L, 4 * L), BF16),
            pltpu.VMEM((4 * L, 4 * L), BF16),
            pltpu.VMEM((4 * L, 4 * L), BF16),
            pltpu.VMEM((Y, L, B), F32),
            pltpu.SemaphoreType.DMA((24,)),
            pltpu.SemaphoreType.DMA((16,)),
            pltpu.SemaphoreType.DMA((16,)),
        ],
        compiler_params=pltpu.CompilerParams(
            collective_id=0,
            has_side_effects=True,
            vmem_limit_bytes=67043328 - memory_state.size * 4 - 8192,
        ),
    )(
        stream.T,
        attn_gain.reshape(1, L),
        mixer_gain.reshape(1, L),
        head_gain.reshape(1, L),
        beta_weight.T,
        decay_weight.T,
        decay_log,
        decay_shift,
        memory_state,
        query_weight,
        key_weight,
        value_weight,
        outgate_weight,
        output_weight,
        up_weight,
        down_weight,
    )
    layer_out, memory_next = pl.pallas_call(
        hand_over,
        out_shape=(
            jax.ShapeDtypeStruct((DT, B), BF16),
            jax.ShapeDtypeStruct(memory_state.shape, F32),
        ),
        in_specs=[anywhere] * 2,
        out_specs=(hbm, hbm),
        scratch_shapes=[pltpu.SemaphoreType.DMA((5,))],
        compiler_params=pltpu.CompilerParams(vmem_limit_bytes=2**20),
    )(layer_out, memory_next)
    return layer_out.T, memory_next


def solution(mesh):
    in_specs = (
        P(None, ("kv", "tp")),
        P("kv", "tp", None, None),
        P("kv"),
        P("kv", "tp"),
        P("kv", "tp"),
        P("kv", "tp"),
        P("kv", "tp"),
        P("kv", "tp"),
        P("kv", "tp"),
        P("tp"),
        P("tp"),
        P(),
        P("tp", "kv"),
        P("kv"),
        P("kv", "tp"),
        P("tp", "kv"),
    )
    out_specs = (P(None, ("kv", "tp")), P("kv", "tp", None, None))
    body = functools.partial(shards, mesh.shape["kv"] // Y, mesh.shape["tp"])
    return jax.shard_map(body, mesh=mesh, in_specs=in_specs, out_specs=out_specs, check_vma=False)
```

```python
import functools

import jax
import jax.numpy as jnp
from jax import lax
from jax.experimental import pallas as pl
from jax.experimental.pallas import tpu as pltpu
from jax.sharding import PartitionSpec as P

MESH = pl.DeviceIdType.MESH
F32 = jnp.float32
BF16 = jnp.bfloat16
EPS = 1e-06
Y = 4
L = 128
HEADS_DEV = 4
ROWS = 4


def transposed(x):
    return jnp.transpose(x, (1, 0))


def silu(x):
    return x * jax.nn.sigmoid(x)


def added(parts):
    while len(parts) > 1:
        parts = [a + b for a, b in zip(parts[::2], parts[1::2])] + parts[len(parts) // 2 * 2 :]
    return parts[0]


def softplus(x):
    return jnp.maximum(x, 0.0) + jnp.log1p(jnp.exp(-jnp.abs(x)))


def layer_kernel(
    Z,
    T,
    stream_hbm,
    attn_gain_hbm,
    mixer_gain_hbm,
    head_gain_hbm,
    beta_hbm,
    decay_hbm,
    decay_log_hbm,
    decay_shift_hbm,
    state_ref,
    wq_ref,
    wk_ref,
    wv_ref,
    wg_ref,
    wo_ref,
    wu_ref,
    wd_ref,
    out_ref,
    next_ref,
    stream_ref,
    attn_gain_ref,
    mixer_gain_ref,
    head_gain_ref,
    beta_ref,
    decay_ref,
    decay_log_ref,
    decay_shift_ref,
    state,
    w_in,
    wo,
    gpos,
    etile,
    sgath,
    w1,
    xz,
    s2,
    r2,
    rows_f,
    hall,
    a4,
    r4,
    mgath,
    wu,
    wd,
    sq,
    u6,
    r6,
    hall7,
    d8,
    r8,
    wot,
    wut,
    wdt,
    gcol,
    lsem,
    ssem,
    rsem,
):
    N = Z * Y
    PL = Y * T
    B = N * ROWS
    DT = L // T
    D = N * L
    kv = lax.axis_index("kv")
    tp = lax.axis_index("tp")
    z = lax.div(kv, Y)
    y = lax.rem(kv, Y)
    me_p = y * T + tp
    pz, py = lax.rem(z, 2), lax.rem(y, 2)
    za, zb = z + 1 - 2 * pz, lax.rem(z - 1 + 2 * pz + Z, Z)
    ya, yb = y + 1 - 2 * py, lax.rem(y - 1 + 2 * py + Y, Y)
    spots = [kv, za * Y + y, z * Y + ya, za * Y + ya, zb * Y + y, z * Y + yb, zb * Y + yb]
    spot_far = z * Y + lax.rem(y + 2, Y)
    head_a = pz * 2 + py
    heads_a = [head_a, (1 - pz) * 2 + py, pz * 2 + 1 - py, (1 - pz) * 2 + 1 - py]
    groups = ((0, (0, 1, 2, 3)), (1, (0, 4, 5, 6)))
    tps = [lax.rem(tp + i, T) for i in range(T)]

    def plane_dev(p):
        return (z * Y + lax.div(p, T), lax.rem(p, T))

    def kv_dev(p):
        return (p, tp)

    def each_peer(n, me, act):
        def step(i, c):
            off = 1 + lax.rem(i + (n // 2 - 1), n - 1)
            act(lax.rem(me + off, n))
            return c

        lax.fori_loop(0, n - 1, step, 0)

    def put(src, dst, k, dev):
        pltpu.make_async_remote_copy(
            src_ref=src,
            dst_ref=dst,
            send_sem=ssem.at[k],
            recv_sem=rsem.at[k],
            device_id=dev,
            device_id_type=MESH,
        ).start()

    def got(ref, k):
        with jax.named_scope(f"got{k}"):
            pltpu.make_async_copy(ref, ref, rsem.at[k]).wait()

    def sent(ref, k):
        pltpu.make_async_copy(ref, ref, ssem.at[k]).wait()

    loads = [
        pltpu.make_async_copy(w, w_in.at[m], lsem.at[m])
        for m, w in enumerate((wq_ref, wk_ref, wv_ref, wg_ref))
    ]
    small = [
        pltpu.make_async_copy(a, b, lsem.at[16 + i])
        for i, (a, b) in enumerate((
            (stream_hbm, stream_ref),
            (attn_gain_hbm, attn_gain_ref),
            (mixer_gain_hbm, mixer_gain_ref),
            (beta_hbm, beta_ref),
            (decay_hbm, decay_ref),
        ))
    ]
    late = [
        pltpu.make_async_copy(a, b, lsem.at[21 + i])
        for i, (a, b) in enumerate((
            (head_gain_hbm, head_gain_ref),
            (decay_log_hbm, decay_log_ref),
            (decay_shift_hbm, decay_shift_ref),
        ))
    ]
    for c in small:
        c.start()
    load_out = pltpu.make_async_copy(wo_ref, wo, lsem.at[4])
    load_state = pltpu.make_async_copy(state_ref, state, lsem.at[5])
    for c in loads:
        c.start()
    load_out.start()
    load_state.start()
    for c in late:
        c.start()

    barrier = pltpu.get_barrier_semaphore()

    def greet(dev):
        pl.semaphore_signal(barrier, inc=1, device_id=dev, device_id_type=MESH)

    with jax.named_scope("greet"):
        for dst in reversed(spots[1:]):
            for t in tps:
                greet((dst, t))
        for off in (4, 3, 5, 2, 6):
            greet((lax.rem(z + off, Z) * Y + y, tp))
        greet((spot_far, tp))
        for t in tps[1:]:
            greet((kv, t))

    for c in small:
        c.wait()
    gpos[0] = jnp.broadcast_to(attn_gain_ref[...], (8, L))
    gpos[0, 1:2, :] = mixer_gain_ref[...]
    etile[0] = jnp.concatenate(
        [beta_ref[...].astype(F32), decay_ref[...].astype(F32), jnp.zeros((8, L), F32)], axis=0
    ).astype(BF16)
    own_stream = stream_ref[...].astype(F32)
    sgath[0, tp] = stream_ref[...]

    with jax.named_scope("greeted"):
        pl.semaphore_wait(barrier, 7 * T - 1 + (Z - 3) + 1)

    for k in (3, 6, 1, 2, 4, 5):
        for t in tps:
            put(sgath.at[0, tp], sgath.at[k, tp], 16 + k, (spots[k], t))
    for t in tps[1:]:
        put(sgath.at[0, tp], sgath.at[0, tp], 16, (kv, t))
    for k in range(1, 7):
        put(gpos.at[0], gpos.at[k], 1, (spots[k], tp))
        if k < 4:
            put(etile.at[0], etile.at[k], 2, (spots[k], tp))
    put(gpos.at[0], gpos.at[7], 1, (spot_far, tp))
    for c in loads:
        c.wait()

    def head_cols(m, h):
        return w_in.at[m, :, pl.ds(pl.multiple_of(h * L, L), L)]

    own_w1 = []
    for g, members in groups:
        for slot in (3, 1, 2):
            h = heads_a[slot]
            h = h if g == 0 else 3 - h
            for i in range(2):
                put(
                    head_cols(2 * g + i, h),
                    w1.at[g, slot, :, pl.ds(i * L, L)],
                    3,
                    (spots[members[slot]], tp),
                )
        for i in range(2):
            own_w1.append(
                pltpu.make_async_copy(
                    head_cols(2 * g + i, head_a if g == 0 else 3 - head_a),
                    w1.at[g, 0, :, pl.ds(i * L, L)],
                    lsem.at[6 + 2 * g + i],
                )
            )
    for c in own_w1:
        c.start()

    got(gpos.at[pl.ds(1, 7)], 1)
    got(etile.at[pl.ds(1, 3)], 2)
    x_part = jnp.zeros((16, B), F32)
    squares = jnp.zeros((1, B), F32)
    scaled = []
    for k in range(7):
        if k == 0:
            got(sgath.at[0, pl.ds(0, T - 1)], 16)
        else:
            got(sgath.at[k], 16 + k)
        block = sgath[k].astype(F32).reshape(L, B)
        part = (transposed(block) * gpos[k, 0:1, :]).astype(BF16)
        scaled.append(part)
        if k < 4:
            squares = squares + jnp.sum(block * block, axis=0, keepdims=True)
            x_part = x_part + lax.dot_general(
                etile[k], part, (((1,), (1,)), ((), ())), preferred_element_type=F32
            )
        if k == 3:
            row16 = lax.broadcasted_iota(jnp.int32, (16, B), 0)
            xslot = lax.div(z, 2) * (Y // 2) + lax.div(y, 2)
            xz[xslot] = jnp.where(row16 == 8, squares, x_part)
            for i in (2, 1, 3, 0):
                for j in (1, 0):
                    if i or j:
                        zz, yy = lax.rem(z + 2 * i, Z), lax.rem(y + 2 * j, Y)
                        put(xz.at[xslot], xz.at[xslot], 4, (zz * Y + yy, tp))

    for c in own_w1:
        c.wait()
    got(w1.at[:, pl.ds(1, 3)], 3)
    proj = []
    for g, members in groups:
        total = jnp.zeros((B, 2 * L), F32)
        for slot, k in enumerate(members):
            total = total + jnp.dot(scaled[k], w1[g, slot], preferred_element_type=F32)
        proj += [total[:, 0:L], total[:, L : 2 * L]]
    low = lax.broadcasted_iota(jnp.int32, (B // 8, 8, L), 1) < 4

    def pair_tiles(a, b):
        return (
            jnp.where(low, a, pltpu.roll(b, 4, 1)),
            jnp.where(low, pltpu.roll(a, 4, 1), b),
        )

    pq, pk, pv, pg = [p.reshape(B // 8, 8, L) for p in proj]
    even_a, odd_a = pair_tiles(pq, pk)
    even_b, odd_b = pair_tiles(pv, pg)
    s2[:, 0] = jnp.concatenate([even_a, even_b], axis=1).astype(BF16)
    s2[:, 1] = jnp.concatenate([odd_a, odd_b], axis=1).astype(BF16)
    each_peer(
        N, kv, lambda p: put(s2.at[lax.div(p, 2), lax.rem(p, 2)], r2.at[kv], 5, kv_dev(p))
    )
    r2[kv] = s2[lax.div(kv, 2), lax.rem(kv, 2)]

    def up_cols(yy):
        return wu_ref.at[:, pl.ds(pl.multiple_of(yy * 4 * L, L), 4 * L)]

    own_up = pltpu.make_async_copy(up_cols(y), wu.at[y], lsem.at[10])
    own_up.start()
    for off in (2, 1, 3):
        yy = lax.rem(y + off, Y)
        put(up_cols(yy), wu.at[y], 6, (z * Y + yy, tp))

    for c in late:
        c.wait()
    got(xz.at[pl.ds(0, Z - 1)], 4)
    x_all = xz[0]
    for j in range(1, Z):
        x_all = x_all + xz[j]
    fac = lax.rsqrt(x_all[8:9] / D + EPS)
    xf = x_all * fac
    dlog = jnp.zeros((16, B), F32)
    dshift = jnp.zeros((16, B), F32)
    for h in range(HEADS_DEV):
        dlog = jnp.where(row16 == 4 + h, decay_log_ref[h], dlog)
        dshift = jnp.where(row16 == 4 + h, decay_shift_ref[h], dshift)
    scal = jnp.where(
        row16 < 4,
        jax.nn.sigmoid(xf),
        jnp.where(row16 < 8, jnp.exp(-jnp.exp(dlog) * softplus(xf + dshift)), fac),
    )
    lane_group = lax.div(lax.broadcasted_iota(jnp.int32, (16, B), 1), 4)
    mine = jnp.zeros((16, B), F32)
    for m in range(4):
        rolled = pltpu.roll(scal, lax.rem(B + m * ROWS - kv * ROWS, B), 1)
        mine = jnp.where(lane_group == m, rolled, mine)
    cols = transposed(jnp.concatenate([mine, jnp.zeros((L - 16, B), F32)], axis=0))[0:16]

    got(r2.at[pl.ds(0, N - 1)], 5)
    load_state.wait()
    row_id = lax.broadcasted_iota(jnp.int32, (16, 1), 0)
    acts = []
    for h in range(HEADS_DEV):
        here = [
            [n for n in range(N) if (n // Y % 2) * 2 + n % 2 == want] for want in (h, 3 - h)
        ]
        qk = [r2[n, 0:8, :].astype(F32) for n in here[0]]
        vg = [r2[n, 8:16, :].astype(F32) for n in here[1]]
        total = jnp.concatenate([added(qk), added(vg)], axis=0)
        a = silu(total * cols[:, 8:9])
        inv = lax.rsqrt(jnp.sum(a * a, axis=1, keepdims=True) + EPS)
        norm = jnp.where(row_id < 4, inv * L ** (-0.5), jnp.where(row_id < 8, inv, 1.0))
        acts.append(a * norm)
        rows_f[1, 4 * h : 4 * h + 4, :] = a[12:16]
    flipped = transposed(jnp.concatenate(acts + [jnp.zeros((L - 64, L), F32)], axis=0))
    for h in range(HEADS_DEV):
        for r in range(ROWS):
            q_col = flipped[:, h * 16 + r : h * 16 + r + 1]
            k_col = flipped[:, h * 16 + 4 + r : h * 16 + 5 + r]
            kept = state[r, h] * cols[r : r + 1, 4 + h : 5 + h]
            recalled = jnp.sum(kept * k_col, axis=0, keepdims=True)
            corr = cols[r : r + 1, h : h + 1] * (acts[h][8 + r : 9 + r] - recalled)
            new = kept + k_col * corr
            next_ref[r, h] = new
            rows_f[0, 4 * h + r : 4 * h + r + 1, :] = jnp.sum(new * q_col, axis=0, keepdims=True)
    readout = rows_f[0]
    readout = readout * lax.rsqrt(jnp.mean(readout * readout, axis=1, keepdims=True) + EPS)
    hall[kv] = (readout * head_gain_ref[...] * rows_f[1]).astype(BF16)

    each_peer(N, kv, lambda p: put(hall.at[kv], hall.at[kv], 7, kv_dev(p)))

    def down_rows(yy):
        return wd_ref.at[pl.ds(pl.multiple_of(yy * 4 * L, L), 4 * L), :]

    own_down = pltpu.make_async_copy(down_rows(y), wd.at[y], lsem.at[12])
    own_down.start()
    for off in (2, 1, 3):
        yy = lax.rem(y + off, Y)
        put(down_rows(yy), wd.at[y], 8, (z * Y + yy, tp))

    load_out.wait()
    for i in range(HEADS_DEV):
        wot[:, i * L : (i + 1) * L] = transposed(wo[i * L : (i + 1) * L, :].astype(F32)).astype(BF16)
    own_up.wait()
    got(wu.at[pl.ds(0, Y - 1)], 6)
    for j in range(Y):
        for i in range(4):
            wut[i * L : (i + 1) * L, j * L : (j + 1) * L] = transposed(
                wu[j, :, i * L : (i + 1) * L].astype(F32)
            ).astype(BF16)
    for slot, yy in ((0, y), (2, ya), (5, yb), (7, lax.rem(y + 2, Y))):
        gcol[yy] = transposed(jnp.broadcast_to(gpos[slot, 1:2, :], (B, L)))
    got(hall.at[pl.ds(0, N - 1)], 7)
    heads = hall[...].astype(F32).reshape(N // 2, 2, 2, 8, L)
    attn = jnp.zeros((L, B), F32)
    for c in range(2):
        h_even, h_odd = pair_tiles(heads[:, 0, c], heads[:, 1, c])
        for i, hh in ((2 * c, h_even), (2 * c + 1, h_odd)):
            attn = attn + lax.dot_general(
                wot[:, i * L : (i + 1) * L],
                hh.reshape(B, L).astype(BF16),
                (((1,), (1,)), ((), ())),
                preferred_element_type=F32,
            )
    a4[...] = attn.reshape(T, DT, B).astype(BF16)
    each_peer(T, tp, lambda p: put(a4.at[p], r4.at[tp], 9, (kv, p)))
    r4[tp] = a4[tp]
    got(r4.at[pl.ds(0, T - 1)], 9)
    attn_mine = r4[0].astype(F32)
    for j in range(1, T):
        attn_mine = attn_mine + r4[j].astype(F32)
    middle = (own_stream + attn_mine).astype(BF16)

    mgath[me_p] = middle
    each_peer(PL, me_p, lambda p: put(mgath.at[me_p], mgath.at[me_p], 10, plane_dev(p)))
    got(mgath.at[pl.ds(0, PL - 1)], 10)
    up = jnp.zeros((4 * L, B), F32)
    squares2 = jnp.zeros((1, B), F32)
    for j in range(Y):
        block = mgath[j * T : (j + 1) * T].astype(F32).reshape(L, B)
        squares2 = squares2 + jnp.sum(block * block, axis=0, keepdims=True)
        part = (block * gcol[j]).astype(BF16)
        up = up + jnp.dot(wut[:, j * L : (j + 1) * L], part, preferred_element_type=F32)
    u6[...] = up.astype(BF16).reshape(Z, 4 * L // Z, B)
    sq[z] = jnp.broadcast_to(squares2, (8, B))
    offs = [o for o in (4, 3, 5, 2, 6, 1, 7) if o < Z]
    for off in offs:
        zz = lax.rem(z + off, Z)
        put(u6.at[zz], r6.at[z], 11, (zz * Y + y, tp))
    r6[z] = u6[z]
    own_down.wait()
    got(wd.at[pl.ds(0, Y - 1)], 8)
    for j in range(Y):
        for i in range(4):
            wdt[j * L : (j + 1) * L, i * L : (i + 1) * L] = transposed(
                wd[j, i * L : (i + 1) * L, :].astype(F32)
            ).astype(BF16)
    got(r6.at[pl.ds(0, Z - 1)], 11)
    up_mine = r6[0].astype(F32)
    for j in range(1, Z):
        up_mine = up_mine + r6[j].astype(F32)
    hidden = jnp.square(jnp.maximum(up_mine, 0.0)).astype(BF16)
    hall7[z] = hidden
    for off in offs:
        zz = lax.rem(z + off, Z)
        put(hall7.at[z], hall7.at[z], 13, (zz * Y + y, tp))
    for off in offs:
        zz = lax.rem(z + off, Z)
        put(sq.at[z], sq.at[z], 12, (zz * Y + y, tp))
    got(hall7.at[pl.ds(0, Z - 1)], 13)
    down = jnp.dot(wdt[...], hall7[...].reshape(4 * L, B), preferred_element_type=F32)
    d8[...] = down.reshape(PL, DT, B).astype(BF16)
    each_peer(PL, me_p, lambda p: put(d8.at[p], r8.at[me_p], 14, plane_dev(p)))
    r8[me_p] = d8[me_p]
    got(sq.at[pl.ds(0, Z - 1)], 12)
    total2 = sq[0, 0:1, :]
    for j in range(1, Z):
        total2 = total2 + sq[j, 0:1, :]
    factor2 = lax.rsqrt(total2 / D + EPS)
    got(r8.at[pl.ds(0, PL - 1)], 14)
    parts = [r8[j].astype(F32) for j in range(4)]
    for j in range(4, PL):
        parts[j % 4] = parts[j % 4] + r8[j].astype(F32)
    mixed = (parts[0] + parts[1]) + (parts[2] + parts[3])
    final = middle.astype(F32) + mixed * (factor2 * factor2)
    out_ref[...] = final.astype(BF16)

    sent(sgath.at[0, pl.ds(0, T - 1)], 16)
    for k in range(1, 7):
        sent(sgath.at[k], 16 + k)
    sent(gpos.at[pl.ds(1, 7)], 1)
    sent(etile.at[pl.ds(1, 3)], 2)
    sent(w1.at[:, pl.ds(1, 3)], 3)
    sent(xz.at[pl.ds(0, Z - 1)], 4)
    sent(r2.at[pl.ds(0, N - 1)], 5)
    sent(wu.at[pl.ds(0, Y - 1)], 6)
    sent(hall.at[pl.ds(0, N - 1)], 7)
    sent(wd.at[pl.ds(0, Y - 1)], 8)
    sent(r4.at[pl.ds(0, T - 1)], 9)
    sent(mgath.at[pl.ds(0, PL - 1)], 10)
    sent(r6.at[pl.ds(0, Z - 1)], 11)
    sent(sq.at[pl.ds(0, Z - 1)], 12)
    sent(hall7.at[pl.ds(0, Z - 1)], 13)
    sent(r8.at[pl.ds(0, PL - 1)], 14)


def hand_over(layer_in, state_in, layer_ref, state_ref, sems):
    copies = [pltpu.make_async_copy(layer_in, layer_ref, sems.at[4])]
    for r in range(ROWS):
        copies.append(pltpu.make_async_copy(state_in.at[r], state_ref.at[r], sems.at[r]))
    for c in copies:
        c.start()
    for c in copies:
        c.wait()


def shards(
    Z,
    T,
    stream,
    memory_state,
    attn_gain,
    query_weight,
    key_weight,
    value_weight,
    outgate_weight,
    beta_weight,
    decay_weight,
    decay_log,
    decay_shift,
    head_gain,
    output_weight,
    mixer_gain,
    up_weight,
    down_weight,
):
    N, PL, B, DT = Z * Y, Y * T, Z * Y * ROWS, L // T
    hbm = pl.BlockSpec(memory_space=pltpu.HBM)
    anywhere = pl.BlockSpec(memory_space=pl.ANY)
    vmem = pl.BlockSpec(memory_space=pltpu.VMEM)
    layer_out, memory_next = pl.pallas_call(
        functools.partial(layer_kernel, Z, T),
        out_shape=(
            pltpu.VMEM((DT, B), BF16),
            pltpu.VMEM(memory_state.shape, F32),
        ),
        in_specs=[hbm] * 16,
        out_specs=(vmem, vmem),
        scratch_shapes=[
            pltpu.VMEM((DT, B), BF16),
            pltpu.VMEM((1, L), F32),
            pltpu.VMEM((1, L), F32),
            pltpu.VMEM((1, L), F32),
            pltpu.VMEM((HEADS_DEV, L), BF16),
            pltpu.VMEM((HEADS_DEV, L), BF16),
            pltpu.SMEM((HEADS_DEV,), F32),
            pltpu.SMEM((HEADS_DEV,), F32),
            pltpu.VMEM((ROWS, HEADS_DEV, L, L), F32),
            pltpu.VMEM((4, L, 4 * L), BF16),
            pltpu.VMEM((4 * L, L), BF16),
            pltpu.VMEM((8, 8, L), F32),
            pltpu.VMEM((4, 16, L), BF16),
            pltpu.VMEM((7, T, DT, B), BF16),
            pltpu.VMEM((2, 4, L, 2 * L), BF16),
            pltpu.VMEM((Z, 16, B), F32),
            pltpu.VMEM((N // 2, 2, 16, L), BF16),
            pltpu.VMEM((N, 16, L), BF16),
            pltpu.VMEM((2, 16, L), F32),
            pltpu.VMEM((N, 16, L), BF16),
            pltpu.VMEM((T, DT, B), BF16),
            pltpu.VMEM((T, DT, B), BF16),
            pltpu.VMEM((PL, DT, B), BF16),
            pltpu.VMEM((Y, L, 4 * L), BF16),
            pltpu.VMEM((Y, 4 * L, L), BF16),
            pltpu.VMEM((Z, 8, B), F32),
            pltpu.VMEM((Z, 4 * L // Z, B), BF16),
            pltpu.VMEM((Z, 4 * L // Z, B), BF16),
            pltpu.VMEM((Z, 4 * L // Z, B), BF16),
            pltpu.VMEM((PL, DT, B), BF16),
            pltpu.VMEM((PL, DT, B), BF16),
            pltpu.VMEM((L, 4 * L), BF16),
            pltpu.VMEM((4 * L, 4 * L), BF16),
            pltpu.VMEM((4 * L, 4 * L), BF16),
            pltpu.VMEM((Y, L, B), F32),
            pltpu.SemaphoreType.DMA((24,)),
            pltpu.SemaphoreType.DMA((24,)),
            pltpu.SemaphoreType.DMA((24,)),
        ],
        compiler_params=pltpu.CompilerParams(
            collective_id=0,
            has_side_effects=True,
            vmem_limit_bytes=67043328 - memory_state.size * 4 - 8192,
        ),
    )(
        stream.T,
        attn_gain.reshape(1, L),
        mixer_gain.reshape(1, L),
        head_gain.reshape(1, L),
        beta_weight.T,
        decay_weight.T,
        decay_log,
        decay_shift,
        memory_state,
        query_weight,
        key_weight,
        value_weight,
        outgate_weight,
        output_weight,
        up_weight,
        down_weight,
    )
    layer_out, memory_next = pl.pallas_call(
        hand_over,
        out_shape=(
            jax.ShapeDtypeStruct((DT, B), BF16),
            jax.ShapeDtypeStruct(memory_state.shape, F32),
        ),
        in_specs=[anywhere] * 2,
        out_specs=(hbm, hbm),
        scratch_shapes=[pltpu.SemaphoreType.DMA((5,))],
        compiler_params=pltpu.CompilerParams(vmem_limit_bytes=2**20),
    )(layer_out, memory_next)
    return layer_out.T, memory_next


def solution(mesh):
    in_specs = (
        P(None, ("kv", "tp")),
        P("kv", "tp", None, None),
        P("kv"),
        P("kv", "tp"),
        P("kv", "tp"),
        P("kv", "tp"),
        P("kv", "tp"),
        P("kv", "tp"),
        P("kv", "tp"),
        P("tp"),
        P("tp"),
        P(),
        P("tp", "kv"),
        P("kv"),
        P("kv", "tp"),
        P("tp", "kv"),
    )
    out_specs = (P(None, ("kv", "tp")), P("kv", "tp", None, None))
    body = functools.partial(shards, mesh.shape["kv"] // Y, mesh.shape["tp"])
    return jax.shard_map(body, mesh=mesh, in_specs=in_specs, out_specs=out_specs, check_vma=False)
```

```python
import functools

import jax
import jax.numpy as jnp
from jax import lax
from jax.experimental import pallas as pl
from jax.experimental.pallas import tpu as pltpu
from jax.sharding import PartitionSpec as P

MESH = pl.DeviceIdType.MESH
F32 = jnp.float32
BF16 = jnp.bfloat16
EPS = 1e-06
Y = 4
L = 128
HEADS_DEV = 4
ROWS = 4


def transposed(x):
    return jnp.transpose(x, (1, 0))


def silu(x):
    return x * jax.nn.sigmoid(x)


def added(parts):
    while len(parts) > 1:
        parts = [a + b for a, b in zip(parts[::2], parts[1::2])] + parts[len(parts) // 2 * 2 :]
    return parts[0]


def softplus(x):
    return jnp.maximum(x, 0.0) + jnp.log1p(jnp.exp(-jnp.abs(x)))


def layer_kernel(
    Z,
    T,
    stream_hbm,
    attn_gain_hbm,
    mixer_gain_hbm,
    head_gain_hbm,
    beta_hbm,
    decay_hbm,
    decay_log_hbm,
    decay_shift_hbm,
    state_ref,
    wq_ref,
    wk_ref,
    wv_ref,
    wg_ref,
    wo_ref,
    wu_ref,
    wd_ref,
    out_ref,
    next_ref,
    stream_ref,
    attn_gain_ref,
    mixer_gain_ref,
    head_gain_ref,
    beta_ref,
    decay_ref,
    decay_log_ref,
    decay_shift_ref,
    state,
    w_in,
    wof,
    gpos,
    etile,
    sgath,
    w1,
    xz,
    s2,
    r2,
    rows_f,
    hall,
    a4,
    r4,
    mgath,
    wu,
    wd,
    sq,
    u6,
    r6,
    hall7,
    d8,
    r8,
    wut,
    wdt,
    gmix,
    mids,
    lsem,
    ssem,
    rsem,
):
    N = Z * Y
    PL = Y * T
    B = N * ROWS
    DT = L // T
    D = N * L
    kv = lax.axis_index("kv")
    tp = lax.axis_index("tp")
    z = lax.div(kv, Y)
    y = lax.rem(kv, Y)
    me_p = y * T + tp
    pz, py = lax.rem(z, 2), lax.rem(y, 2)
    za, zb = z + 1 - 2 * pz, lax.rem(z - 1 + 2 * pz + Z, Z)
    ya, yb = y + 1 - 2 * py, lax.rem(y - 1 + 2 * py + Y, Y)
    spots = [kv, za * Y + y, z * Y + ya, za * Y + ya, zb * Y + y, z * Y + yb, zb * Y + yb]
    spot_far = z * Y + lax.rem(y + 2, Y)
    head_a = pz * 2 + py
    heads_a = [head_a, (1 - pz) * 2 + py, pz * 2 + 1 - py, (1 - pz) * 2 + 1 - py]
    groups = ((0, (0, 1, 2, 3)), (1, (0, 4, 5, 6)))
    tps = [lax.rem(tp + i, T) for i in range(T)]

    def plane_dev(p):
        return (z * Y + lax.div(p, T), lax.rem(p, T))

    def kv_dev(p):
        return (p, tp)

    def each_peer(n, me, act):
        def step(i, c):
            off = 1 + lax.rem(i + (n // 2 - 1), n - 1)
            act(lax.rem(me + off, n))
            return c

        lax.fori_loop(0, n - 1, step, 0)

    def put(src, dst, k, dev):
        pltpu.make_async_remote_copy(
            src_ref=src,
            dst_ref=dst,
            send_sem=ssem.at[k],
            recv_sem=rsem.at[k],
            device_id=dev,
            device_id_type=MESH,
        ).start()

    def got(ref, k):
        with jax.named_scope(f"got{k}"):
            pltpu.make_async_copy(ref, ref, rsem.at[k]).wait()

    def sent(ref, k):
        pltpu.make_async_copy(ref, ref, ssem.at[k]).wait()

    loads = [
        pltpu.make_async_copy(w, w_in.at[m], lsem.at[m])
        for m, w in enumerate((wq_ref, wk_ref, wv_ref, wg_ref))
    ]
    small = [
        pltpu.make_async_copy(a, b, lsem.at[16 + i])
        for i, (a, b) in enumerate((
            (stream_hbm, stream_ref),
            (attn_gain_hbm, attn_gain_ref),
            (mixer_gain_hbm, mixer_gain_ref),
            (beta_hbm, beta_ref),
            (decay_hbm, decay_ref),
        ))
    ]
    late = [
        pltpu.make_async_copy(a, b, lsem.at[21 + i])
        for i, (a, b) in enumerate((
            (head_gain_hbm, head_gain_ref),
            (decay_log_hbm, decay_log_ref),
            (decay_shift_hbm, decay_shift_ref),
        ))
    ]
    for c in small:
        c.start()
    own_out = wof.at[:, pl.ds(pl.multiple_of(y * L, L), L)]
    load_out = pltpu.make_async_copy(wo_ref, own_out, lsem.at[4])
    load_state = pltpu.make_async_copy(state_ref, state, lsem.at[5])
    for c in loads:
        c.start()
    load_out.start()
    load_state.start()
    for c in late:
        c.start()

    barrier = pltpu.get_barrier_semaphore()

    def greet(dev):
        pl.semaphore_signal(barrier, inc=1, device_id=dev, device_id_type=MESH)

    with jax.named_scope("greet"):
        for dst in reversed(spots[1:]):
            for t in tps:
                greet((dst, t))
        for off in (4, 3, 5, 2, 6):
            greet((lax.rem(z + off, Z) * Y + y, tp))
        greet((spot_far, tp))
        for t in tps[1:]:
            greet((kv, t))

    for c in small:
        c.wait()
    gpos[0] = jnp.broadcast_to(attn_gain_ref[...], (8, L))
    gpos[0, 1:2, :] = mixer_gain_ref[...]
    etile[0] = jnp.concatenate(
        [beta_ref[...].astype(F32), decay_ref[...].astype(F32), jnp.zeros((8, L), F32)], axis=0
    ).astype(BF16)
    sgath[0, tp] = stream_ref[...]

    with jax.named_scope("greeted"):
        pl.semaphore_wait(barrier, 7 * T - 1 + (Z - 3) + 1)

    put(gpos.at[0], gpos.at[7], 1, (spot_far, tp))
    for k in (3, 6, 1, 2, 4, 5):
        put(gpos.at[0], gpos.at[k], 1, (spots[k], tp))
        if k < 4:
            put(etile.at[0], etile.at[k], 2, (spots[k], tp))
    for k in (3, 6, 1, 2, 4, 5):
        for i in (4, 3, 5, 2, 6, 1, 7, 0):
            put(sgath.at[0, tp], sgath.at[k, tp], 16 + k, (spots[k], tps[i]))
    for i in (4, 3, 5, 2, 6, 1, 7):
        put(sgath.at[0, tp], sgath.at[0, tp], 16, (kv, tps[i]))
    for c in loads:
        c.wait()

    def head_cols(m, h):
        return w_in.at[m, :, pl.ds(pl.multiple_of(h * L, L), L)]

    own_w1 = []
    for g, members in groups:
        for slot in (3, 1, 2):
            h = heads_a[slot]
            h = h if g == 0 else 3 - h
            for i in range(2):
                put(
                    head_cols(2 * g + i, h),
                    w1.at[g, slot, :, pl.ds(i * L, L)],
                    3,
                    (spots[members[slot]], tp),
                )
        for i in range(2):
            own_w1.append(
                pltpu.make_async_copy(
                    head_cols(2 * g + i, head_a if g == 0 else 3 - head_a),
                    w1.at[g, 0, :, pl.ds(i * L, L)],
                    lsem.at[6 + 2 * g + i],
                )
            )
    for c in own_w1:
        c.start()

    got(gpos.at[pl.ds(1, 7)], 1)
    got(etile.at[pl.ds(1, 3)], 2)
    x_part = jnp.zeros((16, B), F32)
    squares = jnp.zeros((1, B), F32)
    scaled = {}
    for k in (0, 1, 2, 3, 4, 5, 6):
        if k == 0:
            got(sgath.at[0, pl.ds(0, T - 1)], 16)
        else:
            got(sgath.at[k], 16 + k)
        block = sgath[k].astype(F32).reshape(L, B)
        part = (transposed(block) * gpos[k, 0:1, :]).astype(BF16)
        scaled[k] = part
        if k < 4:
            squares = squares + jnp.sum(block * block, axis=0, keepdims=True)
            x_part = x_part + lax.dot_general(
                etile[k], part, (((1,), (1,)), ((), ())), preferred_element_type=F32
            )
        if k == 3:
            row16 = lax.broadcasted_iota(jnp.int32, (16, B), 0)
            xslot = lax.div(z, 2) * (Y // 2) + lax.div(y, 2)
            xz[xslot] = jnp.where(row16 == 8, squares, x_part)
            for i in (2, 1, 3, 0):
                for j in (1, 0):
                    if i or j:
                        zz, yy = lax.rem(z + 2 * i, Z), lax.rem(y + 2 * j, Y)
                        put(xz.at[xslot], xz.at[xslot], 4, (zz * Y + yy, tp))

    for c in own_w1:
        c.wait()
    got(w1.at[:, pl.ds(1, 3)], 3)
    proj = []
    for g, members in groups:
        total = jnp.zeros((B, 2 * L), F32)
        for slot, k in enumerate(members):
            total = total + jnp.dot(scaled[k], w1[g, slot], preferred_element_type=F32)
        proj += [total[:, 0:L], total[:, L : 2 * L]]
    def pair_tiles(a, b):
        low = lax.broadcasted_iota(jnp.int32, a.shape, 1) < 4
        return (
            jnp.where(low, a, pltpu.roll(b, 4, 1)),
            jnp.where(low, pltpu.roll(a, 4, 1), b),
        )

    pq, pk, pv, pg = [p.reshape(B // 8, 8, L) for p in proj]
    even_a, odd_a = pair_tiles(pq, pk)
    even_b, odd_b = pair_tiles(pv, pg)
    s2[:, 0] = jnp.concatenate([even_a, even_b], axis=1).astype(BF16)
    s2[:, 1] = jnp.concatenate([odd_a, odd_b], axis=1).astype(BF16)
    each_peer(
        N, kv, lambda p: put(s2.at[lax.div(p, 2), lax.rem(p, 2)], r2.at[kv], 5, kv_dev(p))
    )
    r2[kv] = s2[lax.div(kv, 2), lax.rem(kv, 2)]

    for t in tps:
        put(sgath.at[0, tp], sgath.at[7, tp], 23, (spot_far, t))
    for off in (2, 1, 3):
        put(wo_ref, own_out, 0, (z * Y + lax.rem(y + off, Y), tp))

    for c in late:
        c.wait()
    got(xz.at[pl.ds(0, Z - 1)], 4)
    x_all = xz[0]
    for j in range(1, Z):
        x_all = x_all + xz[j]
    fac = lax.rsqrt(x_all[8:9] / D + EPS)
    xf = x_all * fac
    dlog = jnp.zeros((16, B), F32)
    dshift = jnp.zeros((16, B), F32)
    for h in range(HEADS_DEV):
        dlog = jnp.where(row16 == 4 + h, decay_log_ref[h], dlog)
        dshift = jnp.where(row16 == 4 + h, decay_shift_ref[h], dshift)
    scal = jnp.where(
        row16 < 4,
        jax.nn.sigmoid(xf),
        jnp.where(row16 < 8, jnp.exp(-jnp.exp(dlog) * softplus(xf + dshift)), fac),
    )
    lane_group = lax.div(lax.broadcasted_iota(jnp.int32, (16, B), 1), 4)
    mine = jnp.zeros((16, B), F32)
    for m in range(4):
        rolled = pltpu.roll(scal, lax.rem(B + m * ROWS - kv * ROWS, B), 1)
        mine = jnp.where(lane_group == m, rolled, mine)
    cols = transposed(jnp.concatenate([mine, jnp.zeros((L - 16, B), F32)], axis=0))[0:16]

    got(r2.at[pl.ds(0, N - 1)], 5)
    load_state.wait()
    row_id = lax.broadcasted_iota(jnp.int32, (16, 1), 0)
    acts = []
    for h in range(HEADS_DEV):
        here = [
            [n for n in range(N) if (n // Y % 2) * 2 + n % 2 == want] for want in (h, 3 - h)
        ]
        qk = [r2[n, 0:8, :].astype(F32) for n in here[0]]
        vg = [r2[n, 8:16, :].astype(F32) for n in here[1]]
        total = jnp.concatenate([added(qk), added(vg)], axis=0)
        a = silu(total * cols[:, 8:9])
        inv = lax.rsqrt(jnp.sum(a * a, axis=1, keepdims=True) + EPS)
        norm = jnp.where(row_id < 4, inv * L ** (-0.5), jnp.where(row_id < 8, inv, 1.0))
        acts.append(a * norm)
        rows_f[1, 4 * h : 4 * h + 4, :] = a[12:16]
    flipped = transposed(jnp.concatenate(acts + [jnp.zeros((L - 64, L), F32)], axis=0))
    for h in range(HEADS_DEV):
        for r in range(ROWS):
            q_col = flipped[:, h * 16 + r : h * 16 + r + 1]
            k_col = flipped[:, h * 16 + 4 + r : h * 16 + 5 + r]
            kept = state[r, h] * cols[r : r + 1, 4 + h : 5 + h]
            recalled = jnp.sum(kept * k_col, axis=0, keepdims=True)
            corr = cols[r : r + 1, h : h + 1] * (acts[h][8 + r : 9 + r] - recalled)
            new = kept + k_col * corr
            next_ref[r, h] = new
            rows_f[0, 4 * h + r : 4 * h + r + 1, :] = jnp.sum(new * q_col, axis=0, keepdims=True)
    readout = rows_f[0]
    readout = readout * lax.rsqrt(jnp.mean(readout * readout, axis=1, keepdims=True) + EPS)
    hall[z] = (readout * head_gain_ref[...] * rows_f[1]).astype(BF16)

    offs = (4, 3, 5, 2, 6, 1, 7)
    for off in offs:
        put(hall.at[z], hall.at[z], 7, (lax.rem(z + off, Z) * Y + y, tp))

    def up_cols(yy):
        return wu_ref.at[:, pl.ds(pl.multiple_of(yy * 4 * L, L), 4 * L)]

    own_up = pltpu.make_async_copy(up_cols(y), wu.at[y], lsem.at[10])
    own_up.start()
    for off in (2, 1, 3):
        yy = lax.rem(y + off, Y)
        put(up_cols(yy), wu.at[y], 6, (z * Y + yy, tp))

    got(sgath.at[7], 23)
    row_mid = (tp * Y + y) * ROWS
    sel_row = lax.broadcasted_iota(jnp.int32, (16, B), 0)
    sel_lane = lax.broadcasted_iota(jnp.int32, (16, B), 1)
    mid = jnp.zeros((16, L), F32)
    for slot, yy in ((0, y), (2, ya), (5, yb), (7, lax.rem(y + 2, Y))):
        gmix[yy] = gpos[slot]
        pick = (lax.div(sel_row, 4) == yy) & (sel_lane == row_mid + lax.rem(sel_row, 4))
        mid = mid + lax.dot_general(
            jnp.where(pick, 1.0, 0.0).astype(BF16),
            sgath[slot].reshape(L, B),
            (((1,), (1,)), ((), ())),
            preferred_element_type=F32,
        )
    load_out.wait()
    got(wof.at[:, pl.ds(0, 3 * L)], 0)

    got(hall.at[pl.ds(0, Z - 1)], 7)
    heads = hall[...].astype(F32).reshape(Z // 2, 2, 2, 8, L)
    attn = jnp.zeros((Z * ROWS, 4 * L), F32)
    for c in range(2):
        h_even, h_odd = pair_tiles(heads[:, 0, c], heads[:, 1, c])
        for i, hh in ((2 * c, h_even), (2 * c + 1, h_odd)):
            attn = attn + jnp.dot(
                hh.reshape(Z * ROWS, L).astype(BF16),
                wof[i * L : (i + 1) * L, :],
                preferred_element_type=F32,
            )
    a_d = [attn[:, d * L : (d + 1) * L].reshape(Z // 2, 8, L) for d in range(4)]
    even_a, odd_a = pair_tiles(a_d[0], a_d[1])
    even_b, odd_b = pair_tiles(a_d[2], a_d[3])
    a4[:, 0] = jnp.concatenate([even_a, even_b], axis=1).astype(BF16)
    a4[:, 1] = jnp.concatenate([odd_a, odd_b], axis=1).astype(BF16)
    for i in offs:
        put(a4.at[lax.div(tps[i], 2), lax.rem(tps[i], 2)], r4.at[tp], 9, (kv, tps[i]))
    r4[tp] = a4[lax.div(tp, 2), lax.rem(tp, 2)]
    got(r4.at[pl.ds(0, T - 1)], 9)
    mid = mid + added([r4[j].astype(F32) for j in range(T)])

    slot_mid = tp * Y + y
    mgath[slot_mid] = mid.astype(BF16)
    each_peer(
        PL, me_p, lambda p: put(mgath.at[slot_mid], mgath.at[slot_mid], 10, plane_dev(p))
    )
    own_up.wait()
    got(wu.at[pl.ds(0, Y - 1)], 6)
    for j in range(Y):
        for i in range(4):
            wut[i * L : (i + 1) * L, j * L : (j + 1) * L] = transposed(
                wu[j, :, i * L : (i + 1) * L].astype(F32)
            ).astype(BF16)
    got(mgath.at[pl.ds(0, PL - 1)], 10)
    pairs = mgath[...].astype(F32).reshape(N // 2, 2, 2, 8, L)
    up = jnp.zeros((4 * L, B), F32)
    middles = []
    for c in range(2):
        middles += pair_tiles(pairs[:, 0, c], pairs[:, 1, c])
    middles = [m.reshape(B, L) for m in middles]
    for d in range(Y):
        up = up + lax.dot_general(
            wut[:, d * L : (d + 1) * L],
            (middles[d] * gmix[d, 1:2, :]).astype(BF16),
            (((1,), (1,)), ((), ())),
            preferred_element_type=F32,
        )
    u6[...] = up.astype(BF16).reshape(Z, 4 * L // Z, B)
    for off in offs:
        zz = lax.rem(z + off, Z)
        put(u6.at[zz], r6.at[z], 11, (zz * Y + y, tp))
    r6[z] = u6[z]
    def down_rows(yy):
        return wd_ref.at[pl.ds(pl.multiple_of(yy * 4 * L, L), 4 * L), :]

    own_down = pltpu.make_async_copy(down_rows(y), wd.at[y], lsem.at[12])
    own_down.start()
    for off in (2, 1, 3):
        yy = lax.rem(y + off, Y)
        put(down_rows(yy), wd.at[y], 8, (z * Y + yy, tp))

    squares2 = jnp.zeros((8, B), F32)
    for d in range(Y):
        mids[d] = middles[d].astype(BF16)
        squares2 = squares2 + lax.dot_general(
            jnp.ones((8, L), F32),
            middles[d] * middles[d],
            (((1,), (1,)), ((), ())),
            preferred_element_type=F32,
            precision=lax.Precision.HIGHEST,
        )
    sq[z] = squares2
    own_row = lax.broadcasted_iota(jnp.int32, (DT, L), 0) + tp * DT
    own_lane = lax.broadcasted_iota(jnp.int32, (DT, L), 1)
    middle = lax.dot_general(
        jnp.where(own_row == own_lane, 1.0, 0.0).astype(BF16),
        mids[y],
        (((1,), (1,)), ((), ())),
        preferred_element_type=F32,
    )
    got(r6.at[pl.ds(0, Z - 1)], 11)
    up_mine = r6[0].astype(F32)
    for j in range(1, Z):
        up_mine = up_mine + r6[j].astype(F32)
    hidden = jnp.square(jnp.maximum(up_mine, 0.0)).astype(BF16)
    hall7[z] = hidden
    for off in offs:
        zz = lax.rem(z + off, Z)
        put(hall7.at[z], hall7.at[z], 13, (zz * Y + y, tp))
    for off in offs:
        zz = lax.rem(z + off, Z)
        put(sq.at[z], sq.at[z], 12, (zz * Y + y, tp))
    own_down.wait()
    got(wd.at[pl.ds(0, Y - 1)], 8)
    for j in range(Y):
        for i in range(4):
            wdt[j * L : (j + 1) * L, i * L : (i + 1) * L] = transposed(
                wd[j, i * L : (i + 1) * L, :].astype(F32)
            ).astype(BF16)
    got(hall7.at[pl.ds(0, Z - 1)], 13)
    hid = hall7[...].reshape(4 * L, B)
    for off in (2, 1, 3, 0):
        yy = lax.rem(y + off, Y)
        first = yy * T
        down = jnp.dot(
            wdt[pl.ds(pl.multiple_of(yy * L, L), L), :], hid, preferred_element_type=F32
        )
        d8[pl.ds(first, T)] = down.reshape(T, DT, B).astype(BF16)
        for i in (4, 3, 5, 2, 6, 1, 7, 0):
            if off or i:
                t = tps[i]
                put(d8.at[first + t], r8.at[me_p], 14, (z * Y + yy, t))
    r8[me_p] = d8[me_p]
    got(sq.at[pl.ds(0, Z - 1)], 12)
    total2 = sq[0, 0:1, :]
    for j in range(1, Z):
        total2 = total2 + sq[j, 0:1, :]
    factor2 = lax.rsqrt(total2 / D + EPS)
    sent(sgath.at[0, pl.ds(0, T - 1)], 16)
    for k in range(1, 7):
        sent(sgath.at[k], 16 + k)
    sent(gpos.at[pl.ds(1, 7)], 1)
    sent(etile.at[pl.ds(1, 3)], 2)
    sent(w1.at[:, pl.ds(1, 3)], 3)
    sent(xz.at[pl.ds(0, Z - 1)], 4)
    sent(r2.at[pl.ds(0, N - 1)], 5)
    sent(wu.at[pl.ds(0, Y - 1)], 6)
    sent(hall.at[pl.ds(0, Z - 1)], 7)
    sent(wof.at[:, pl.ds(0, 3 * L)], 0)
    sent(sgath.at[7], 23)
    sent(wd.at[pl.ds(0, Y - 1)], 8)
    sent(r4.at[pl.ds(0, T - 1)], 9)
    sent(mgath.at[pl.ds(0, PL - 1)], 10)
    sent(r6.at[pl.ds(0, Z - 1)], 11)
    sent(sq.at[pl.ds(0, Z - 1)], 12)
    sent(hall7.at[pl.ds(0, Z - 1)], 13)
    got(r8.at[pl.ds(0, PL - 1)], 14)
    parts = [r8[j].astype(F32) for j in range(4)]
    for j in range(4, PL):
        parts[j % 4] = parts[j % 4] + r8[j].astype(F32)
    mixed = (parts[0] + parts[1]) + (parts[2] + parts[3])
    final = middle + mixed * (factor2 * factor2)
    out_ref[...] = final.astype(BF16)
    sent(r8.at[pl.ds(0, PL - 1)], 14)


def hand_over(layer_in, state_in, layer_ref, state_ref, sems):
    copies = [pltpu.make_async_copy(layer_in, layer_ref, sems.at[4])]
    for r in range(ROWS):
        copies.append(pltpu.make_async_copy(state_in.at[r], state_ref.at[r], sems.at[r]))
    for c in copies:
        c.start()
    for c in copies:
        c.wait()


def shards(
    Z,
    T,
    stream,
    memory_state,
    attn_gain,
    query_weight,
    key_weight,
    value_weight,
    outgate_weight,
    beta_weight,
    decay_weight,
    decay_log,
    decay_shift,
    head_gain,
    output_weight,
    mixer_gain,
    up_weight,
    down_weight,
):
    N, PL, B, DT = Z * Y, Y * T, Z * Y * ROWS, L // T
    hbm = pl.BlockSpec(memory_space=pltpu.HBM)
    anywhere = pl.BlockSpec(memory_space=pl.ANY)
    vmem = pl.BlockSpec(memory_space=pltpu.VMEM)
    layer_out, memory_next = pl.pallas_call(
        functools.partial(layer_kernel, Z, T),
        out_shape=(
            pltpu.VMEM((DT, B), BF16),
            pltpu.VMEM(memory_state.shape, F32),
        ),
        in_specs=[hbm] * 16,
        out_specs=(vmem, vmem),
        scratch_shapes=[
            pltpu.VMEM((DT, B), BF16),
            pltpu.VMEM((1, L), F32),
            pltpu.VMEM((1, L), F32),
            pltpu.VMEM((1, L), F32),
            pltpu.VMEM((HEADS_DEV, L), BF16),
            pltpu.VMEM((HEADS_DEV, L), BF16),
            pltpu.SMEM((HEADS_DEV,), F32),
            pltpu.SMEM((HEADS_DEV,), F32),
            pltpu.VMEM((ROWS, HEADS_DEV, L, L), F32),
            pltpu.VMEM((4, L, 4 * L), BF16),
            pltpu.VMEM((4 * L, 4 * L), BF16),
            pltpu.VMEM((8, 8, L), F32),
            pltpu.VMEM((4, 16, L), BF16),
            pltpu.VMEM((8, T, DT, B), BF16),
            pltpu.VMEM((2, 4, L, 2 * L), BF16),
            pltpu.VMEM((Z, 16, B), F32),
            pltpu.VMEM((N // 2, 2, 16, L), BF16),
            pltpu.VMEM((N, 16, L), BF16),
            pltpu.VMEM((2, 16, L), F32),
            pltpu.VMEM((Z, 16, L), BF16),
            pltpu.VMEM((Z // 2, 2, 16, L), BF16),
            pltpu.VMEM((T, 16, L), BF16),
            pltpu.VMEM((N, 16, L), BF16),
            pltpu.VMEM((Y, L, 4 * L), BF16),
            pltpu.VMEM((Y, 4 * L, L), BF16),
            pltpu.VMEM((Z, 8, B), F32),
            pltpu.VMEM((Z, 4 * L // Z, B), BF16),
            pltpu.VMEM((Z, 4 * L // Z, B), BF16),
            pltpu.VMEM((Z, 4 * L // Z, B), BF16),
            pltpu.VMEM((PL, DT, B), BF16),
            pltpu.VMEM((PL, DT, B), BF16),
            pltpu.VMEM((4 * L, 4 * L), BF16),
            pltpu.VMEM((4 * L, 4 * L), BF16),
            pltpu.VMEM((Y, 8, L), F32),
            pltpu.VMEM((Y, B, L), BF16),
            pltpu.SemaphoreType.DMA((24,)),
            pltpu.SemaphoreType.DMA((24,)),
            pltpu.SemaphoreType.DMA((24,)),
        ],
        compiler_params=pltpu.CompilerParams(
            collective_id=0,
            has_side_effects=True,
            vmem_limit_bytes=67043328 - memory_state.size * 4 - 8192,
        ),
    )(
        stream.T,
        attn_gain.reshape(1, L),
        mixer_gain.reshape(1, L),
        head_gain.reshape(1, L),
        beta_weight.T,
        decay_weight.T,
        decay_log,
        decay_shift,
        memory_state,
        query_weight,
        key_weight,
        value_weight,
        outgate_weight,
        output_weight,
        up_weight,
        down_weight,
    )
    layer_out, memory_next = pl.pallas_call(
        hand_over,
        out_shape=(
            jax.ShapeDtypeStruct((DT, B), BF16),
            jax.ShapeDtypeStruct(memory_state.shape, F32),
        ),
        in_specs=[anywhere] * 2,
        out_specs=(hbm, hbm),
        scratch_shapes=[pltpu.SemaphoreType.DMA((5,))],
        compiler_params=pltpu.CompilerParams(vmem_limit_bytes=2**20),
    )(layer_out, memory_next)
    return layer_out.T, memory_next


def solution(mesh):
    in_specs = (
        P(None, ("kv", "tp")),
        P("kv", "tp", None, None),
        P("kv"),
        P("kv", "tp"),
        P("kv", "tp"),
        P("kv", "tp"),
        P("kv", "tp"),
        P("kv", "tp"),
        P("kv", "tp"),
        P("tp"),
        P("tp"),
        P(),
        P("tp", "kv"),
        P("kv"),
        P("kv", "tp"),
        P("tp", "kv"),
    )
    out_specs = (P(None, ("kv", "tp")), P("kv", "tp", None, None))
    body = functools.partial(shards, mesh.shape["kv"] // Y, mesh.shape["tp"])
    return jax.shard_map(body, mesh=mesh, in_specs=in_specs, out_specs=out_specs, check_vma=False)
```

```python
import functools

import jax
import jax.numpy as jnp
from jax import lax
from jax.experimental import pallas as pl
from jax.experimental.pallas import tpu as pltpu
from jax.sharding import PartitionSpec as P

MESH = pl.DeviceIdType.MESH
F32 = jnp.float32
BF16 = jnp.bfloat16
EPS = 1e-06
Y = 4
L = 128
HEADS_DEV = 4
ROWS = 4


def transposed(x):
    return jnp.transpose(x, (1, 0))


def silu(x):
    return x * jax.nn.sigmoid(x)


def added(parts):
    while len(parts) > 1:
        parts = [a + b for a, b in zip(parts[::2], parts[1::2])] + parts[len(parts) // 2 * 2 :]
    return parts[0]


def softplus(x):
    return jnp.maximum(x, 0.0) + jnp.log1p(jnp.exp(-jnp.abs(x)))


def layer_kernel(
    Z,
    T,
    stream_hbm,
    attn_gain_hbm,
    mixer_gain_hbm,
    head_gain_hbm,
    beta_hbm,
    decay_hbm,
    decay_log_hbm,
    decay_shift_hbm,
    state_ref,
    wq_ref,
    wk_ref,
    wv_ref,
    wg_ref,
    wo_ref,
    wu_ref,
    wd_ref,
    out_ref,
    next_ref,
    stream_ref,
    attn_gain_ref,
    mixer_gain_ref,
    head_gain_ref,
    beta_ref,
    decay_ref,
    decay_log_ref,
    decay_shift_ref,
    state,
    w_in,
    wof,
    gpos,
    etile,
    sgath,
    w1,
    xz,
    s2,
    r2,
    rows_f,
    hall,
    a4,
    r4,
    mgath,
    wu,
    wd,
    sq,
    u6,
    r6,
    hall7,
    d8,
    r8,
    wut,
    wdt,
    gmix,
    mids,
    all_sent,
    lsem,
    ssem,
    rsem,
):
    N = Z * Y
    PL = Y * T
    B = N * ROWS
    DT = L // T
    D = N * L
    kv = lax.axis_index("kv")
    tp = lax.axis_index("tp")
    z = lax.div(kv, Y)
    y = lax.rem(kv, Y)
    me_p = y * T + tp
    pz, py = lax.rem(z, 2), lax.rem(y, 2)
    za, zb = z + 1 - 2 * pz, lax.rem(z - 1 + 2 * pz + Z, Z)
    ya, yb = y + 1 - 2 * py, lax.rem(y - 1 + 2 * py + Y, Y)
    spots = [kv, za * Y + y, z * Y + ya, za * Y + ya, zb * Y + y, z * Y + yb, zb * Y + yb]
    spot_far = z * Y + lax.rem(y + 2, Y)
    head_a = pz * 2 + py
    heads_a = [head_a, (1 - pz) * 2 + py, pz * 2 + 1 - py, (1 - pz) * 2 + 1 - py]
    groups = ((0, (0, 1, 2, 3)), (1, (0, 4, 5, 6)))
    tps = [lax.rem(tp + i, T) for i in range(T)]

    def plane_dev(p):
        return (z * Y + lax.div(p, T), lax.rem(p, T))

    def kv_dev(p):
        return (p, tp)

    def each_peer(n, me, act):
        def step(i, c):
            off = 1 + lax.rem(i + (n // 2 - 1), n - 1)
            act(lax.rem(me + off, n))
            return c

        lax.fori_loop(0, n - 1, step, 0)

    def put(src, dst, k, dev):
        pltpu.make_async_remote_copy(
            src_ref=src,
            dst_ref=dst,
            send_sem=ssem,
            recv_sem=rsem.at[k],
            device_id=dev,
            device_id_type=MESH,
        ).start()

    def got(ref, k):
        with jax.named_scope(f"got{k}"):
            pltpu.make_async_copy(ref, ref, rsem.at[k]).wait()


    loads = [
        pltpu.make_async_copy(w, w_in.at[m], lsem.at[0])
        for m, w in enumerate((wq_ref, wk_ref, wv_ref, wg_ref))
    ]
    small = [
        pltpu.make_async_copy(a, b, lsem.at[3 + i])
        for i, (a, b) in enumerate((
            (stream_hbm, stream_ref),
            (attn_gain_hbm, attn_gain_ref),
            (mixer_gain_hbm, mixer_gain_ref),
            (beta_hbm, beta_ref),
            (decay_hbm, decay_ref),
        ))
    ]
    late = [
        pltpu.make_async_copy(a, b, lsem.at[3 + i])
        for i, (a, b) in enumerate((
            (head_gain_hbm, head_gain_ref),
            (decay_log_hbm, decay_log_ref),
            (decay_shift_hbm, decay_shift_ref),
        ))
    ]
    for c in small:
        c.start()
    own_out = wof.at[:, pl.ds(pl.multiple_of(y * L, L), L)]
    load_out = pltpu.make_async_copy(wo_ref, own_out, lsem.at[1])
    load_state = pltpu.make_async_copy(state_ref, state, lsem.at[2])
    for c in loads:
        c.start()
    load_out.start()
    load_state.start()

    barrier = pltpu.get_barrier_semaphore()

    def greet(dev):
        pl.semaphore_signal(barrier, inc=1, device_id=dev, device_id_type=MESH)

    with jax.named_scope("greet"):
        for dst in reversed(spots[1:]):
            for t in tps:
                greet((dst, t))
        for off in (4, 3, 5, 2, 6):
            greet((lax.rem(z + off, Z) * Y + y, tp))
        greet((spot_far, tp))
        for t in tps[1:]:
            greet((kv, t))

    for c in small:
        c.wait()
    for c in late:
        c.start()
    gpos[0] = jnp.broadcast_to(attn_gain_ref[...], (8, L))
    gpos[0, 1:2, :] = mixer_gain_ref[...]
    etile[0] = jnp.concatenate(
        [beta_ref[...].astype(F32), decay_ref[...].astype(F32), jnp.zeros((8, L), F32)], axis=0
    ).astype(BF16)
    sgath[0, tp] = stream_ref[...]

    with jax.named_scope("greeted"):
        pl.semaphore_wait(barrier, 7 * T - 1 + (Z - 3) + 1)

    put(gpos.at[0], gpos.at[7], 1, (spot_far, tp))
    for k in (3, 6, 1, 2, 4, 5):
        put(gpos.at[0], gpos.at[k], 1, (spots[k], tp))
        if k < 4:
            put(etile.at[0], etile.at[k], 2, (spots[k], tp))
    for k in (3, 6, 1, 2, 4, 5):
        for i in (4, 3, 5, 2, 6, 1, 7, 0):
            put(sgath.at[0, tp], sgath.at[k, tp], (16 if k < 4 else 17), (spots[k], tps[i]))
    for i in (4, 3, 5, 2, 6, 1, 7):
        put(sgath.at[0, tp], sgath.at[0, tp], 15, (kv, tps[i]))
    pltpu.make_async_copy(w_in, w_in, lsem.at[0]).wait()

    def head_cols(m, h):
        return w_in.at[m, :, pl.ds(pl.multiple_of(h * L, L), L)]

    def send_weights(g):
        members = groups[g][1]
        for slot in (3, 1, 2):
            h = heads_a[slot]
            h = h if g == 0 else 3 - h
            for i in range(2):
                put(
                    head_cols(2 * g + i, h),
                    w1.at[g, slot, :, pl.ds(i * L, L)],
                    3 if g == 0 else 19,
                    (spots[members[slot]], tp),
                )

    send_weights(0)
    for g in range(2):
        for i in range(2):
            pltpu.make_async_copy(
                head_cols(2 * g + i, head_a if g == 0 else 3 - head_a),
                w1.at[g, 0, :, pl.ds(i * L, L)],
                lsem.at[0],
            ).start()
    send_weights(1)
    got(gpos.at[pl.ds(1, 7)], 1)
    got(etile.at[pl.ds(1, 3)], 2)
    x_part = jnp.zeros((16, B), F32)
    squares = jnp.zeros((1, B), F32)
    scaled = {}
    for k in (0, 1, 2, 3, 4, 5, 6):
        if k == 0:
            got(sgath.at[0, pl.ds(0, T - 1)], 15)
        elif k == 1:
            got(sgath.at[pl.ds(1, 3)], 16)
        elif k == 4:
            got(sgath.at[pl.ds(4, 3)], 17)
        block = sgath[k].astype(F32).reshape(L, B)
        part = (transposed(block) * gpos[k, 0:1, :]).astype(BF16)
        scaled[k] = part
        if k < 4:
            squares = squares + jnp.sum(block * block, axis=0, keepdims=True)
            x_part = x_part + lax.dot_general(
                etile[k], part, (((1,), (1,)), ((), ())), preferred_element_type=F32
            )
        if k == 3:
            row16 = lax.broadcasted_iota(jnp.int32, (16, B), 0)
            xslot = lax.div(z, 2) * (Y // 2) + lax.div(y, 2)
            xz[xslot] = jnp.where(row16 == 8, squares, x_part).astype(BF16)
            for i in (2, 1, 3, 0):
                for j in (1, 0):
                    if i or j:
                        zz, yy = lax.rem(z + 2 * i, Z), lax.rem(y + 2 * j, Y)
                        put(xz.at[xslot], xz.at[xslot], 4, (zz * Y + yy, tp))

    pltpu.make_async_copy(w1.at[:, 0], w1.at[:, 0], lsem.at[0]).wait()
    proj = []
    for g, members in groups:
        got(w1.at[g, pl.ds(1, 3)], 3 if g == 0 else 19)
        total = jnp.zeros((B, 2 * L), F32)
        for slot, k in enumerate(members):
            total = total + jnp.dot(scaled[k], w1[g, slot], preferred_element_type=F32)
        proj += [total[:, 0:L], total[:, L : 2 * L]]
    def pair_tiles(a, b):
        low = lax.broadcasted_iota(jnp.int32, a.shape, 1) < 4
        return (
            jnp.where(low, a, pltpu.roll(b, 4, 1)),
            jnp.where(low, pltpu.roll(a, 4, 1), b),
        )

    pq, pk, pv, pg = [p.reshape(B // 8, 8, L) for p in proj]
    even_a, odd_a = pair_tiles(pq, pk)
    even_b, odd_b = pair_tiles(pv, pg)
    s2[:, 0] = jnp.concatenate([even_a, even_b], axis=1).astype(BF16)
    s2[:, 1] = jnp.concatenate([odd_a, odd_b], axis=1).astype(BF16)
    each_peer(
        N, kv, lambda p: put(s2.at[lax.div(p, 2), lax.rem(p, 2)], r2.at[kv], 5, kv_dev(p))
    )
    r2[kv] = s2[lax.div(kv, 2), lax.rem(kv, 2)]

    for t in tps:
        put(sgath.at[0, tp], sgath.at[7, tp], 18, (spot_far, t))
    for off in (2, 1, 3):
        put(wo_ref, own_out, 0, (z * Y + lax.rem(y + off, Y), tp))

    for c in late:
        c.wait()
    got(xz.at[pl.ds(0, Z - 1)], 4)
    x_all = added([xz[j].astype(F32) for j in range(Z)])
    fac = lax.rsqrt(x_all[8:9] / D + EPS)
    xf = x_all * fac
    dlog = jnp.zeros((16, B), F32)
    dshift = jnp.zeros((16, B), F32)
    for h in range(HEADS_DEV):
        dlog = jnp.where(row16 == 4 + h, decay_log_ref[h], dlog)
        dshift = jnp.where(row16 == 4 + h, decay_shift_ref[h], dshift)
    scal = jnp.where(
        row16 < 4,
        jax.nn.sigmoid(xf),
        jnp.where(row16 < 8, jnp.exp(-jnp.exp(dlog) * softplus(xf + dshift)), fac),
    )
    lane_group = lax.div(lax.broadcasted_iota(jnp.int32, (16, B), 1), 4)
    mine = jnp.zeros((16, B), F32)
    for m in range(4):
        rolled = pltpu.roll(scal, lax.rem(B + m * ROWS - kv * ROWS, B), 1)
        mine = jnp.where(lane_group == m, rolled, mine)
    cols = transposed(jnp.concatenate([mine, jnp.zeros((L - 16, B), F32)], axis=0))[0:16]

    head_of = lax.div(lax.broadcasted_iota(jnp.int32, (16, L), 0), 4)
    lane16 = lax.broadcasted_iota(jnp.int32, (16, L), 1)
    beta16 = jnp.sum(jnp.where(lane16 == head_of, cols, 0.0), axis=1, keepdims=True)
    decay16 = jnp.sum(jnp.where(lane16 == 4 + head_of, cols, 0.0), axis=1, keepdims=True)

    got(r2.at[pl.ds(0, N - 1)], 5)
    load_state.wait()
    row_id = lax.broadcasted_iota(jnp.int32, (16, 1), 0)
    acts = []
    for h in range(HEADS_DEV):
        here = [
            [n for n in range(N) if (n // Y % 2) * 2 + n % 2 == want] for want in (h, 3 - h)
        ]
        qk = [r2[n, 0:8, :].astype(F32) for n in here[0]]
        vg = [r2[n, 8:16, :].astype(F32) for n in here[1]]
        total = jnp.concatenate([added(qk), added(vg)], axis=0)
        a = silu(total * cols[:, 8:9])
        inv = lax.rsqrt(jnp.sum(a * a, axis=1, keepdims=True) + EPS)
        norm = jnp.where(row_id < 4, inv * L ** (-0.5), jnp.where(row_id < 8, inv, 1.0))
        acts.append(a * norm)
        for n, lo in ((0, 0), (1, 4), (2, 8), (3, 12)):
            rows_f[n, 4 * h : 4 * h + 4, :] = acts[h][lo : lo + 4]
    flipped = transposed(jnp.concatenate(acts + [jnp.zeros((L - 64, L), F32)], axis=0))
    pieces = [(h, r) for h in range(HEADS_DEV) for r in range(ROWS)]
    for h, r in pieces:
        at = h * 16 + r
        own = state[r, h]
        row = 4 * h + r
        rows_f[4, row : row + 1, :] = jnp.sum(
            own * flipped[:, at : at + 1], axis=0, keepdims=True
        )
        rows_f[5, row : row + 1, :] = jnp.sum(
            own * flipped[:, at + 4 : at + 5], axis=0, keepdims=True
        )
    corr = beta16 * (rows_f[2] - decay16 * rows_f[5])
    along = jnp.sum(rows_f[0] * rows_f[1], axis=1, keepdims=True)
    readout = decay16 * rows_f[4] + along * corr
    readout = readout * lax.rsqrt(jnp.mean(readout * readout, axis=1, keepdims=True) + EPS)
    hall[z] = (readout * head_gain_ref[...] * rows_f[3]).astype(BF16)

    offs = (4, 3, 5, 2, 6, 1, 7)
    for off in offs:
        put(hall.at[z], hall.at[z], 7, (lax.rem(z + off, Z) * Y + y, tp))

    def up_cols(yy):
        return wu_ref.at[:, pl.ds(pl.multiple_of(yy * 4 * L, L), 4 * L)]

    own_up = pltpu.make_async_copy(up_cols(y), wu.at[y], lsem.at[0])
    own_up.start()
    for off in (2, 1, 3):
        yy = lax.rem(y + off, Y)
        put(up_cols(yy), wu.at[y], 6, (z * Y + yy, tp))

    for h, r in pieces:
        row = 4 * h + r
        at = h * 16 + 4 + r
        next_ref[r, h] = (
            state[r, h] * decay16[row : row + 1] + flipped[:, at : at + 1] * corr[row : row + 1]
        )

    got(sgath.at[7], 18)
    row_mid = (tp * Y + y) * ROWS
    sel_row = lax.broadcasted_iota(jnp.int32, (16, B), 0)
    sel_lane = lax.broadcasted_iota(jnp.int32, (16, B), 1)
    mid = jnp.zeros((16, L), F32)
    for slot, yy in ((0, y), (2, ya), (5, yb), (7, lax.rem(y + 2, Y))):
        gmix[yy] = gpos[slot]
        pick = (lax.div(sel_row, 4) == yy) & (sel_lane == row_mid + lax.rem(sel_row, 4))
        mid = mid + lax.dot_general(
            jnp.where(pick, 1.0, 0.0).astype(BF16),
            sgath[slot].reshape(L, B),
            (((1,), (1,)), ((), ())),
            preferred_element_type=F32,
        )
    load_out.wait()
    got(wof.at[:, pl.ds(0, 3 * L)], 0)

    got(hall.at[pl.ds(0, Z - 1)], 7)
    heads = hall[...].astype(F32).reshape(Z // 2, 2, 2, 8, L)
    attn = jnp.zeros((Z * ROWS, 4 * L), F32)
    for c in range(2):
        h_even, h_odd = pair_tiles(heads[:, 0, c], heads[:, 1, c])
        for i, hh in ((2 * c, h_even), (2 * c + 1, h_odd)):
            attn = attn + jnp.dot(
                hh.reshape(Z * ROWS, L).astype(BF16),
                wof[i * L : (i + 1) * L, :],
                preferred_element_type=F32,
            )
    a_d = [attn[:, d * L : (d + 1) * L].reshape(Z // 2, 8, L) for d in range(4)]
    even_a, odd_a = pair_tiles(a_d[0], a_d[1])
    even_b, odd_b = pair_tiles(a_d[2], a_d[3])
    a4[:, 0] = jnp.concatenate([even_a, even_b], axis=1).astype(BF16)
    a4[:, 1] = jnp.concatenate([odd_a, odd_b], axis=1).astype(BF16)
    for i in offs:
        put(a4.at[lax.div(tps[i], 2), lax.rem(tps[i], 2)], r4.at[tp], 9, (kv, tps[i]))
    r4[tp] = a4[lax.div(tp, 2), lax.rem(tp, 2)]
    got(r4.at[pl.ds(0, T - 1)], 9)
    mid = mid + added([r4[j].astype(F32) for j in range(T)])

    slot_mid = tp * Y + y
    mgath[slot_mid] = mid.astype(BF16)
    each_peer(
        PL, me_p, lambda p: put(mgath.at[slot_mid], mgath.at[slot_mid], 10, plane_dev(p))
    )
    own_up.wait()
    got(wu.at[pl.ds(0, Y - 1)], 6)
    for j in range(Y):
        for i in range(4):
            wut[i * L : (i + 1) * L, j * L : (j + 1) * L] = transposed(
                wu[j, :, i * L : (i + 1) * L].astype(F32)
            ).astype(BF16)
    got(mgath.at[pl.ds(0, PL - 1)], 10)
    pairs = mgath[...].astype(F32).reshape(N // 2, 2, 2, 8, L)
    up = jnp.zeros((4 * L, B), F32)
    middles = []
    for c in range(2):
        middles += pair_tiles(pairs[:, 0, c], pairs[:, 1, c])
    middles = [m.reshape(B, L) for m in middles]
    for d in range(Y):
        up = up + lax.dot_general(
            wut[:, d * L : (d + 1) * L],
            (middles[d] * gmix[d, 1:2, :]).astype(BF16),
            (((1,), (1,)), ((), ())),
            preferred_element_type=F32,
        )
    u6[...] = up.astype(BF16).reshape(Z, 4 * L // Z, B)
    for zz in (4, 3, 5, 2, 6, 1, 7, 0):
        @pl.when(z != zz)
        def _(zz=zz):
            put(u6.at[zz], r6.at[z], 11, (zz * Y + y, tp))

    r6[z] = u6[z]
    def down_rows(yy):
        return wd_ref.at[pl.ds(pl.multiple_of(yy * 4 * L, L), 4 * L), :]

    own_down = pltpu.make_async_copy(down_rows(y), wd.at[y], lsem.at[0])
    own_down.start()
    for off in (2, 1, 3):
        yy = lax.rem(y + off, Y)
        put(down_rows(yy), wd.at[y], 8, (z * Y + yy, tp))

    squares2 = jnp.zeros((8, B), F32)
    for d in range(Y):
        mids[d] = middles[d].astype(BF16)
        squares2 = squares2 + lax.dot_general(
            jnp.ones((8, L), F32),
            middles[d] * middles[d],
            (((1,), (1,)), ((), ())),
            preferred_element_type=F32,
            precision=lax.Precision.HIGHEST,
        )
    sq[z] = squares2
    own_row = lax.broadcasted_iota(jnp.int32, (DT, L), 0) + tp * DT
    own_lane = lax.broadcasted_iota(jnp.int32, (DT, L), 1)
    middle = lax.dot_general(
        jnp.where(own_row == own_lane, 1.0, 0.0).astype(BF16),
        mids[y],
        (((1,), (1,)), ((), ())),
        preferred_element_type=F32,
    )
    got(r6.at[pl.ds(0, Z - 1)], 11)
    up_mine = r6[0].astype(F32)
    for j in range(1, Z):
        up_mine = up_mine + r6[j].astype(F32)
    hidden = jnp.square(jnp.maximum(up_mine, 0.0)).astype(BF16)
    hall7[z] = hidden
    for ref, k in ((hall7, 13), (sq, 12)):
        for zz in range(Z):
            @pl.when(z != zz)
            def _(ref=ref, k=k, zz=zz):
                put(ref.at[z], ref.at[z], k, (zz * Y + y, tp))

    own_down.wait()
    got(wd.at[pl.ds(0, Y - 1)], 8)
    for j in range(Y):
        for i in range(4):
            wdt[j * L : (j + 1) * L, i * L : (i + 1) * L] = transposed(
                wd[j, i * L : (i + 1) * L, :].astype(F32)
            ).astype(BF16)
    got(hall7.at[pl.ds(0, Z - 1)], 13)
    hid = hall7[...].reshape(4 * L, B)
    for yy in (0, 1, 3, 2):
        down = jnp.dot(wdt[yy * L : (yy + 1) * L, :], hid, preferred_element_type=F32)
        d8[yy * T : (yy + 1) * T] = down.reshape(T, DT, B).astype(BF16)
        for t in (1, 0, 3, 2, 7, 6, 5, 4):
            @pl.when(me_p != yy * T + t)
            def _(yy=yy, t=t):
                put(d8.at[yy * T + t], r8.at[me_p], 14, (z * Y + yy, t))

    r8[me_p] = d8[me_p]
    got(sq.at[pl.ds(0, Z - 1)], 12)
    total2 = sq[0, 0:1, :]
    for j in range(1, Z):
        total2 = total2 + sq[j, 0:1, :]
    factor2 = lax.rsqrt(total2 / D + EPS)
    got(r8.at[pl.ds(0, PL - 1)], 14)
    parts = [r8[j].astype(F32) for j in range(4)]
    for j in range(4, PL):
        parts[j % 4] = parts[j % 4] + r8[j].astype(F32)
    mixed = (parts[0] + parts[1]) + (parts[2] + parts[3])
    final = middle + mixed * (factor2 * factor2)
    out_ref[...] = final.astype(BF16)
    pltpu.make_async_copy(all_sent, all_sent, ssem).wait()


def hand_over(layer_in, state_in, layer_ref, state_ref, sems):
    copies = [pltpu.make_async_copy(layer_in, layer_ref, sems.at[4])]
    for r in range(ROWS):
        copies.append(pltpu.make_async_copy(state_in.at[r], state_ref.at[r], sems.at[r]))
    for c in copies:
        c.start()
    for c in copies:
        c.wait()


def shards(
    Z,
    T,
    stream,
    memory_state,
    attn_gain,
    query_weight,
    key_weight,
    value_weight,
    outgate_weight,
    beta_weight,
    decay_weight,
    decay_log,
    decay_shift,
    head_gain,
    output_weight,
    mixer_gain,
    up_weight,
    down_weight,
):
    N, PL, B, DT = Z * Y, Y * T, Z * Y * ROWS, L // T
    sent_tiles = (
        3 * 3 * 32
        + 12 * 8
        + 7 + 3
        + 7 * 8 - 1 + 8
        + 7 + (N - 1)
        + (Z - 1) + (T - 1) + (PL - 1)
        + 2 * 4 * (Z - 1) + (Z - 1)
        + (PL - 1)
    )
    hbm = pl.BlockSpec(memory_space=pltpu.HBM)
    anywhere = pl.BlockSpec(memory_space=pl.ANY)
    vmem = pl.BlockSpec(memory_space=pltpu.VMEM)
    layer_out, memory_next = pl.pallas_call(
        functools.partial(layer_kernel, Z, T),
        out_shape=(
            pltpu.VMEM((DT, B), BF16),
            pltpu.VMEM(memory_state.shape, F32),
        ),
        in_specs=[hbm] * 16,
        out_specs=(vmem, vmem),
        scratch_shapes=[
            pltpu.VMEM((DT, B), BF16),
            pltpu.VMEM((1, L), F32),
            pltpu.VMEM((1, L), F32),
            pltpu.VMEM((1, L), F32),
            pltpu.VMEM((HEADS_DEV, L), BF16),
            pltpu.VMEM((HEADS_DEV, L), BF16),
            pltpu.SMEM((HEADS_DEV,), F32),
            pltpu.SMEM((HEADS_DEV,), F32),
            pltpu.VMEM((ROWS, HEADS_DEV, L, L), F32),
            pltpu.VMEM((4, L, 4 * L), BF16),
            pltpu.VMEM((4 * L, 4 * L), BF16),
            pltpu.VMEM((8, 8, L), F32),
            pltpu.VMEM((4, 16, L), BF16),
            pltpu.VMEM((8, T, DT, B), BF16),
            pltpu.VMEM((2, 4, L, 2 * L), BF16),
            pltpu.VMEM((Z, 16, B), BF16),
            pltpu.VMEM((N // 2, 2, 16, L), BF16),
            pltpu.VMEM((N, 16, L), BF16),
            pltpu.VMEM((6, 16, L), F32),
            pltpu.VMEM((Z, 16, L), BF16),
            pltpu.VMEM((Z // 2, 2, 16, L), BF16),
            pltpu.VMEM((T, 16, L), BF16),
            pltpu.VMEM((N, 16, L), BF16),
            pltpu.VMEM((Y, L, 4 * L), BF16),
            pltpu.VMEM((Y, 4 * L, L), BF16),
            pltpu.VMEM((Z, 8, B), F32),
            pltpu.VMEM((Z, 4 * L // Z, B), BF16),
            pltpu.VMEM((Z, 4 * L // Z, B), BF16),
            pltpu.VMEM((Z, 4 * L // Z, B), BF16),
            pltpu.VMEM((PL, DT, B), BF16),
            pltpu.VMEM((PL, DT, B), BF16),
            pltpu.VMEM((4 * L, 4 * L), BF16),
            pltpu.VMEM((4 * L, 4 * L), BF16),
            pltpu.VMEM((Y, 8, L), F32),
            pltpu.VMEM((Y, B, L), BF16),
            pltpu.VMEM((sent_tiles, 16, L), BF16),
            pltpu.SemaphoreType.DMA((8,)),
            pltpu.SemaphoreType.DMA,
            pltpu.SemaphoreType.DMA((20,)),
        ],
        compiler_params=pltpu.CompilerParams(
            collective_id=0,
            has_side_effects=True,
            vmem_limit_bytes=67043328 - memory_state.size * 4 - 8192,
        ),
    )(
        stream.T,
        attn_gain.reshape(1, L),
        mixer_gain.reshape(1, L),
        head_gain.reshape(1, L),
        beta_weight.T,
        decay_weight.T,
        decay_log,
        decay_shift,
        memory_state,
        query_weight,
        key_weight,
        value_weight,
        outgate_weight,
        output_weight,
        up_weight,
        down_weight,
    )
    layer_out, memory_next = pl.pallas_call(
        hand_over,
        out_shape=(
            jax.ShapeDtypeStruct((DT, B), BF16),
            jax.ShapeDtypeStruct(memory_state.shape, F32),
        ),
        in_specs=[anywhere] * 2,
        out_specs=(hbm, hbm),
        scratch_shapes=[pltpu.SemaphoreType.DMA((5,))],
        compiler_params=pltpu.CompilerParams(vmem_limit_bytes=2**20),
    )(layer_out, memory_next)
    return layer_out.T, memory_next


def solution(mesh):
    in_specs = (
        P(None, ("kv", "tp")),
        P("kv", "tp", None, None),
        P("kv"),
        P("kv", "tp"),
        P("kv", "tp"),
        P("kv", "tp"),
        P("kv", "tp"),
        P("kv", "tp"),
        P("kv", "tp"),
        P("tp"),
        P("tp"),
        P(),
        P("tp", "kv"),
        P("kv"),
        P("kv", "tp"),
        P("tp", "kv"),
    )
    out_specs = (P(None, ("kv", "tp")), P("kv", "tp", None, None))
    body = functools.partial(shards, mesh.shape["kv"] // Y, mesh.shape["tp"])
    return jax.shard_map(body, mesh=mesh, in_specs=in_specs, out_specs=out_specs, check_vma=False)
```

```python
import functools

import jax
import jax.numpy as jnp
from jax import lax
from jax.experimental import pallas as pl
from jax.experimental.pallas import tpu as pltpu
from jax.sharding import PartitionSpec as P

MESH = pl.DeviceIdType.MESH
F32 = jnp.float32
BF16 = jnp.bfloat16
EPS = 1e-06
Y = 4
L = 128
HEADS_DEV = 4
ROWS = 4


def transposed(x):
    return jnp.transpose(x, (1, 0))


def silu(x):
    return x * jax.nn.sigmoid(x)


def added(parts):
    while len(parts) > 1:
        parts = [a + b for a, b in zip(parts[::2], parts[1::2])] + parts[len(parts) // 2 * 2 :]
    return parts[0]


def softplus(x):
    return jnp.maximum(x, 0.0) + jnp.log1p(jnp.exp(-jnp.abs(x)))


def layer_kernel(
    Z,
    T,
    stream_hbm,
    attn_gain_hbm,
    mixer_gain_hbm,
    head_gain_hbm,
    beta_hbm,
    decay_hbm,
    decay_log_hbm,
    decay_shift_hbm,
    state_ref,
    wq_ref,
    wk_ref,
    wv_ref,
    wg_ref,
    wo_ref,
    wu_ref,
    wd_ref,
    out_ref,
    next_ref,
    stream_ref,
    attn_gain_ref,
    mixer_gain_ref,
    head_gain_ref,
    beta_ref,
    decay_ref,
    decay_log_ref,
    decay_shift_ref,
    state,
    w_in,
    wof,
    gpos,
    etile,
    sgath,
    w1,
    xz,
    s2,
    r2,
    rows_f,
    hall,
    a4,
    r4,
    mgath,
    wu,
    wd,
    sq,
    u6,
    r6,
    hall7,
    d8,
    r8,
    wut,
    wdt,
    gmix,
    mids,
    all_sent,
    lsem,
    ssem,
    rsem,
):
    N = Z * Y
    PL = Y * T
    B = N * ROWS
    DT = L // T
    D = N * L
    kv = lax.axis_index("kv")
    tp = lax.axis_index("tp")
    z = lax.div(kv, Y)
    y = lax.rem(kv, Y)
    me_p = y * T + tp
    pz, py = lax.rem(z, 2), lax.rem(y, 2)
    za, zb = z + 1 - 2 * pz, lax.rem(z - 1 + 2 * pz + Z, Z)
    ya, yb = y + 1 - 2 * py, lax.rem(y - 1 + 2 * py + Y, Y)
    spots = [kv, za * Y + y, z * Y + ya, za * Y + ya, zb * Y + y, z * Y + yb, zb * Y + yb]
    spot_far = z * Y + lax.rem(y + 2, Y)
    head_a = pz * 2 + py
    heads_a = [head_a, (1 - pz) * 2 + py, pz * 2 + 1 - py, (1 - pz) * 2 + 1 - py]
    groups = ((0, (0, 1, 2, 3)), (1, (0, 4, 5, 6)))
    tps = [lax.rem(tp + i, T) for i in range(T)]
    zs_ = [lax.rem(z + i, Z) for i in range(Z)]
    ys_ = [lax.rem(y + i, Y) for i in range(Y)]
    ys_half, ys_odd = [lax.div(v, 2) for v in ys_], [lax.rem(v, 2) for v in ys_]

    def put(src, dst, k, dev):
        pltpu.make_async_remote_copy(
            src_ref=src,
            dst_ref=dst,
            send_sem=ssem,
            recv_sem=rsem.at[k],
            device_id=dev,
            device_id_type=MESH,
        ).start()

    def got(ref, k):
        with jax.named_scope(f"got{k}"):
            pltpu.make_async_copy(ref, ref, rsem.at[k]).wait()


    loads = [
        pltpu.make_async_copy(w, w_in.at[m], lsem.at[0])
        for m, w in enumerate((wq_ref, wk_ref, wv_ref, wg_ref))
    ]
    small = [
        pltpu.make_async_copy(a, b, lsem.at[3 + i])
        for i, (a, b) in enumerate((
            (stream_hbm, stream_ref),
            (attn_gain_hbm, attn_gain_ref),
            (mixer_gain_hbm, mixer_gain_ref),
            (beta_hbm, beta_ref),
            (decay_hbm, decay_ref),
        ))
    ]
    late = [
        pltpu.make_async_copy(a, b, lsem.at[3 + i])
        for i, (a, b) in enumerate((
            (head_gain_hbm, head_gain_ref),
            (decay_log_hbm, decay_log_ref),
            (decay_shift_hbm, decay_shift_ref),
        ))
    ]
    for c in small:
        c.start()
    own_out = wof.at[:, pl.ds(pl.multiple_of(y * L, L), L)]
    load_out = pltpu.make_async_copy(wo_ref, own_out, lsem.at[1])
    load_state = pltpu.make_async_copy(state_ref, state, lsem.at[2])
    for c in loads:
        c.start()
    load_out.start()
    load_state.start()

    barrier = pltpu.get_barrier_semaphore()

    def greet(dev):
        pl.semaphore_signal(barrier, inc=1, device_id=dev, device_id_type=MESH)

    with jax.named_scope("greet"):
        for dst in reversed(spots[1:]):
            for t in tps:
                greet((dst, t))
        for off in (4, 3, 5, 2, 6):
            greet((lax.rem(z + off, Z) * Y + y, tp))
        greet((spot_far, tp))
        for t in tps[1:]:
            greet((kv, t))

    for c in small:
        c.wait()
    for c in late:
        c.start()
    gpos[0] = jnp.broadcast_to(attn_gain_ref[...], (8, L))
    gpos[0, 1:2, :] = mixer_gain_ref[...]
    etile[0] = jnp.concatenate(
        [beta_ref[...].astype(F32), decay_ref[...].astype(F32), jnp.zeros((8, L), F32)], axis=0
    ).astype(BF16)
    sgath[0, tp] = stream_ref[...]

    with jax.named_scope("greeted"):
        pl.semaphore_wait(barrier, 7 * T - 1 + (Z - 3) + 1)

    put(gpos.at[0], gpos.at[7], 1, (spot_far, tp))
    for k in (3, 6, 1, 2, 4, 5):
        put(gpos.at[0], gpos.at[k], 1, (spots[k], tp))
        if k < 4:
            put(etile.at[0], etile.at[k], 2, (spots[k], tp))
    for k in (3, 6, 1, 2, 4, 5):
        for i in (4, 3, 5, 2, 6, 1, 7, 0):
            put(sgath.at[0, tp], sgath.at[k, tp], (16 if k < 4 else 17), (spots[k], tps[i]))
    for i in (4, 3, 5, 2, 6, 1, 7):
        put(sgath.at[0, tp], sgath.at[0, tp], 15, (kv, tps[i]))
    pltpu.make_async_copy(w_in, w_in, lsem.at[0]).wait()

    def head_cols(m, h):
        return w_in.at[m, :, pl.ds(pl.multiple_of(h * L, L), L)]

    def send_weights(g):
        members = groups[g][1]
        for slot in (3, 1, 2):
            h = heads_a[slot]
            h = h if g == 0 else 3 - h
            for i in range(2):
                put(
                    head_cols(2 * g + i, h),
                    w1.at[g, slot, :, pl.ds(i * L, L)],
                    3 if g == 0 else 19,
                    (spots[members[slot]], tp),
                )

    send_weights(0)
    for g in range(2):
        for i in range(2):
            pltpu.make_async_copy(
                head_cols(2 * g + i, head_a if g == 0 else 3 - head_a),
                w1.at[g, 0, :, pl.ds(i * L, L)],
                lsem.at[0],
            ).start()
    send_weights(1)
    got(gpos.at[pl.ds(1, 7)], 1)
    got(etile.at[pl.ds(1, 3)], 2)
    x_part = jnp.zeros((16, B), F32)
    squares = jnp.zeros((1, B), F32)
    scaled = {}
    for k in (0, 1, 2, 3, 4, 5, 6):
        if k == 0:
            got(sgath.at[0, pl.ds(0, T - 1)], 15)
        elif k == 1:
            got(sgath.at[pl.ds(1, 3)], 16)
        elif k == 4:
            got(sgath.at[pl.ds(4, 3)], 17)
        block = sgath[k].astype(F32).reshape(L, B)
        part = (transposed(block) * gpos[k, 0:1, :]).astype(BF16)
        scaled[k] = part
        if k < 4:
            squares = squares + jnp.sum(block * block, axis=0, keepdims=True)
            x_part = x_part + lax.dot_general(
                etile[k], part, (((1,), (1,)), ((), ())), preferred_element_type=F32
            )
        if k == 3:
            row16 = lax.broadcasted_iota(jnp.int32, (16, B), 0)
            xslot = lax.div(z, 2) * (Y // 2) + lax.div(y, 2)
            xz[xslot] = jnp.where(row16 == 8, squares, x_part).astype(BF16)
            for i in (2, 1, 3, 0):
                for j in (1, 0):
                    if i or j:
                        zz, yy = lax.rem(z + 2 * i, Z), lax.rem(y + 2 * j, Y)
                        put(xz.at[xslot], xz.at[xslot], 4, (zz * Y + yy, tp))

    pltpu.make_async_copy(w1.at[:, 0], w1.at[:, 0], lsem.at[0]).wait()
    proj = []
    for g, members in groups:
        got(w1.at[g, pl.ds(1, 3)], 3 if g == 0 else 19)
        total = jnp.zeros((B, 2 * L), F32)
        for slot, k in enumerate(members):
            total = total + jnp.dot(scaled[k], w1[g, slot], preferred_element_type=F32)
        proj += [total[:, 0:L], total[:, L : 2 * L]]
    def pair_tiles(a, b):
        low = lax.broadcasted_iota(jnp.int32, a.shape, 1) < 4
        return (
            jnp.where(low, a, pltpu.roll(b, 4, 1)),
            jnp.where(low, pltpu.roll(a, 4, 1), b),
        )

    pq, pk, pv, pg = [p.reshape(B // 8, 8, L) for p in proj]
    even_a, odd_a = pair_tiles(pq, pk)
    even_b, odd_b = pair_tiles(pv, pg)
    s2[:, 0] = jnp.concatenate([even_a, even_b], axis=1).astype(BF16)
    s2[:, 1] = jnp.concatenate([odd_a, odd_b], axis=1).astype(BF16)
    for dz in (4, 3, 5, 2, 6, 1, 7, 0):
        for dy in (2, 1, 3, 0):
            if dz or dy:
                zz, yy = zs_[dz], ys_[dy]
                put(s2.at[2 * zz + ys_half[dy], ys_odd[dy]], r2.at[kv], 5, (zz * Y + yy, tp))
    r2[kv] = s2[lax.div(kv, 2), lax.rem(kv, 2)]

    for t in tps:
        put(sgath.at[0, tp], sgath.at[7, tp], 18, (spot_far, t))
    for off in (2, 1, 3):
        put(wo_ref, own_out, 0, (z * Y + lax.rem(y + off, Y), tp))

    for c in late:
        c.wait()
    got(xz.at[pl.ds(0, Z - 1)], 4)
    x_all = added([xz[j].astype(F32) for j in range(Z)])
    fac = lax.rsqrt(x_all[8:9] / D + EPS)
    xf = x_all * fac
    dlog = jnp.zeros((16, B), F32)
    dshift = jnp.zeros((16, B), F32)
    for h in range(HEADS_DEV):
        dlog = jnp.where(row16 == 4 + h, decay_log_ref[h], dlog)
        dshift = jnp.where(row16 == 4 + h, decay_shift_ref[h], dshift)
    scal = jnp.where(
        row16 < 4,
        jax.nn.sigmoid(xf),
        jnp.where(row16 < 8, jnp.exp(-jnp.exp(dlog) * softplus(xf + dshift)), fac),
    )
    lane_group = lax.div(lax.broadcasted_iota(jnp.int32, (16, B), 1), 4)
    mine = jnp.zeros((16, B), F32)
    for m in range(4):
        rolled = pltpu.roll(scal, lax.rem(B + m * ROWS - kv * ROWS, B), 1)
        mine = jnp.where(lane_group == m, rolled, mine)
    cols = transposed(jnp.concatenate([mine, jnp.zeros((L - 16, B), F32)], axis=0))[0:16]

    head_of = lax.div(lax.broadcasted_iota(jnp.int32, (16, L), 0), 4)
    lane16 = lax.broadcasted_iota(jnp.int32, (16, L), 1)
    beta16 = jnp.sum(jnp.where(lane16 == head_of, cols, 0.0), axis=1, keepdims=True)
    decay16 = jnp.sum(jnp.where(lane16 == 4 + head_of, cols, 0.0), axis=1, keepdims=True)

    got(r2.at[pl.ds(0, N - 1)], 5)
    load_state.wait()
    row_id = lax.broadcasted_iota(jnp.int32, (16, 1), 0)
    acts = []
    for h in range(HEADS_DEV):
        here = [
            [n for n in range(N) if (n // Y % 2) * 2 + n % 2 == want] for want in (h, 3 - h)
        ]
        qk = [r2[n, 0:8, :].astype(F32) for n in here[0]]
        vg = [r2[n, 8:16, :].astype(F32) for n in here[1]]
        total = jnp.concatenate([added(qk), added(vg)], axis=0)
        a = silu(total * cols[:, 8:9])
        inv = lax.rsqrt(jnp.sum(a * a, axis=1, keepdims=True) + EPS)
        norm = jnp.where(row_id < 4, inv * L ** (-0.5), jnp.where(row_id < 8, inv, 1.0))
        acts.append(a * norm)
        for n, lo in ((0, 0), (1, 4), (2, 8), (3, 12)):
            rows_f[n, 4 * h : 4 * h + 4, :] = acts[h][lo : lo + 4]
    flipped = transposed(jnp.concatenate(acts + [jnp.zeros((L - 64, L), F32)], axis=0))
    pieces = [(h, r) for h in range(HEADS_DEV) for r in range(ROWS)]
    for h, r in pieces:
        at = h * 16 + r
        own = state[r, h]
        row = 4 * h + r
        rows_f[4, row : row + 1, :] = jnp.sum(
            own * flipped[:, at : at + 1], axis=0, keepdims=True
        )
        rows_f[5, row : row + 1, :] = jnp.sum(
            own * flipped[:, at + 4 : at + 5], axis=0, keepdims=True
        )
    corr = beta16 * (rows_f[2] - decay16 * rows_f[5])
    along = jnp.sum(rows_f[0] * rows_f[1], axis=1, keepdims=True)
    readout = decay16 * rows_f[4] + along * corr
    readout = readout * lax.rsqrt(jnp.mean(readout * readout, axis=1, keepdims=True) + EPS)
    hall[z] = (readout * head_gain_ref[...] * rows_f[3]).astype(BF16)

    offs = (4, 3, 5, 2, 6, 1, 7)
    for zz in (0, 1, 7, 2, 6, 3, 5, 4):
        @pl.when(z != zz)
        def _(zz=zz):
            put(hall.at[z], hall.at[z], 7, (zz * Y + y, tp))


    def up_cols(yy):
        return wu_ref.at[:, pl.ds(pl.multiple_of(yy * 4 * L, L), 4 * L)]

    own_up = pltpu.make_async_copy(up_cols(y), wu.at[y], lsem.at[0])
    own_up.start()
    for off in (2, 1, 3):
        yy = lax.rem(y + off, Y)
        put(up_cols(yy), wu.at[y], 6, (z * Y + yy, tp))

    got(sgath.at[7], 18)
    for h, r in pieces:
        row = 4 * h + r
        at = h * 16 + 4 + r
        next_ref[r, h] = (
            state[r, h] * decay16[row : row + 1] + flipped[:, at : at + 1] * corr[row : row + 1]
        )
    row_mid = (tp * Y + y) * ROWS
    sel_row = lax.broadcasted_iota(jnp.int32, (16, B), 0)
    sel_lane = lax.broadcasted_iota(jnp.int32, (16, B), 1)
    mid = jnp.zeros((16, L), F32)
    for slot, yy in ((0, y), (2, ya), (5, yb), (7, lax.rem(y + 2, Y))):
        gmix[yy] = gpos[slot]
        pick = (lax.div(sel_row, 4) == yy) & (sel_lane == row_mid + lax.rem(sel_row, 4))
        mid = mid + lax.dot_general(
            jnp.where(pick, 1.0, 0.0).astype(BF16),
            sgath[slot].reshape(L, B),
            (((1,), (1,)), ((), ())),
            preferred_element_type=F32,
        )
    load_out.wait()
    got(wof.at[:, pl.ds(0, 3 * L)], 0)

    got(hall.at[pl.ds(0, Z - 1)], 7)
    heads = hall[...].astype(F32).reshape(Z // 2, 2, 2, 8, L)
    attn = jnp.zeros((Z * ROWS, 4 * L), F32)
    for c in range(2):
        h_even, h_odd = pair_tiles(heads[:, 0, c], heads[:, 1, c])
        for i, hh in ((2 * c, h_even), (2 * c + 1, h_odd)):
            attn = attn + jnp.dot(
                hh.reshape(Z * ROWS, L).astype(BF16),
                wof[i * L : (i + 1) * L, :],
                preferred_element_type=F32,
            )
    a_d = [attn[:, d * L : (d + 1) * L].reshape(Z // 2, 8, L) for d in range(4)]
    even_a, odd_a = pair_tiles(a_d[0], a_d[1])
    even_b, odd_b = pair_tiles(a_d[2], a_d[3])
    a4[:, 0] = jnp.concatenate([even_a, even_b], axis=1).astype(BF16)
    a4[:, 1] = jnp.concatenate([odd_a, odd_b], axis=1).astype(BF16)
    for i in offs:
        put(a4.at[lax.div(tps[i], 2), lax.rem(tps[i], 2)], r4.at[tp], 9, (kv, tps[i]))
    r4[tp] = a4[lax.div(tp, 2), lax.rem(tp, 2)]
    got(r4.at[pl.ds(0, T - 1)], 9)
    mid = mid + added([r4[j].astype(F32) for j in range(T)])

    slot_mid = tp * Y + y
    mgath[slot_mid] = mid.astype(BF16)
    for dy in (2, 1, 3, 0):
        for i in (4, 3, 5, 2, 6, 1, 7, 0):
            if dy or i:
                put(mgath.at[slot_mid], mgath.at[slot_mid], 10, (z * Y + ys_[dy], tps[i]))
    own_up.wait()
    got(wu.at[pl.ds(0, Y - 1)], 6)
    for j in range(Y):
        for i in range(4):
            wut[i * L : (i + 1) * L, j * L : (j + 1) * L] = transposed(
                wu[j, :, i * L : (i + 1) * L].astype(F32)
            ).astype(BF16)
    got(mgath.at[pl.ds(0, PL - 1)], 10)
    pairs = mgath[...].astype(F32).reshape(N // 2, 2, 2, 8, L)
    middles = []
    for c in range(2):
        middles += pair_tiles(pairs[:, 0, c], pairs[:, 1, c])
    middles = [m.reshape(B, L) for m in middles]
    parts = [(middles[d] * gmix[d, 1:2, :]).astype(BF16) for d in range(Y)]
    part = jnp.concatenate(parts, axis=1)
    fz = 4 * L // Z
    for lo, hi, zs in ((2, 6, (4, 3, 5, 2)), (6, 8, (6, 7)), (0, 2, (1, 0))):
        up = lax.dot_general(
            wut[lo * fz : hi * fz, :],
            part,
            (((1,), (1,)), ((), ())),
            preferred_element_type=F32,
        )
        u6[lo:hi] = up.astype(BF16).reshape(hi - lo, fz, B)
        for zz in zs:
            @pl.when(z != zz)
            def _(zz=zz):
                put(u6.at[zz], r6.at[z], 11, (zz * Y + y, tp))

    r6[z] = u6[z]
    def down_rows(yy):
        return wd_ref.at[pl.ds(pl.multiple_of(yy * 4 * L, L), 4 * L), :]

    own_down = pltpu.make_async_copy(down_rows(y), wd.at[y], lsem.at[0])
    own_down.start()
    for off in (2, 1, 3):
        yy = lax.rem(y + off, Y)
        put(down_rows(yy), wd.at[y], 8, (z * Y + yy, tp))

    squares2 = jnp.zeros((8, B), F32)
    for d in range(Y):
        mids[d] = middles[d].astype(BF16)
        squares2 = squares2 + lax.dot_general(
            jnp.ones((8, L), F32),
            middles[d] * middles[d],
            (((1,), (1,)), ((), ())),
            preferred_element_type=F32,
            precision=lax.Precision.HIGHEST,
        )
    sq[z] = squares2
    own_row = lax.broadcasted_iota(jnp.int32, (DT, L), 0) + tp * DT
    own_lane = lax.broadcasted_iota(jnp.int32, (DT, L), 1)
    middle = lax.dot_general(
        jnp.where(own_row == own_lane, 1.0, 0.0).astype(BF16),
        mids[y],
        (((1,), (1,)), ((), ())),
        preferred_element_type=F32,
    )
    got(r6.at[pl.ds(0, Z - 1)], 11)
    up_mine = r6[0].astype(F32)
    for j in range(1, Z):
        up_mine = up_mine + r6[j].astype(F32)
    hidden = jnp.square(jnp.maximum(up_mine, 0.0)).astype(BF16)
    hall7[z] = hidden
    for ref, k in ((hall7, 13), (sq, 12)):
        for zz in range(Z):
            @pl.when(z != zz)
            def _(ref=ref, k=k, zz=zz):
                put(ref.at[z], ref.at[z], k, (zz * Y + y, tp))

    own_down.wait()
    got(wd.at[pl.ds(0, Y - 1)], 8)
    for j in range(Y):
        for i in range(4):
            wdt[j * L : (j + 1) * L, i * L : (i + 1) * L] = transposed(
                wd[j, i * L : (i + 1) * L, :].astype(F32)
            ).astype(BF16)
    got(hall7.at[pl.ds(0, Z - 1)], 13)
    hid = hall7[...].reshape(4 * L, B)
    for lo, hi, ys in ((0, 1, (0,)), (1, Y, (1, 3, 2))):
        down = jnp.dot(wdt[lo * L : hi * L, :], hid, preferred_element_type=F32)
        d8[lo * T : hi * T] = down.reshape((hi - lo) * T, DT, B).astype(BF16)
        for yy in ys:
            for t in (1, 0, 3, 2, 7, 6, 5, 4):
                @pl.when(me_p != yy * T + t)
                def _(yy=yy, t=t):
                    put(d8.at[yy * T + t], r8.at[me_p], 14, (z * Y + yy, t))

    r8[me_p] = d8[me_p]
    got(sq.at[pl.ds(0, Z - 1)], 12)
    total2 = sq[0, 0:1, :]
    for j in range(1, Z):
        total2 = total2 + sq[j, 0:1, :]
    factor2 = lax.rsqrt(total2 / D + EPS)
    got(r8.at[pl.ds(0, PL - 1)], 14)
    parts = [r8[j].astype(F32) for j in range(4)]
    for j in range(4, PL):
        parts[j % 4] = parts[j % 4] + r8[j].astype(F32)
    mixed = (parts[0] + parts[1]) + (parts[2] + parts[3])
    final = middle + mixed * (factor2 * factor2)
    out_ref[...] = final.astype(BF16)
    pltpu.make_async_copy(all_sent, all_sent, ssem).wait()


def hand_over(layer_in, state_in, layer_ref, state_ref, sems):
    copies = [
        pltpu.make_async_copy(state_in, state_ref, sems.at[0]),
        pltpu.make_async_copy(layer_in, layer_ref, sems.at[1]),
    ]
    for c in copies:
        c.start()
    for c in copies:
        c.wait()


def shards(
    Z,
    T,
    stream,
    memory_state,
    attn_gain,
    query_weight,
    key_weight,
    value_weight,
    outgate_weight,
    beta_weight,
    decay_weight,
    decay_log,
    decay_shift,
    head_gain,
    output_weight,
    mixer_gain,
    up_weight,
    down_weight,
):
    N, PL, B, DT = Z * Y, Y * T, Z * Y * ROWS, L // T
    sent_tiles = (
        3 * 3 * 32
        + 12 * 8
        + 7 + 3
        + 7 * 8 - 1 + 8
        + 7 + (N - 1)
        + (Z - 1) + (T - 1) + (PL - 1)
        + 2 * 4 * (Z - 1) + (Z - 1)
        + (PL - 1)
    )
    hbm = pl.BlockSpec(memory_space=pltpu.HBM)
    anywhere = pl.BlockSpec(memory_space=pl.ANY)
    vmem = pl.BlockSpec(memory_space=pltpu.VMEM)
    layer_out, memory_next = pl.pallas_call(
        functools.partial(layer_kernel, Z, T),
        out_shape=(
            pltpu.VMEM((DT, B), BF16),
            pltpu.VMEM(memory_state.shape, F32),
        ),
        in_specs=[hbm] * 16,
        out_specs=(vmem, vmem),
        scratch_shapes=[
            pltpu.VMEM((DT, B), BF16),
            pltpu.VMEM((1, L), F32),
            pltpu.VMEM((1, L), F32),
            pltpu.VMEM((1, L), F32),
            pltpu.VMEM((HEADS_DEV, L), BF16),
            pltpu.VMEM((HEADS_DEV, L), BF16),
            pltpu.SMEM((HEADS_DEV,), F32),
            pltpu.SMEM((HEADS_DEV,), F32),
            pltpu.VMEM((ROWS, HEADS_DEV, L, L), F32),
            pltpu.VMEM((4, L, 4 * L), BF16),
            pltpu.VMEM((4 * L, 4 * L), BF16),
            pltpu.VMEM((8, 8, L), F32),
            pltpu.VMEM((4, 16, L), BF16),
            pltpu.VMEM((8, T, DT, B), BF16),
            pltpu.VMEM((2, 4, L, 2 * L), BF16),
            pltpu.VMEM((Z, 16, B), BF16),
            pltpu.VMEM((N // 2, 2, 16, L), BF16),
            pltpu.VMEM((N, 16, L), BF16),
            pltpu.VMEM((6, 16, L), F32),
            pltpu.VMEM((Z, 16, L), BF16),
            pltpu.VMEM((Z // 2, 2, 16, L), BF16),
            pltpu.VMEM((T, 16, L), BF16),
            pltpu.VMEM((N, 16, L), BF16),
            pltpu.VMEM((Y, L, 4 * L), BF16),
            pltpu.VMEM((Y, 4 * L, L), BF16),
            pltpu.VMEM((Z, 8, B), F32),
            pltpu.VMEM((Z, 4 * L // Z, B), BF16),
            pltpu.VMEM((Z, 4 * L // Z, B), BF16),
            pltpu.VMEM((Z, 4 * L // Z, B), BF16),
            pltpu.VMEM((PL, DT, B), BF16),
            pltpu.VMEM((PL, DT, B), BF16),
            pltpu.VMEM((4 * L, 4 * L), BF16),
            pltpu.VMEM((4 * L, 4 * L), BF16),
            pltpu.VMEM((Y, 8, L), F32),
            pltpu.VMEM((Y, B, L), BF16),
            pltpu.VMEM((sent_tiles, 16, L), BF16),
            pltpu.SemaphoreType.DMA((8,)),
            pltpu.SemaphoreType.DMA,
            pltpu.SemaphoreType.DMA((20,)),
        ],
        compiler_params=pltpu.CompilerParams(
            collective_id=0,
            has_side_effects=True,
            vmem_limit_bytes=67043328 - memory_state.size * 4 - 8192,
        ),
    )(
        stream.T,
        attn_gain.reshape(1, L),
        mixer_gain.reshape(1, L),
        head_gain.reshape(1, L),
        beta_weight.T,
        decay_weight.T,
        decay_log,
        decay_shift,
        memory_state,
        query_weight,
        key_weight,
        value_weight,
        outgate_weight,
        output_weight,
        up_weight,
        down_weight,
    )
    layer_out, memory_next = pl.pallas_call(
        hand_over,
        out_shape=(
            jax.ShapeDtypeStruct((DT, B), BF16),
            jax.ShapeDtypeStruct(memory_state.shape, F32),
        ),
        in_specs=[anywhere] * 2,
        out_specs=(hbm, hbm),
        scratch_shapes=[pltpu.SemaphoreType.DMA((2,))],
        compiler_params=pltpu.CompilerParams(vmem_limit_bytes=2**20),
    )(layer_out, memory_next)
    return layer_out.T, memory_next


def solution(mesh):
    in_specs = (
        P(None, ("kv", "tp")),
        P("kv", "tp", None, None),
        P("kv"),
        P("kv", "tp"),
        P("kv", "tp"),
        P("kv", "tp"),
        P("kv", "tp"),
        P("kv", "tp"),
        P("kv", "tp"),
        P("tp"),
        P("tp"),
        P(),
        P("tp", "kv"),
        P("kv"),
        P("kv", "tp"),
        P("tp", "kv"),
    )
    out_specs = (P(None, ("kv", "tp")), P("kv", "tp", None, None))
    body = functools.partial(shards, mesh.shape["kv"] // Y, mesh.shape["tp"])
    return jax.shard_map(body, mesh=mesh, in_specs=in_specs, out_specs=out_specs, check_vma=False)
```

```python
import functools

import jax
import jax.numpy as jnp
from jax import lax
from jax.experimental import pallas as pl
from jax.experimental.pallas import tpu as pltpu
from jax.sharding import PartitionSpec as P

MESH = pl.DeviceIdType.MESH
F32 = jnp.float32
BF16 = jnp.bfloat16
EPS = 1e-06
Y = 4
L = 128
HEADS_DEV = 4
ROWS = 4


def transposed(x):
    return jnp.transpose(x, (1, 0))


def silu(x):
    return x * jax.nn.sigmoid(x)


def added(parts):
    while len(parts) > 1:
        parts = [a + b for a, b in zip(parts[::2], parts[1::2])] + parts[len(parts) // 2 * 2 :]
    return parts[0]


def softplus(x):
    return jnp.maximum(x, 0.0) + jnp.log1p(jnp.exp(-jnp.abs(x)))


def layer_kernel(
    Z,
    T,
    stream_hbm,
    attn_gain_hbm,
    mixer_gain_hbm,
    head_gain_hbm,
    beta_hbm,
    decay_hbm,
    decay_log_hbm,
    decay_shift_hbm,
    state_ref,
    wq_ref,
    wk_ref,
    wv_ref,
    wg_ref,
    wo_ref,
    wu_ref,
    wd_ref,
    out_ref,
    next_ref,
    stream_ref,
    attn_gain_ref,
    mixer_gain_ref,
    head_gain_ref,
    beta_ref,
    decay_ref,
    decay_log_ref,
    decay_shift_ref,
    state,
    w_in,
    wof,
    gpos,
    etile,
    sgath,
    w1,
    xz,
    s2,
    r2,
    sb,
    hall,
    a4,
    r4,
    mgath,
    wu,
    wd,
    sq,
    u6,
    r6,
    hall7,
    d8,
    r8,
    wut,
    wdt,
    gmix,
    mids,
    all_sent,
    lsem,
    ssem,
    rsem,
):
    N = Z * Y
    PL = Y * T
    B = N * ROWS
    DT = L // T
    D = N * L
    kv = lax.axis_index("kv")
    tp = lax.axis_index("tp")
    z = lax.div(kv, Y)
    y = lax.rem(kv, Y)
    me_p = y * T + tp
    pz, py = lax.rem(z, 2), lax.rem(y, 2)
    za, zb = z + 1 - 2 * pz, lax.rem(z - 1 + 2 * pz + Z, Z)
    ya, yb = y + 1 - 2 * py, lax.rem(y - 1 + 2 * py + Y, Y)
    spots = [kv, za * Y + y, z * Y + ya, za * Y + ya, zb * Y + y, z * Y + yb, zb * Y + yb]
    spot_far = z * Y + lax.rem(y + 2, Y)
    head_a = pz * 2 + py
    heads_a = [head_a, (1 - pz) * 2 + py, pz * 2 + 1 - py, (1 - pz) * 2 + 1 - py]
    groups = ((0, (0, 1, 2, 3)), (1, (0, 4, 5, 6)))
    tps = [lax.rem(tp + i, T) for i in range(T)]
    zs_ = [lax.rem(z + i, Z) for i in range(Z)]
    ys_ = [lax.rem(y + i, Y) for i in range(Y)]
    ys_half, ys_odd = [lax.div(v, 2) for v in ys_], [lax.rem(v, 2) for v in ys_]

    def put(src, dst, k, dev):
        pltpu.make_async_remote_copy(
            src_ref=src,
            dst_ref=dst,
            send_sem=ssem,
            recv_sem=rsem.at[k],
            device_id=dev,
            device_id_type=MESH,
        ).start()

    def got(ref, k):
        with jax.named_scope(f"got{k}"):
            pltpu.make_async_copy(ref, ref, rsem.at[k]).wait()


    loads = [
        pltpu.make_async_copy(w, w_in.at[m], lsem.at[0])
        for m, w in enumerate((wq_ref, wk_ref, wv_ref, wg_ref))
    ]
    small = [
        pltpu.make_async_copy(a, b, lsem.at[3 + i])
        for i, (a, b) in enumerate((
            (stream_hbm, stream_ref),
            (attn_gain_hbm, attn_gain_ref),
            (mixer_gain_hbm, mixer_gain_ref),
            (beta_hbm, beta_ref),
            (decay_hbm, decay_ref),
        ))
    ]
    late = [
        pltpu.make_async_copy(a, b, lsem.at[3 + i])
        for i, (a, b) in enumerate((
            (head_gain_hbm, head_gain_ref),
            (decay_log_hbm, decay_log_ref),
            (decay_shift_hbm, decay_shift_ref),
        ))
    ]
    for c in small:
        c.start()
    own_out = wof.at[:, pl.ds(pl.multiple_of(y * L, L), L)]
    load_out = pltpu.make_async_copy(wo_ref, own_out, lsem.at[1])
    load_state = pltpu.make_async_copy(state_ref, state, lsem.at[2])
    for c in loads:
        c.start()
    load_out.start()
    load_state.start()

    barrier = pltpu.get_barrier_semaphore()

    def greet(dev):
        pl.semaphore_signal(barrier, inc=1, device_id=dev, device_id_type=MESH)

    with jax.named_scope("greet"):
        for dst in reversed(spots[1:]):
            for t in tps:
                greet((dst, t))
        for off in (4, 3, 5, 2, 6):
            greet((lax.rem(z + off, Z) * Y + y, tp))
        greet((spot_far, tp))
        for t in tps[1:]:
            greet((kv, t))

    for c in small:
        c.wait()
    for c in late:
        c.start()
    gpos[0] = jnp.broadcast_to(attn_gain_ref[...], (8, L))
    gpos[0, 1:2, :] = mixer_gain_ref[...]
    etile[0] = jnp.concatenate(
        [beta_ref[...].astype(F32), decay_ref[...].astype(F32), jnp.zeros((8, L), F32)], axis=0
    ).astype(BF16)
    sgath[0, tp] = stream_ref[...]

    with jax.named_scope("greeted"):
        pl.semaphore_wait(barrier, 7 * T - 1 + (Z - 3) + 1)

    put(gpos.at[0], gpos.at[7], 1, (spot_far, tp))
    for k in (3, 6, 1, 2, 4, 5):
        put(gpos.at[0], gpos.at[k], 1, (spots[k], tp))
        if k < 4:
            put(etile.at[0], etile.at[k], 2, (spots[k], tp))
    for k in (3, 6, 1, 2, 4, 5):
        for i in (4, 3, 5, 2, 6, 1, 7, 0):
            put(sgath.at[0, tp], sgath.at[k, tp], (16 if k < 4 else 17), (spots[k], tps[i]))
    for i in (4, 3, 5, 2, 6, 1, 7):
        put(sgath.at[0, tp], sgath.at[0, tp], 15, (kv, tps[i]))
    pltpu.make_async_copy(w_in, w_in, lsem.at[0]).wait()

    def head_cols(m, h):
        return w_in.at[m, :, pl.ds(pl.multiple_of(h * L, L), L)]

    def send_weights(g):
        members = groups[g][1]
        for slot in (3, 1, 2):
            h = heads_a[slot]
            h = h if g == 0 else 3 - h
            for i in range(2):
                put(
                    head_cols(2 * g + i, h),
                    w1.at[g, slot, :, pl.ds(i * L, L)],
                    3 if g == 0 else 19,
                    (spots[members[slot]], tp),
                )

    send_weights(0)
    for g in range(2):
        for i in range(2):
            pltpu.make_async_copy(
                head_cols(2 * g + i, head_a if g == 0 else 3 - head_a),
                w1.at[g, 0, :, pl.ds(i * L, L)],
                lsem.at[0],
            ).start()
    send_weights(1)
    got(gpos.at[pl.ds(1, 7)], 1)
    got(etile.at[pl.ds(1, 3)], 2)
    x_part = jnp.zeros((16, B), F32)
    squares = jnp.zeros((1, B), F32)
    scaled = {}
    for k in (0, 1, 2, 3, 4, 5, 6):
        if k == 0:
            got(sgath.at[0, pl.ds(0, T - 1)], 15)
        elif k == 1:
            got(sgath.at[pl.ds(1, 3)], 16)
        elif k == 4:
            got(sgath.at[pl.ds(4, 3)], 17)
        block = sgath[k].astype(F32).reshape(L, B)
        part = (transposed(block) * gpos[k, 0:1, :]).astype(BF16)
        scaled[k] = part
        if k < 4:
            squares = squares + jnp.sum(block * block, axis=0, keepdims=True)
            x_part = x_part + lax.dot_general(
                etile[k], part, (((1,), (1,)), ((), ())), preferred_element_type=F32
            )
        if k == 3:
            row16 = lax.broadcasted_iota(jnp.int32, (16, B), 0)
            xslot = lax.div(z, 2) * (Y // 2) + lax.div(y, 2)
            xz[xslot] = jnp.where(row16 == 8, squares, x_part).astype(BF16)
            for i in (2, 1, 3, 0):
                for j in (1, 0):
                    if i or j:
                        zz, yy = lax.rem(z + 2 * i, Z), lax.rem(y + 2 * j, Y)
                        put(xz.at[xslot], xz.at[xslot], 4, (zz * Y + yy, tp))

    pltpu.make_async_copy(w1.at[:, 0], w1.at[:, 0], lsem.at[0]).wait()
    proj = []
    for g, members in groups:
        got(w1.at[g, pl.ds(1, 3)], 3 if g == 0 else 19)
        total = jnp.zeros((B, 2 * L), F32)
        for slot, k in enumerate(members):
            total = total + jnp.dot(scaled[k], w1[g, slot], preferred_element_type=F32)
        proj += [total[:, 0:L], total[:, L : 2 * L]]
    def pair_tiles(a, b):
        low = lax.broadcasted_iota(jnp.int32, a.shape, 1) < 4
        return (
            jnp.where(low, a, pltpu.roll(b, 4, 1)),
            jnp.where(low, pltpu.roll(a, 4, 1), b),
        )

    pq, pk, pv, pg = [p.reshape(B // 8, 8, L) for p in proj]
    even_a, odd_a = pair_tiles(pq, pk)
    even_b, odd_b = pair_tiles(pv, pg)
    s2[:, 0] = jnp.concatenate([even_a, even_b], axis=1).astype(BF16)
    s2[:, 1] = jnp.concatenate([odd_a, odd_b], axis=1).astype(BF16)
    for dz in (4, 3, 5, 2, 6, 1, 7, 0):
        for dy in (2, 1, 3, 0):
            if dz or dy:
                zz, yy = zs_[dz], ys_[dy]
                put(s2.at[2 * zz + ys_half[dy], ys_odd[dy]], r2.at[kv], 5, (zz * Y + yy, tp))
    r2[kv] = s2[lax.div(kv, 2), lax.rem(kv, 2)]

    for t in tps:
        put(sgath.at[0, tp], sgath.at[7, tp], 18, (spot_far, t))
    for off in (2, 1, 3):
        put(wo_ref, own_out, 0, (z * Y + lax.rem(y + off, Y), tp))

    for c in late:
        c.wait()
    got(xz.at[pl.ds(0, Z - 1)], 4)
    x_all = added([xz[j].astype(F32) for j in range(Z)])
    fac = lax.rsqrt(x_all[8:9] / D + EPS)
    xf = x_all * fac
    dlog = jnp.zeros((16, B), F32)
    dshift = jnp.zeros((16, B), F32)
    for h in range(HEADS_DEV):
        dlog = jnp.where(row16 == 4 + h, decay_log_ref[h], dlog)
        dshift = jnp.where(row16 == 4 + h, decay_shift_ref[h], dshift)
    scal = jnp.where(
        row16 < 4,
        jax.nn.sigmoid(xf),
        jnp.where(row16 < 8, jnp.exp(-jnp.exp(dlog) * softplus(xf + dshift)), fac),
    )
    lane_group = lax.div(lax.broadcasted_iota(jnp.int32, (16, B), 1), 4)
    mine = jnp.zeros((16, B), F32)
    for m in range(4):
        rolled = pltpu.roll(scal, lax.rem(B + m * ROWS - kv * ROWS, B), 1)
        mine = jnp.where(lane_group == m, rolled, mine)
    cols = transposed(jnp.concatenate([mine, jnp.zeros((L - 16, B), F32)], axis=0))[0:16]

    pieces = [(h, r) for h in range(HEADS_DEV) for r in range(ROWS)]
    load_state.wait()
    for h, r in pieces:
        tall, wide = h // 2 * L, h % 2 * L
        sb[r, tall : tall + L, wide : wide + L] = state[r, h].astype(BF16)
    row8 = lax.broadcasted_iota(jnp.int32, (8, L), 0)
    row_of = lax.rem(row8, 4)

    got(r2.at[pl.ds(0, N - 1)], 5)
    acts = []
    for h in range(HEADS_DEV):
        here = [
            [n for n in range(N) if (n // Y % 2) * 2 + n % 2 == want] for want in (h, 3 - h)
        ]
        qk = [r2[n, 0:8, :].astype(F32) for n in here[0]]
        vg = [r2[n, 8:16, :].astype(F32) for n in here[1]]
        total = jnp.concatenate([added(qk), added(vg)], axis=0)
        acts.append(silu(total * cols[:, 8:9]))
    none = jnp.zeros((8, L), F32)
    lhs = [
        jnp.concatenate([acts[h][0:8], none] if h < 2 else [none, acts[h][0:8]], axis=1)
        for h in range(HEADS_DEV)
    ]
    lhs = jnp.concatenate(lhs, axis=0).astype(BF16)
    taken = [jnp.dot(lhs, sb[r], preferred_element_type=F32) for r in range(ROWS)]
    corrs, gated = [], []
    for h in range(HEADS_DEV):
        wide = h % 2 * L
        got_qk = taken[3][8 * h : 8 * h + 8, wide : wide + L]
        for r in range(3):
            got_qk = jnp.where(row_of == r, taken[r][8 * h : 8 * h + 8, wide : wide + L], got_qk)
        q_rows, v_rows = acts[h][0:8], acts[h][8:16]
        k_rows, gates = pltpu.roll(q_rows, 4, 0), pltpu.roll(v_rows, 4, 0)
        q_norm = lax.rsqrt(jnp.sum(q_rows * q_rows, axis=1, keepdims=True) + EPS) * L ** (-0.5)
        k_norm = lax.rsqrt(jnp.sum(k_rows * k_rows, axis=1, keepdims=True) + EPS)
        along = jnp.sum(q_rows * k_rows, axis=1, keepdims=True) * (q_norm * k_norm)
        beta, decay = cols[0:8, h : h + 1], cols[0:8, 4 + h : 5 + h]
        corr = beta * (v_rows - (decay * k_norm) * pltpu.roll(got_qk, 4, 0))
        readout = (decay * q_norm) * got_qk + along * corr
        readout = readout * lax.rsqrt(jnp.mean(readout * readout, axis=1, keepdims=True) + EPS)
        gated.append(readout * head_gain_ref[...] * gates)
        corrs.append(k_norm * corr)
    gated = [
        jnp.where(row8 < 4, gated[h], pltpu.roll(gated[h + 1], 4, 0)) for h in (0, 2)
    ]
    hall[z] = jnp.concatenate(gated, axis=0).astype(BF16)

    offs = (4, 3, 5, 2, 6, 1, 7)
    for zz in (0, 1, 7, 2, 6, 3, 5, 4):
        @pl.when(z != zz)
        def _(zz=zz):
            put(hall.at[z], hall.at[z], 7, (zz * Y + y, tp))


    def up_cols(yy):
        return wu_ref.at[:, pl.ds(pl.multiple_of(yy * 4 * L, L), 4 * L)]

    own_up = pltpu.make_async_copy(up_cols(y), wu.at[y], lsem.at[0])
    own_up.start()
    for off in (2, 1, 3):
        yy = lax.rem(y + off, Y)
        put(up_cols(yy), wu.at[y], 6, (z * Y + yy, tp))

    got(sgath.at[7], 18)
    flipped = transposed(jnp.concatenate(acts + [jnp.zeros((L - 64, L), F32)], axis=0))
    for h, r in pieces:
        at = h * 16 + 4 + r
        next_ref[r, h] = (
            state[r, h] * cols[r : r + 1, 4 + h : 5 + h]
            + flipped[:, at : at + 1] * corrs[h][r : r + 1]
        )
    row_mid = (tp * Y + y) * ROWS
    sel_row = lax.broadcasted_iota(jnp.int32, (16, B), 0)
    sel_lane = lax.broadcasted_iota(jnp.int32, (16, B), 1)
    mid = jnp.zeros((16, L), F32)
    for slot, yy in ((0, y), (2, ya), (5, yb), (7, lax.rem(y + 2, Y))):
        gmix[yy] = gpos[slot]
        pick = (lax.div(sel_row, 4) == yy) & (sel_lane == row_mid + lax.rem(sel_row, 4))
        mid = mid + lax.dot_general(
            jnp.where(pick, 1.0, 0.0).astype(BF16),
            sgath[slot].reshape(L, B),
            (((1,), (1,)), ((), ())),
            preferred_element_type=F32,
        )
    load_out.wait()
    got(wof.at[:, pl.ds(0, 3 * L)], 0)

    got(hall.at[pl.ds(0, Z - 1)], 7)
    heads = hall[...].astype(F32).reshape(Z // 2, 2, 2, 8, L)
    attn = jnp.zeros((Z * ROWS, 4 * L), F32)
    for c in range(2):
        h_even, h_odd = pair_tiles(heads[:, 0, c], heads[:, 1, c])
        for i, hh in ((2 * c, h_even), (2 * c + 1, h_odd)):
            attn = attn + jnp.dot(
                hh.reshape(Z * ROWS, L).astype(BF16),
                wof[i * L : (i + 1) * L, :],
                preferred_element_type=F32,
            )
    a_d = [attn[:, d * L : (d + 1) * L].reshape(Z // 2, 8, L) for d in range(4)]
    even_a, odd_a = pair_tiles(a_d[0], a_d[1])
    even_b, odd_b = pair_tiles(a_d[2], a_d[3])
    a4[:, 0] = jnp.concatenate([even_a, even_b], axis=1).astype(BF16)
    a4[:, 1] = jnp.concatenate([odd_a, odd_b], axis=1).astype(BF16)
    for i in offs:
        put(a4.at[lax.div(tps[i], 2), lax.rem(tps[i], 2)], r4.at[tp], 9, (kv, tps[i]))
    r4[tp] = a4[lax.div(tp, 2), lax.rem(tp, 2)]
    got(r4.at[pl.ds(0, T - 1)], 9)
    mid = mid + added([r4[j].astype(F32) for j in range(T)])

    slot_mid = tp * Y + y
    mgath[slot_mid] = mid.astype(BF16)
    for dy in (2, 1, 3, 0):
        for i in (4, 3, 5, 2, 6, 1, 7, 0):
            if dy or i:
                put(mgath.at[slot_mid], mgath.at[slot_mid], 10, (z * Y + ys_[dy], tps[i]))
    own_up.wait()
    got(wu.at[pl.ds(0, Y - 1)], 6)
    for j in range(Y):
        for i in range(4):
            wut[i * L : (i + 1) * L, j * L : (j + 1) * L] = transposed(
                wu[j, :, i * L : (i + 1) * L].astype(F32)
            ).astype(BF16)
    got(mgath.at[pl.ds(0, PL - 1)], 10)
    pairs = mgath[...].astype(F32).reshape(N // 2, 2, 2, 8, L)
    middles = []
    for c in range(2):
        middles += pair_tiles(pairs[:, 0, c], pairs[:, 1, c])
    middles = [m.reshape(B, L) for m in middles]
    parts = [(middles[d] * gmix[d, 1:2, :]).astype(BF16) for d in range(Y)]
    part = jnp.concatenate(parts, axis=1)
    fz = 4 * L // Z
    for lo, hi, zs in ((2, 6, (4, 3, 5, 2)), (6, 8, (6, 7)), (0, 2, (1, 0))):
        up = lax.dot_general(
            wut[lo * fz : hi * fz, :],
            part,
            (((1,), (1,)), ((), ())),
            preferred_element_type=F32,
        )
        u6[lo:hi] = up.astype(BF16).reshape(hi - lo, fz, B)
        for zz in zs:
            @pl.when(z != zz)
            def _(zz=zz):
                put(u6.at[zz], r6.at[z], 11, (zz * Y + y, tp))

    r6[z] = u6[z]
    def down_rows(yy):
        return wd_ref.at[pl.ds(pl.multiple_of(yy * 4 * L, L), 4 * L), :]

    own_down = pltpu.make_async_copy(down_rows(y), wd.at[y], lsem.at[0])
    own_down.start()
    for off in (2, 1, 3):
        yy = lax.rem(y + off, Y)
        put(down_rows(yy), wd.at[y], 8, (z * Y + yy, tp))

    squares2 = jnp.zeros((8, B), F32)
    for d in range(Y):
        mids[d] = middles[d].astype(BF16)
        squares2 = squares2 + lax.dot_general(
            jnp.ones((8, L), F32),
            middles[d] * middles[d],
            (((1,), (1,)), ((), ())),
            preferred_element_type=F32,
            precision=lax.Precision.HIGHEST,
        )
    sq[z] = squares2
    own_row = lax.broadcasted_iota(jnp.int32, (DT, L), 0) + tp * DT
    own_lane = lax.broadcasted_iota(jnp.int32, (DT, L), 1)
    middle = lax.dot_general(
        jnp.where(own_row == own_lane, 1.0, 0.0).astype(BF16),
        mids[y],
        (((1,), (1,)), ((), ())),
        preferred_element_type=F32,
    )
    got(r6.at[pl.ds(0, Z - 1)], 11)
    up_mine = r6[0].astype(F32)
    for j in range(1, Z):
        up_mine = up_mine + r6[j].astype(F32)
    hidden = jnp.square(jnp.maximum(up_mine, 0.0)).astype(BF16)
    hall7[z] = hidden
    for ref, k in ((hall7, 13), (sq, 12)):
        for zz in range(Z):
            @pl.when(z != zz)
            def _(ref=ref, k=k, zz=zz):
                put(ref.at[z], ref.at[z], k, (zz * Y + y, tp))

    own_down.wait()
    got(wd.at[pl.ds(0, Y - 1)], 8)
    for j in range(Y):
        for i in range(4):
            wdt[j * L : (j + 1) * L, i * L : (i + 1) * L] = transposed(
                wd[j, i * L : (i + 1) * L, :].astype(F32)
            ).astype(BF16)
    got(hall7.at[pl.ds(0, Z - 1)], 13)
    hid = hall7[...].reshape(4 * L, B)
    for lo, hi, ys in ((0, 1, (0,)), (1, Y, (1, 3, 2))):
        down = jnp.dot(wdt[lo * L : hi * L, :], hid, preferred_element_type=F32)
        d8[lo * T : hi * T] = down.reshape((hi - lo) * T, DT, B).astype(BF16)
        for yy in ys:
            for t in (1, 0, 3, 2, 7, 6, 5, 4):
                @pl.when(me_p != yy * T + t)
                def _(yy=yy, t=t):
                    put(d8.at[yy * T + t], r8.at[me_p], 14, (z * Y + yy, t))

    r8[me_p] = d8[me_p]
    got(sq.at[pl.ds(0, Z - 1)], 12)
    total2 = sq[0, 0:1, :]
    for j in range(1, Z):
        total2 = total2 + sq[j, 0:1, :]
    factor2 = lax.rsqrt(total2 / D + EPS)
    got(r8.at[pl.ds(0, PL - 1)], 14)
    parts = [r8[j].astype(F32) for j in range(4)]
    for j in range(4, PL):
        parts[j % 4] = parts[j % 4] + r8[j].astype(F32)
    mixed = (parts[0] + parts[1]) + (parts[2] + parts[3])
    final = middle + mixed * (factor2 * factor2)
    out_ref[...] = final.astype(BF16)
    pltpu.make_async_copy(all_sent, all_sent, ssem).wait()


def hand_over(layer_in, state_in, layer_ref, state_ref, sems):
    copies = [
        pltpu.make_async_copy(state_in, state_ref, sems.at[0]),
        pltpu.make_async_copy(layer_in, layer_ref, sems.at[1]),
    ]
    for c in copies:
        c.start()
    for c in copies:
        c.wait()


def shards(
    Z,
    T,
    stream,
    memory_state,
    attn_gain,
    query_weight,
    key_weight,
    value_weight,
    outgate_weight,
    beta_weight,
    decay_weight,
    decay_log,
    decay_shift,
    head_gain,
    output_weight,
    mixer_gain,
    up_weight,
    down_weight,
):
    N, PL, B, DT = Z * Y, Y * T, Z * Y * ROWS, L // T
    sent_tiles = (
        3 * 3 * 32
        + 12 * 8
        + 7 + 3
        + 7 * 8 - 1 + 8
        + 7 + (N - 1)
        + (Z - 1) + (T - 1) + (PL - 1)
        + 2 * 4 * (Z - 1) + (Z - 1)
        + (PL - 1)
    )
    hbm = pl.BlockSpec(memory_space=pltpu.HBM)
    anywhere = pl.BlockSpec(memory_space=pl.ANY)
    vmem = pl.BlockSpec(memory_space=pltpu.VMEM)
    layer_out, memory_next = pl.pallas_call(
        functools.partial(layer_kernel, Z, T),
        out_shape=(
            pltpu.VMEM((DT, B), BF16),
            pltpu.VMEM(memory_state.shape, F32),
        ),
        in_specs=[hbm] * 16,
        out_specs=(vmem, vmem),
        scratch_shapes=[
            pltpu.VMEM((DT, B), BF16),
            pltpu.VMEM((1, L), F32),
            pltpu.VMEM((1, L), F32),
            pltpu.VMEM((1, L), F32),
            pltpu.VMEM((HEADS_DEV, L), BF16),
            pltpu.VMEM((HEADS_DEV, L), BF16),
            pltpu.SMEM((HEADS_DEV,), F32),
            pltpu.SMEM((HEADS_DEV,), F32),
            pltpu.VMEM((ROWS, HEADS_DEV, L, L), F32),
            pltpu.VMEM((4, L, 4 * L), BF16),
            pltpu.VMEM((4 * L, 4 * L), BF16),
            pltpu.VMEM((8, 8, L), F32),
            pltpu.VMEM((4, 16, L), BF16),
            pltpu.VMEM((8, T, DT, B), BF16),
            pltpu.VMEM((2, 4, L, 2 * L), BF16),
            pltpu.VMEM((Z, 16, B), BF16),
            pltpu.VMEM((N // 2, 2, 16, L), BF16),
            pltpu.VMEM((N, 16, L), BF16),
            pltpu.VMEM((ROWS, 2 * L, 2 * L), BF16),
            pltpu.VMEM((Z, 16, L), BF16),
            pltpu.VMEM((Z // 2, 2, 16, L), BF16),
            pltpu.VMEM((T, 16, L), BF16),
            pltpu.VMEM((N, 16, L), BF16),
            pltpu.VMEM((Y, L, 4 * L), BF16),
            pltpu.VMEM((Y, 4 * L, L), BF16),
            pltpu.VMEM((Z, 8, B), F32),
            pltpu.VMEM((Z, 4 * L // Z, B), BF16),
            pltpu.VMEM((Z, 4 * L // Z, B), BF16),
            pltpu.VMEM((Z, 4 * L // Z, B), BF16),
            pltpu.VMEM((PL, DT, B), BF16),
            pltpu.VMEM((PL, DT, B), BF16),
            pltpu.VMEM((4 * L, 4 * L), BF16),
            pltpu.VMEM((4 * L, 4 * L), BF16),
            pltpu.VMEM((Y, 8, L), F32),
            pltpu.VMEM((Y, B, L), BF16),
            pltpu.VMEM((sent_tiles, 16, L), BF16),
            pltpu.SemaphoreType.DMA((8,)),
            pltpu.SemaphoreType.DMA,
            pltpu.SemaphoreType.DMA((20,)),
        ],
        compiler_params=pltpu.CompilerParams(
            collective_id=0,
            has_side_effects=True,
            vmem_limit_bytes=67043328 - memory_state.size * 4 - 8192,
        ),
    )(
        stream.T,
        attn_gain.reshape(1, L),
        mixer_gain.reshape(1, L),
        head_gain.reshape(1, L),
        beta_weight.T,
        decay_weight.T,
        decay_log,
        decay_shift,
        memory_state,
        query_weight,
        key_weight,
        value_weight,
        outgate_weight,
        output_weight,
        up_weight,
        down_weight,
    )
    layer_out, memory_next = pl.pallas_call(
        hand_over,
        out_shape=(
            jax.ShapeDtypeStruct((DT, B), BF16),
            jax.ShapeDtypeStruct(memory_state.shape, F32),
        ),
        in_specs=[anywhere] * 2,
        out_specs=(hbm, hbm),
        scratch_shapes=[pltpu.SemaphoreType.DMA((2,))],
        compiler_params=pltpu.CompilerParams(vmem_limit_bytes=2**20),
    )(layer_out, memory_next)
    return layer_out.T, memory_next


def solution(mesh):
    in_specs = (
        P(None, ("kv", "tp")),
        P("kv", "tp", None, None),
        P("kv"),
        P("kv", "tp"),
        P("kv", "tp"),
        P("kv", "tp"),
        P("kv", "tp"),
        P("kv", "tp"),
        P("kv", "tp"),
        P("tp"),
        P("tp"),
        P(),
        P("tp", "kv"),
        P("kv"),
        P("kv", "tp"),
        P("tp", "kv"),
    )
    out_specs = (P(None, ("kv", "tp")), P("kv", "tp", None, None))
    body = functools.partial(shards, mesh.shape["kv"] // Y, mesh.shape["tp"])
    return jax.shard_map(body, mesh=mesh, in_specs=in_specs, out_specs=out_specs, check_vma=False)
```

```python
import functools

import jax
import jax.numpy as jnp
from jax import lax
from jax.experimental import pallas as pl
from jax.experimental.pallas import tpu as pltpu
from jax.sharding import PartitionSpec as P

MESH = pl.DeviceIdType.MESH
F32 = jnp.float32
BF16 = jnp.bfloat16
EPS = 1e-06
Y = 4
L = 128
HEADS_DEV = 4
ROWS = 4


def transposed(x):
    return jnp.transpose(x, (1, 0))


def silu(x):
    return x * jax.nn.sigmoid(x)


def added(parts):
    while len(parts) > 1:
        parts = [a + b for a, b in zip(parts[::2], parts[1::2])] + parts[len(parts) // 2 * 2 :]
    return parts[0]


def softplus(x):
    return jnp.maximum(x, 0.0) + jnp.log1p(jnp.exp(-jnp.abs(x)))


def layer_kernel(
    Z,
    T,
    stream_hbm,
    attn_gain_hbm,
    mixer_gain_hbm,
    head_gain_hbm,
    beta_hbm,
    decay_hbm,
    decay_log_hbm,
    decay_shift_hbm,
    state_ref,
    wq_ref,
    wk_ref,
    wv_ref,
    wg_ref,
    wo_ref,
    wu_ref,
    wd_ref,
    out_ref,
    next_ref,
    stream_ref,
    attn_gain_ref,
    mixer_gain_ref,
    head_gain_ref,
    beta_ref,
    decay_ref,
    decay_log_ref,
    decay_shift_ref,
    state,
    w_in,
    wof,
    gpos,
    etile,
    sgath,
    w1,
    xz,
    s2,
    r2,
    sb,
    hall,
    a4,
    r4,
    mgath,
    wu,
    wd,
    sq,
    u6,
    r6,
    hall7,
    d8,
    r8,
    wut,
    wdt,
    gmix,
    mids,
    all_sent,
    lsem,
    ssem,
    rsem,
):
    N = Z * Y
    PL = Y * T
    B = N * ROWS
    DT = L // T
    D = N * L
    kv = lax.axis_index("kv")
    tp = lax.axis_index("tp")
    z = lax.div(kv, Y)
    y = lax.rem(kv, Y)
    me_p = y * T + tp
    pz, py = lax.rem(z, 2), lax.rem(y, 2)
    za, zb = z + 1 - 2 * pz, lax.rem(z - 1 + 2 * pz + Z, Z)
    ya, yb = y + 1 - 2 * py, lax.rem(y - 1 + 2 * py + Y, Y)
    spots = [kv, za * Y + y, z * Y + ya, za * Y + ya, zb * Y + y, z * Y + yb, zb * Y + yb]
    spot_far = z * Y + lax.rem(y + 2, Y)
    head_a = pz * 2 + py
    heads_a = [head_a, (1 - pz) * 2 + py, pz * 2 + 1 - py, (1 - pz) * 2 + 1 - py]
    groups = ((0, (0, 1, 2, 3)), (1, (0, 4, 5, 6)))
    tps = [lax.rem(tp + i, T) for i in range(T)]
    zs_ = [lax.rem(z + i, Z) for i in range(Z)]
    ys_ = [lax.rem(y + i, Y) for i in range(Y)]
    ys_half, ys_odd = [lax.div(v, 2) for v in ys_], [lax.rem(v, 2) for v in ys_]

    def put(src, dst, k, dev):
        pltpu.make_async_remote_copy(
            src_ref=src,
            dst_ref=dst,
            send_sem=ssem,
            recv_sem=rsem.at[k],
            device_id=dev,
            device_id_type=MESH,
        ).start()

    def got(ref, k):
        with jax.named_scope(f"got{k}"):
            pltpu.make_async_copy(ref, ref, rsem.at[k]).wait()


    loads = [
        pltpu.make_async_copy(w, w_in.at[m], lsem.at[0])
        for m, w in enumerate((wq_ref, wk_ref, wv_ref, wg_ref))
    ]
    small = [
        pltpu.make_async_copy(a, b, lsem.at[3 + i])
        for i, (a, b) in enumerate((
            (stream_hbm, stream_ref),
            (attn_gain_hbm, attn_gain_ref),
            (mixer_gain_hbm, mixer_gain_ref),
            (beta_hbm, beta_ref),
            (decay_hbm, decay_ref),
        ))
    ]
    late = [
        pltpu.make_async_copy(a, b, lsem.at[3 + i])
        for i, (a, b) in enumerate((
            (head_gain_hbm, head_gain_ref),
            (decay_log_hbm, decay_log_ref),
            (decay_shift_hbm, decay_shift_ref),
        ))
    ]
    for c in small:
        c.start()
    own_out = wof.at[:, pl.ds(pl.multiple_of(y * L, L), L)]
    load_out = pltpu.make_async_copy(wo_ref, own_out, lsem.at[1])
    load_state = pltpu.make_async_copy(state_ref, state, lsem.at[2])
    for c in loads:
        c.start()
    load_out.start()
    load_state.start()

    barrier = pltpu.get_barrier_semaphore()

    def greet(dev):
        pl.semaphore_signal(barrier, inc=1, device_id=dev, device_id_type=MESH)

    with jax.named_scope("greet"):
        for dst in reversed(spots[1:]):
            for t in tps:
                greet((dst, t))
        for off in (4, 3, 5, 2, 6):
            greet((lax.rem(z + off, Z) * Y + y, tp))
        greet((spot_far, tp))
        for t in tps[1:]:
            greet((kv, t))

    for c in small:
        c.wait()
    for c in late:
        c.start()
    gpos[0] = jnp.broadcast_to(attn_gain_ref[...], (8, L))
    gpos[0, 1:2, :] = mixer_gain_ref[...]
    etile[0] = jnp.concatenate(
        [beta_ref[...].astype(F32), decay_ref[...].astype(F32), jnp.zeros((8, L), F32)], axis=0
    ).astype(BF16)
    sgath[0, tp] = stream_ref[...]

    with jax.named_scope("greeted"):
        pl.semaphore_wait(barrier, 7 * T - 1 + (Z - 3) + 1)

    put(gpos.at[0], gpos.at[7], 1, (spot_far, tp))
    for k in (3, 6, 1, 2, 4, 5):
        put(gpos.at[0], gpos.at[k], 1, (spots[k], tp))
        if k < 4:
            put(etile.at[0], etile.at[k], 2, (spots[k], tp))
    for k in (3, 6, 1, 2, 4, 5):
        for i in (4, 3, 5, 2, 6, 1, 7, 0):
            put(sgath.at[0, tp], sgath.at[k, tp], (16 if k < 4 else 17), (spots[k], tps[i]))
    for i in (4, 3, 5, 2, 6, 1, 7):
        put(sgath.at[0, tp], sgath.at[0, tp], 15, (kv, tps[i]))
    pltpu.make_async_copy(w_in, w_in, lsem.at[0]).wait()

    def head_cols(m, h):
        return w_in.at[m, :, pl.ds(pl.multiple_of(h * L, L), L)]

    def send_weights(g):
        members = groups[g][1]
        for slot in (3, 1, 2):
            h = heads_a[slot]
            h = h if g == 0 else 3 - h
            for i in range(2):
                put(
                    head_cols(2 * g + i, h),
                    w1.at[g, slot, :, pl.ds(i * L, L)],
                    3 if g == 0 else 19,
                    (spots[members[slot]], tp),
                )

    send_weights(0)
    for g in range(2):
        for i in range(2):
            pltpu.make_async_copy(
                head_cols(2 * g + i, head_a if g == 0 else 3 - head_a),
                w1.at[g, 0, :, pl.ds(i * L, L)],
                lsem.at[0],
            ).start()
    send_weights(1)
    got(gpos.at[pl.ds(1, 7)], 1)
    got(etile.at[pl.ds(1, 3)], 2)
    x_part = jnp.zeros((16, B), F32)
    squares = jnp.zeros((1, B), F32)
    scaled = {}
    for k in (0, 1, 2, 3, 4, 5, 6):
        if k == 0:
            got(sgath.at[0, pl.ds(0, T - 1)], 15)
        elif k == 1:
            got(sgath.at[pl.ds(1, 3)], 16)
        elif k == 4:
            got(sgath.at[pl.ds(4, 3)], 17)
        block = sgath[k].astype(F32).reshape(L, B)
        part = (transposed(block) * gpos[k, 0:1, :]).astype(BF16)
        scaled[k] = part
        if k < 4:
            squares = squares + jnp.sum(block * block, axis=0, keepdims=True)
            x_part = x_part + lax.dot_general(
                etile[k], part, (((1,), (1,)), ((), ())), preferred_element_type=F32
            )
        if k == 3:
            row16 = lax.broadcasted_iota(jnp.int32, (16, B), 0)
            xslot = lax.div(z, 2) * (Y // 2) + lax.div(y, 2)
            xz[xslot] = jnp.where(row16 == 8, squares, x_part).astype(BF16)
            for i in (2, 1, 3, 0):
                for j in (1, 0):
                    if i or j:
                        zz, yy = lax.rem(z + 2 * i, Z), lax.rem(y + 2 * j, Y)
                        put(xz.at[xslot], xz.at[xslot], 4, (zz * Y + yy, tp))

    pltpu.make_async_copy(w1.at[:, 0], w1.at[:, 0], lsem.at[0]).wait()
    proj = []
    for g, members in groups:
        got(w1.at[g, pl.ds(1, 3)], 3 if g == 0 else 19)
        total = jnp.zeros((B, 2 * L), F32)
        for slot, k in enumerate(members):
            total = total + jnp.dot(scaled[k], w1[g, slot], preferred_element_type=F32)
        proj += [total[:, 0:L], total[:, L : 2 * L]]
    def pair_tiles(a, b):
        low = lax.broadcasted_iota(jnp.int32, a.shape, 1) < 4
        return (
            jnp.where(low, a, pltpu.roll(b, 4, 1)),
            jnp.where(low, pltpu.roll(a, 4, 1), b),
        )

    pq, pk, pv, pg = [p.reshape(B // 8, 8, L) for p in proj]
    even_a, odd_a = pair_tiles(pq, pk)
    even_b, odd_b = pair_tiles(pv, pg)
    s2[:, 0] = jnp.concatenate([even_a, even_b], axis=1).astype(BF16)
    s2[:, 1] = jnp.concatenate([odd_a, odd_b], axis=1).astype(BF16)
    for dz in (4, 3, 5, 2, 6, 1, 7, 0):
        for dy in (2, 1, 3, 0):
            if dz or dy:
                zz, yy = zs_[dz], ys_[dy]
                put(s2.at[2 * zz + ys_half[dy], ys_odd[dy]], r2.at[kv], 5, (zz * Y + yy, tp))
    r2[kv] = s2[lax.div(kv, 2), lax.rem(kv, 2)]

    for t in tps:
        put(sgath.at[0, tp], sgath.at[7, tp], 18, (spot_far, t))
    load_out.wait()
    for off in (2, 1, 3):
        put(own_out, own_out, 0, (z * Y + ys_[off], tp))

    for c in late:
        c.wait()
    got(xz.at[pl.ds(0, Z - 1)], 4)
    x_all = added([xz[j].astype(F32) for j in range(Z)])
    fac = lax.rsqrt(x_all[8:9] / D + EPS)
    xf = x_all * fac
    dlog = jnp.zeros((16, B), F32)
    dshift = jnp.zeros((16, B), F32)
    for h in range(HEADS_DEV):
        dlog = jnp.where(row16 == 4 + h, decay_log_ref[h], dlog)
        dshift = jnp.where(row16 == 4 + h, decay_shift_ref[h], dshift)
    scal = jnp.where(
        row16 < 4,
        jax.nn.sigmoid(xf),
        jnp.where(row16 < 8, jnp.exp(-jnp.exp(dlog) * softplus(xf + dshift)), fac),
    )
    lane_group = lax.div(lax.broadcasted_iota(jnp.int32, (16, B), 1), 4)
    mine = jnp.zeros((16, B), F32)
    for m in range(4):
        rolled = pltpu.roll(scal, lax.rem(B + m * ROWS - kv * ROWS, B), 1)
        mine = jnp.where(lane_group == m, rolled, mine)
    cols = transposed(jnp.concatenate([mine, jnp.zeros((L - 16, B), F32)], axis=0))[0:16]

    pieces = [(h, r) for h in range(HEADS_DEV) for r in range(ROWS)]
    load_state.wait()
    for h, r in pieces:
        tall, wide = h // 2 * L, h % 2 * L
        sb[r, tall : tall + L, wide : wide + L] = state[r, h].astype(BF16)
    row8 = lax.broadcasted_iota(jnp.int32, (8, L), 0)
    row_of = lax.rem(row8, 4)

    got(r2.at[pl.ds(0, N - 1)], 5)
    acts = []
    for h in range(HEADS_DEV):
        here = [
            [n for n in range(N) if (n // Y % 2) * 2 + n % 2 == want] for want in (h, 3 - h)
        ]
        qk = [r2[n, 0:8, :].astype(F32) for n in here[0]]
        vg = [r2[n, 8:16, :].astype(F32) for n in here[1]]
        total = jnp.concatenate([added(qk), added(vg)], axis=0)
        acts.append(silu(total * cols[:, 8:9]))
    none = jnp.zeros((8, L), F32)
    lhs = [
        jnp.concatenate([acts[h][0:8], none] if h < 2 else [none, acts[h][0:8]], axis=1)
        for h in range(HEADS_DEV)
    ]
    lhs = jnp.concatenate(lhs, axis=0)
    high = lhs.astype(BF16)
    low = (lhs - high.astype(F32)).astype(BF16)
    both = jnp.concatenate([high, low], axis=0)
    taken = [jnp.dot(both, sb[r], preferred_element_type=F32) for r in range(ROWS)]
    taken = [part[0:32] + part[32:64] for part in taken]
    corrs, gated = [], []
    for h in range(HEADS_DEV):
        wide = h % 2 * L
        got_qk = taken[3][8 * h : 8 * h + 8, wide : wide + L]
        for r in range(3):
            got_qk = jnp.where(row_of == r, taken[r][8 * h : 8 * h + 8, wide : wide + L], got_qk)
        q_rows, v_rows = acts[h][0:8], acts[h][8:16]
        k_rows, gates = pltpu.roll(q_rows, 4, 0), pltpu.roll(v_rows, 4, 0)
        q_norm = lax.rsqrt(jnp.sum(q_rows * q_rows, axis=1, keepdims=True) + EPS) * L ** (-0.5)
        k_norm = lax.rsqrt(jnp.sum(k_rows * k_rows, axis=1, keepdims=True) + EPS)
        along = jnp.sum(q_rows * k_rows, axis=1, keepdims=True) * (q_norm * k_norm)
        beta, decay = cols[0:8, h : h + 1], cols[0:8, 4 + h : 5 + h]
        corr = beta * (v_rows - (decay * k_norm) * pltpu.roll(got_qk, 4, 0))
        readout = (decay * q_norm) * got_qk + along * corr
        readout = readout * lax.rsqrt(jnp.mean(readout * readout, axis=1, keepdims=True) + EPS)
        gated.append(readout * head_gain_ref[...] * gates)
        corrs.append(k_norm * corr)
    gated = [
        jnp.where(row8 < 4, gated[h], pltpu.roll(gated[h + 1], 4, 0)) for h in (0, 2)
    ]
    hall[z] = jnp.concatenate(gated, axis=0).astype(BF16)

    offs = (4, 3, 5, 2, 6, 1, 7)
    for zz in (0, 1, 7, 2, 6, 3, 5, 4):
        @pl.when(z != zz)
        def _(zz=zz):
            put(hall.at[z], hall.at[z], 7, (zz * Y + y, tp))


    def up_cols(yy):
        return wu_ref.at[:, pl.ds(pl.multiple_of(yy * 4 * L, L), 4 * L)]

    own_up = pltpu.make_async_copy(up_cols(y), wu.at[y], lsem.at[0])
    own_up.start()
    for off in (2, 1, 3):
        yy = lax.rem(y + off, Y)
        put(up_cols(yy), wu.at[y], 6, (z * Y + yy, tp))

    got(sgath.at[7], 18)
    flipped = transposed(jnp.concatenate(acts + [jnp.zeros((L - 64, L), F32)], axis=0))
    for h, r in pieces:
        at = h * 16 + 4 + r
        next_ref[r, h] = (
            state[r, h] * cols[r : r + 1, 4 + h : 5 + h]
            + flipped[:, at : at + 1] * corrs[h][r : r + 1]
        )
    row_mid = (tp * Y + y) * ROWS
    sel_row = lax.broadcasted_iota(jnp.int32, (16, B), 0)
    sel_lane = lax.broadcasted_iota(jnp.int32, (16, B), 1)
    mid = jnp.zeros((16, L), F32)
    for slot, yy in ((0, y), (2, ya), (5, yb), (7, lax.rem(y + 2, Y))):
        gmix[yy] = gpos[slot]
        pick = (lax.div(sel_row, 4) == yy) & (sel_lane == row_mid + lax.rem(sel_row, 4))
        mid = mid + lax.dot_general(
            jnp.where(pick, 1.0, 0.0).astype(BF16),
            sgath[slot].reshape(L, B),
            (((1,), (1,)), ((), ())),
            preferred_element_type=F32,
        )
    got(wof.at[:, pl.ds(0, 3 * L)], 0)

    got(hall.at[pl.ds(0, Z - 1)], 7)
    heads = hall[...].astype(F32).reshape(Z // 2, 2, 2, 8, L)
    attn = jnp.zeros((Z * ROWS, 4 * L), F32)
    for c in range(2):
        h_even, h_odd = pair_tiles(heads[:, 0, c], heads[:, 1, c])
        for i, hh in ((2 * c, h_even), (2 * c + 1, h_odd)):
            attn = attn + jnp.dot(
                hh.reshape(Z * ROWS, L).astype(BF16),
                wof[i * L : (i + 1) * L, :],
                preferred_element_type=F32,
            )
    a_d = [attn[:, d * L : (d + 1) * L].reshape(Z // 2, 8, L) for d in range(4)]
    even_a, odd_a = pair_tiles(a_d[0], a_d[1])
    even_b, odd_b = pair_tiles(a_d[2], a_d[3])
    a4[:, 0] = jnp.concatenate([even_a, even_b], axis=1).astype(BF16)
    a4[:, 1] = jnp.concatenate([odd_a, odd_b], axis=1).astype(BF16)
    for i in offs:
        put(a4.at[lax.div(tps[i], 2), lax.rem(tps[i], 2)], r4.at[tp], 9, (kv, tps[i]))
    r4[tp] = a4[lax.div(tp, 2), lax.rem(tp, 2)]
    got(r4.at[pl.ds(0, T - 1)], 9)
    mid = mid + added([r4[j].astype(F32) for j in range(T)])

    slot_mid = tp * Y + y
    mgath[slot_mid] = mid.astype(BF16)
    for dy in (2, 1, 3, 0):
        for i in (4, 3, 5, 2, 6, 1, 7, 0):
            if dy or i:
                put(mgath.at[slot_mid], mgath.at[slot_mid], 10, (z * Y + ys_[dy], tps[i]))
    own_up.wait()
    got(wu.at[pl.ds(0, Y - 1)], 6)
    for j in range(Y):
        for i in range(4):
            wut[i * L : (i + 1) * L, j * L : (j + 1) * L] = transposed(
                wu[j, :, i * L : (i + 1) * L].astype(F32)
            ).astype(BF16)
    got(mgath.at[pl.ds(0, PL - 1)], 10)
    pairs = mgath[...].astype(F32).reshape(N // 2, 2, 2, 8, L)
    middles = []
    for c in range(2):
        middles += pair_tiles(pairs[:, 0, c], pairs[:, 1, c])
    middles = [m.reshape(B, L) for m in middles]
    parts = [(middles[d] * gmix[d, 1:2, :]).astype(BF16) for d in range(Y)]
    part = jnp.concatenate(parts, axis=1)
    fz = 4 * L // Z
    for lo, hi, zs in ((2, 6, (4, 3, 5, 2)), (6, 8, (6, 7)), (0, 2, (1, 0))):
        up = lax.dot_general(
            wut[lo * fz : hi * fz, :],
            part,
            (((1,), (1,)), ((), ())),
            preferred_element_type=F32,
        )
        u6[lo:hi] = up.astype(BF16).reshape(hi - lo, fz, B)
        for zz in zs:
            @pl.when(z != zz)
            def _(zz=zz):
                put(u6.at[zz], r6.at[z], 11, (zz * Y + y, tp))

    r6[z] = u6[z]
    def down_rows(yy):
        return wd_ref.at[pl.ds(pl.multiple_of(yy * 4 * L, L), 4 * L), :]

    own_down = pltpu.make_async_copy(down_rows(y), wd.at[y], lsem.at[0])
    own_down.start()
    for off in (2, 1, 3):
        yy = lax.rem(y + off, Y)
        put(down_rows(yy), wd.at[y], 8, (z * Y + yy, tp))

    squares2 = jnp.zeros((8, B), F32)
    for d in range(Y):
        mids[d] = middles[d].astype(BF16)
        squares2 = squares2 + lax.dot_general(
            jnp.ones((8, L), F32),
            middles[d] * middles[d],
            (((1,), (1,)), ((), ())),
            preferred_element_type=F32,
            precision=lax.Precision.HIGHEST,
        )
    sq[z] = squares2
    own_row = lax.broadcasted_iota(jnp.int32, (DT, L), 0) + tp * DT
    own_lane = lax.broadcasted_iota(jnp.int32, (DT, L), 1)
    middle = lax.dot_general(
        jnp.where(own_row == own_lane, 1.0, 0.0).astype(BF16),
        mids[y],
        (((1,), (1,)), ((), ())),
        preferred_element_type=F32,
    )
    got(r6.at[pl.ds(0, Z - 1)], 11)
    up_mine = r6[0].astype(F32)
    for j in range(1, Z):
        up_mine = up_mine + r6[j].astype(F32)
    hidden = jnp.square(jnp.maximum(up_mine, 0.0)).astype(BF16)
    hall7[z] = hidden
    for ref, k in ((hall7, 13), (sq, 12)):
        for zz in range(Z):
            @pl.when(z != zz)
            def _(ref=ref, k=k, zz=zz):
                put(ref.at[z], ref.at[z], k, (zz * Y + y, tp))

    own_down.wait()
    got(wd.at[pl.ds(0, Y - 1)], 8)
    for j in range(Y):
        for i in range(4):
            wdt[j * L : (j + 1) * L, i * L : (i + 1) * L] = transposed(
                wd[j, i * L : (i + 1) * L, :].astype(F32)
            ).astype(BF16)
    got(hall7.at[pl.ds(0, Z - 1)], 13)
    hid = hall7[...].reshape(4 * L, B)
    for lo, hi, ys in ((0, 1, (0,)), (1, Y, (1, 3, 2))):
        down = jnp.dot(wdt[lo * L : hi * L, :], hid, preferred_element_type=F32)
        d8[lo * T : hi * T] = down.reshape((hi - lo) * T, DT, B).astype(BF16)
        for yy in ys:
            for t in (1, 0, 3, 2, 7, 6, 5, 4):
                @pl.when(me_p != yy * T + t)
                def _(yy=yy, t=t):
                    put(d8.at[yy * T + t], r8.at[me_p], 14, (z * Y + yy, t))

    r8[me_p] = d8[me_p]
    got(sq.at[pl.ds(0, Z - 1)], 12)
    total2 = sq[0, 0:1, :]
    for j in range(1, Z):
        total2 = total2 + sq[j, 0:1, :]
    factor2 = lax.rsqrt(total2 / D + EPS)
    got(r8.at[pl.ds(0, PL - 1)], 14)
    parts = [r8[j].astype(F32) for j in range(4)]
    for j in range(4, PL):
        parts[j % 4] = parts[j % 4] + r8[j].astype(F32)
    mixed = (parts[0] + parts[1]) + (parts[2] + parts[3])
    final = middle + mixed * (factor2 * factor2)
    out_ref[...] = final.astype(BF16)
    pltpu.make_async_copy(all_sent, all_sent, ssem).wait()


def hand_over(layer_in, state_in, layer_ref, state_ref, sems):
    copies = [
        pltpu.make_async_copy(state_in, state_ref, sems.at[0]),
        pltpu.make_async_copy(layer_in, layer_ref, sems.at[1]),
    ]
    for c in copies:
        c.start()
    for c in copies:
        c.wait()


def shards(
    Z,
    T,
    stream,
    memory_state,
    attn_gain,
    query_weight,
    key_weight,
    value_weight,
    outgate_weight,
    beta_weight,
    decay_weight,
    decay_log,
    decay_shift,
    head_gain,
    output_weight,
    mixer_gain,
    up_weight,
    down_weight,
):
    N, PL, B, DT = Z * Y, Y * T, Z * Y * ROWS, L // T
    sent_tiles = (
        3 * 3 * 32
        + 12 * 8
        + 7 + 3
        + 7 * 8 - 1 + 8
        + 7 + (N - 1)
        + (Z - 1) + (T - 1) + (PL - 1)
        + 2 * 4 * (Z - 1) + (Z - 1)
        + (PL - 1)
    )
    hbm = pl.BlockSpec(memory_space=pltpu.HBM)
    anywhere = pl.BlockSpec(memory_space=pl.ANY)
    vmem = pl.BlockSpec(memory_space=pltpu.VMEM)
    layer_out, memory_next = pl.pallas_call(
        functools.partial(layer_kernel, Z, T),
        out_shape=(
            pltpu.VMEM((DT, B), BF16),
            pltpu.VMEM(memory_state.shape, F32),
        ),
        in_specs=[hbm] * 16,
        out_specs=(vmem, vmem),
        scratch_shapes=[
            pltpu.VMEM((DT, B), BF16),
            pltpu.VMEM((1, L), F32),
            pltpu.VMEM((1, L), F32),
            pltpu.VMEM((1, L), F32),
            pltpu.VMEM((HEADS_DEV, L), BF16),
            pltpu.VMEM((HEADS_DEV, L), BF16),
            pltpu.SMEM((HEADS_DEV,), F32),
            pltpu.SMEM((HEADS_DEV,), F32),
            pltpu.VMEM((ROWS, HEADS_DEV, L, L), F32),
            pltpu.VMEM((4, L, 4 * L), BF16),
            pltpu.VMEM((4 * L, 4 * L), BF16),
            pltpu.VMEM((8, 8, L), F32),
            pltpu.VMEM((4, 16, L), BF16),
            pltpu.VMEM((8, T, DT, B), BF16),
            pltpu.VMEM((2, 4, L, 2 * L), BF16),
            pltpu.VMEM((Z, 16, B), BF16),
            pltpu.VMEM((N // 2, 2, 16, L), BF16),
            pltpu.VMEM((N, 16, L), BF16),
            pltpu.VMEM((ROWS, 2 * L, 2 * L), BF16),
            pltpu.VMEM((Z, 16, L), BF16),
            pltpu.VMEM((Z // 2, 2, 16, L), BF16),
            pltpu.VMEM((T, 16, L), BF16),
            pltpu.VMEM((N, 16, L), BF16),
            pltpu.VMEM((Y, L, 4 * L), BF16),
            pltpu.VMEM((Y, 4 * L, L), BF16),
            pltpu.VMEM((Z, 8, B), F32),
            pltpu.VMEM((Z, 4 * L // Z, B), BF16),
            pltpu.VMEM((Z, 4 * L // Z, B), BF16),
            pltpu.VMEM((Z, 4 * L // Z, B), BF16),
            pltpu.VMEM((PL, DT, B), BF16),
            pltpu.VMEM((PL, DT, B), BF16),
            pltpu.VMEM((4 * L, 4 * L), BF16),
            pltpu.VMEM((4 * L, 4 * L), BF16),
            pltpu.VMEM((Y, 8, L), F32),
            pltpu.VMEM((Y, B, L), BF16),
            pltpu.VMEM((sent_tiles, 16, L), BF16),
            pltpu.SemaphoreType.DMA((8,)),
            pltpu.SemaphoreType.DMA,
            pltpu.SemaphoreType.DMA((20,)),
        ],
        compiler_params=pltpu.CompilerParams(
            collective_id=0,
            has_side_effects=True,
            vmem_limit_bytes=67043328 - memory_state.size * 4 - 8192,
        ),
    )(
        stream.T,
        attn_gain.reshape(1, L),
        mixer_gain.reshape(1, L),
        head_gain.reshape(1, L),
        beta_weight.T,
        decay_weight.T,
        decay_log,
        decay_shift,
        memory_state,
        query_weight,
        key_weight,
        value_weight,
        outgate_weight,
        output_weight,
        up_weight,
        down_weight,
    )
    layer_out, memory_next = pl.pallas_call(
        hand_over,
        out_shape=(
            jax.ShapeDtypeStruct((DT, B), BF16),
            jax.ShapeDtypeStruct(memory_state.shape, F32),
        ),
        in_specs=[anywhere] * 2,
        out_specs=(hbm, hbm),
        scratch_shapes=[pltpu.SemaphoreType.DMA((2,))],
        compiler_params=pltpu.CompilerParams(vmem_limit_bytes=2**20),
    )(layer_out, memory_next)
    return layer_out.T, memory_next


def solution(mesh):
    in_specs = (
        P(None, ("kv", "tp")),
        P("kv", "tp", None, None),
        P("kv"),
        P("kv", "tp"),
        P("kv", "tp"),
        P("kv", "tp"),
        P("kv", "tp"),
        P("kv", "tp"),
        P("kv", "tp"),
        P("tp"),
        P("tp"),
        P(),
        P("tp", "kv"),
        P("kv"),
        P("kv", "tp"),
        P("tp", "kv"),
    )
    out_specs = (P(None, ("kv", "tp")), P("kv", "tp", None, None))
    body = functools.partial(shards, mesh.shape["kv"] // Y, mesh.shape["tp"])
    return jax.shard_map(body, mesh=mesh, in_specs=in_specs, out_specs=out_specs, check_vma=False)
```
